512 devices in a mesh: sp: 64 (over z, y), tp: 8 (over x, core).
Axes of the slice: x: 4, y: 8, z: 8, core: 2. Of those that a mesh axis runs over, the one named last changes fastest.
Arguments:
- query_one: bfloat16 [8192, 1024], P('sp', 'tp'), may hold values from -6 to 6
- key_one: bfloat16 [8192, 1024], P('sp', 'tp'), may hold values from -6 to 6
- query_two: bfloat16 [8192, 512], P('sp', 'tp'), may hold values from -6 to 6
- key_two: bfloat16 [8192, 512], P('sp', 'tp'), may hold values from -6 to 6
- values: bfloat16 [8192, 2048], P('sp', 'tp'), may hold values from -6 to 6
- out_gate: bfloat16 [8192, 2048], P('sp', 'tp'), may hold values from -6 to 6
- in_gate: float32 [16, 8192], P('tp', 'sp'), may hold values from -3 to 150
- forget_gate: float32 [16, 8192], P('tp', 'sp'), may hold values from -1 to 24
- head_gain: float32 [2048], P('tp'), may hold values from 0.1 to 1.9
- out_weight: bfloat16 [2048, 2048], P('tp'), may hold values from -0.125 to 0.125
- stream: bfloat16 [8192, 2048], P('sp'), may hold values from -6 to 6
- mix_gain: float32 [2048], replicated, may hold values from 0.1 to 1.9
- up_weight: bfloat16 [2048, 8192], P('sp', 'tp'), may hold values from -0.125 to 0.125
- down_weight: bfloat16 [8192, 2048], P('tp', 'sp'), may hold values from -0.0625 to 0.0625
- out_gain: float32 [2048], replicated, may hold values from 0.1 to 1.9
Outputs:
- result: bfloat16 [8192, 2048], P(('sp', 'tp'))
The draws below stay inside these ranges and needn't reach their ends.
All inputs are finite; a program needn't handle non-finite values.
Results may differ from the reference program's by a relative error of at most 0.018.
Values may be sent and summed in bfloat16 or wider, within the bound.
A program may use at most 64 MiB of HBM per device.

```python
import jax
import jax.numpy as jnp
from jax import lax

D = 2048
HEADS = 8
KA = 128
KB = 64
DV = 128
FF = 8192
BLOCK = 64
TOK_DEV = 128
SEQUENCE_TOKENS = 8192
MIX = 2048
GATE_HEADS = 16
N_TP = 8


def draw_forget_gate(key, part):
    merged_keys = jax.random.split(jax.random.fold_in(key, 11), 5)
    slow_share = 0.5
    noise = jnp.clip(jax.random.normal(merged_keys[1], (GATE_HEADS, SEQUENCE_TOKENS), jnp.float32), -3.0, 3.0)
    slow_heads = jax.random.uniform(merged_keys[0], (GATE_HEADS, 1), jnp.float32) < slow_share
    base_level = jnp.where(slow_heads, jnp.log(SEQUENCE_TOKENS / 0.3), jnp.log(40.0))
    device_shift = jax.random.uniform(merged_keys[2], (1, SEQUENCE_TOKENS // TOK_DEV), jnp.float32, -0.7, 0.7)
    device_shift = jnp.repeat(device_shift, TOK_DEV, axis=1)
    level_values = base_level + noise + device_shift
    spike_locations = jax.random.randint(merged_keys[3], (GATE_HEADS, 3), 0, SEQUENCE_TOKENS)
    token_positions = jnp.arange(SEQUENCE_TOKENS, dtype=jnp.int32)
    spike_mask = jnp.any(token_positions[None, None, :] == spike_locations[:, :, None], 1)
    spike_level = jax.random.uniform(merged_keys[4], (GATE_HEADS, SEQUENCE_TOKENS), jnp.float32, 0.3, 1.4)
    return jnp.where(spike_mask, spike_level, level_values).astype(jnp.float32)


def draw_in_gate(key, part):
    merged_keys = jax.random.split(jax.random.fold_in(key, 23), 1)
    level_values = jnp.clip(jax.random.normal(merged_keys[0], (GATE_HEADS, SEQUENCE_TOKENS), jnp.float32), -3.0, 3.0)
    return level_values.astype(jnp.float32)


def level_of(stream_key, shape, cuts, smallest, largest):
    level, own = 1.0, jax.random.fold_in(stream_key, 6)
    for dim, parts in cuts:
        steps = jnp.exp(jax.random.uniform(jax.random.fold_in(own, dim), (parts,), jnp.float32, smallest / len(cuts), largest / len(cuts)))
        level = level * jnp.repeat(steps, shape[dim] // parts).reshape([-1 if axis == dim else 1 for axis in range(len(shape))])
    return level


def gaussian(own_key, extent, deviation, bound, cuts=(), kind=jnp.bfloat16):
    drawn = jax.random.normal(own_key, extent, jnp.float32) * deviation
    if len(cuts) > 0:
        drawn = level_of(own_key, extent, cuts, -0.22, 0.18) * drawn
    return jnp.clip(drawn, min=-bound, max=bound).astype(kind)


def setup_inputs(seed: int = 0) -> dict:
    splits = jax.random.split(jax.random.key(seed), 16)
    query_one = gaussian(splits[0], (SEQUENCE_TOKENS, HEADS * KA), 1.0, 6.0, ((0, 64), (1, 8)))
    key_one = gaussian(splits[1], (SEQUENCE_TOKENS, HEADS * KA), 1.0, 6.0, ((0, 64), (1, 8)))
    query_two = gaussian(splits[2], (SEQUENCE_TOKENS, HEADS * KB), 1.0, 6.0, ((0, 64), (1, 8)))
    key_two = gaussian(splits[3], (SEQUENCE_TOKENS, HEADS * KB), 1.0, 6.0, ((0, 64), (1, 8)))
    values = gaussian(splits[4], (SEQUENCE_TOKENS, MIX), 1.0, 6.0, ((0, 64), (1, 8)))
    out_gate = gaussian(splits[5], (SEQUENCE_TOKENS, MIX), 1.5, 6.0, ((0, 64), (1, 8)))
    in_gate = draw_in_gate(jax.random.fold_in(splits[15], 71), 0)
    forget_gate = draw_forget_gate(jax.random.fold_in(splits[15], 71), 0)
    head_gain = jnp.clip(1.0 + 0.18 * jax.random.normal(splits[8], (MIX,), jnp.float32), 0.1, 1.9)
    out_weight = gaussian(splits[9], (MIX, D), MIX ** -0.5, 0.125, ((0, 8),))
    stream = gaussian(splits[10], (SEQUENCE_TOKENS, D), 1.0, 6.0, ((0, 64),))
    mix_gain = jnp.clip(1.0 + 0.18 * jax.random.normal(splits[11], (D,), jnp.float32), 0.1, 1.9)
    up_weight = gaussian(splits[12], (D, FF), D ** -0.5, 0.125, ((0, 64), (1, 8)))
    down_weight = gaussian(splits[13], (FF, D), FF ** -0.5, 0.0625, ((0, 8), (1, 64)))
    out_gain = jnp.clip(1.0 + 0.18 * jax.random.normal(splits[14], (D,), jnp.float32), 0.1, 1.9)
    return dict(query_one=query_one, key_one=key_one, query_two=query_two, key_two=key_two, values=values, out_gate=out_gate, in_gate=in_gate, forget_gate=forget_gate, head_gain=head_gain, out_weight=out_weight, stream=stream, mix_gain=mix_gain, up_weight=up_weight, down_weight=down_weight, out_gain=out_gain)


NEG_BIG = -1e+30
EPS = 1e-05

def combine(earlier, later):
    decay_early, cell_early, norm_early, peak_early = earlier
    decay_late, cell_late, norm_late, peak_late = later
    ceiling = jnp.maximum(decay_late + peak_early, peak_late)
    keep_share = jnp.exp(decay_late + peak_early - ceiling)
    fresh_share = jnp.exp(peak_late - ceiling)
    cell_new = keep_share[..., None, None] * cell_early + fresh_share[..., None, None] * cell_late
    norm_new = keep_share[..., None] * norm_early + fresh_share[..., None] * norm_late
    return (decay_early + decay_late, cell_new, norm_new, ceiling)

def summarize(queries, keys_in, values_in, in_pre, forget_pre, block_len):
    length, width_k = queries.shape
    block_count = length // block_len
    scaled_keys = keys_in.astype(jnp.float32).reshape(block_count, block_len, width_k) * width_k ** (-0.5)
    values_f = values_in.astype(jnp.float32).reshape(block_count, block_len, -1)
    width_v = values_f.shape[-1]
    log_forget = jax.nn.log_sigmoid(forget_pre).reshape(block_count, block_len)
    log_input = in_pre.reshape(block_count, block_len)
    cumulative = jnp.cumsum(log_forget, 1)
    decay_total = cumulative[:, -1]
    weight_log = decay_total[:, None] - cumulative + log_input
    peak_log = lax.optimization_barrier(jnp.max(weight_log, 1))
    weighted = jnp.exp(weight_log - peak_log[:, None])[..., None] * scaled_keys
    cell_states = jnp.einsum('cld,cle->cde', weighted, values_f, precision=lax.Precision.HIGHEST)
    norm_states = lax.optimization_barrier(jnp.sum(weighted, 1))
    identity = (jnp.zeros((), jnp.float32), jnp.zeros((width_k, width_v), jnp.float32), jnp.zeros((width_k,), jnp.float32), jnp.full((), NEG_BIG, jnp.float32))

    def advance(running, element):
        return (combine(running, element), running)
    closing, prefix = lax.scan(advance, identity, (decay_total, cell_states, norm_states, peak_log))
    return (closing, prefix, (scaled_keys, values_f, cumulative, log_input))

def finish(queries, prefix, pieces, incoming):
    scaled_keys, values_f, cumulative, log_input = pieces
    block_count, block_len, width_k = scaled_keys.shape
    spread_in = jax.tree.map(lambda leaf: jnp.broadcast_to(leaf, (block_count,) + leaf.shape), incoming)
    _, cell_states, norm_states, peaks = combine(spread_in, prefix)
    query_f = queries.astype(jnp.float32).reshape(block_count, block_len, width_k)
    log_gaps = cumulative[:, :, None] - cumulative[:, None, :] + log_input[:, None, :]
    causal = jnp.arange(block_len)[:, None] >= jnp.arange(block_len)[None, :]
    log_gaps = jnp.where(causal[None], log_gaps, -jnp.inf)
    carried = cumulative + peaks[:, None]
    ceiling = jnp.maximum(carried, lax.optimization_barrier(jnp.max(log_gaps, 2)))
    scores = jnp.einsum('cld,csd->cls', query_f, scaled_keys, precision=lax.Precision.HIGHEST)
    scores = scores * jnp.exp(log_gaps - ceiling[..., None])
    carry_weight = jnp.exp(carried - ceiling)
    numerator = carry_weight[..., None] * jnp.einsum('cld,cde->cle', query_f, cell_states, precision=lax.Precision.HIGHEST)
    numerator = numerator + jnp.einsum('cls,cse->cle', scores, values_f, precision=lax.Precision.HIGHEST)
    denominator = carry_weight * jnp.einsum('cld,cd->cl', query_f, norm_states, precision=lax.Precision.HIGHEST)
    denominator = denominator + lax.optimization_barrier(jnp.sum(scores, 2))
    result = numerator / jnp.maximum(jnp.abs(denominator), jnp.exp(-ceiling))[..., None]
    return result.reshape(block_count * block_len, -1)

def run_head(queries, keys_in, values_in, in_pre, forget_pre):
    closing, prefix, pieces = summarize(queries, keys_in, values_in, in_pre, forget_pre, BLOCK)
    identity = jax.tree.map(lambda leaf: jnp.zeros_like(leaf), closing)
    identity = (identity[0], identity[1], identity[2], jnp.full((), NEG_BIG, jnp.float32))
    return finish(queries, prefix, pieces, identity)

def head_norm(cell_out):
    center = lax.optimization_barrier(jnp.mean(cell_out, -1, keepdims=True))
    spread = lax.optimization_barrier(jnp.mean(jnp.square(cell_out - center), -1, keepdims=True))
    return (cell_out - center) * lax.rsqrt(spread + EPS)

def layer_norm(rows_f, gain):
    center = lax.optimization_barrier(jnp.mean(rows_f, -1, keepdims=True))
    spread = lax.optimization_barrier(jnp.mean(jnp.square(rows_f - center), -1, keepdims=True))
    return (rows_f - center) * lax.rsqrt(spread + EPS) * gain

def reference(query_one, key_one, query_two, key_two, values, out_gate, in_gate, forget_gate, head_gain, out_weight, stream, mix_gain, up_weight, down_weight, out_gain):
    columns = []
    for pair_index in range(HEADS):
        base_v = 2 * pair_index * DV
        out_one = run_head(query_one[:, pair_index * KA:(pair_index + 1) * KA], key_one[:, pair_index * KA:(pair_index + 1) * KA], values[:, base_v:base_v + DV], in_gate[2 * pair_index], forget_gate[2 * pair_index])
        out_two = run_head(query_two[:, pair_index * KB:(pair_index + 1) * KB], key_two[:, pair_index * KB:(pair_index + 1) * KB], values[:, base_v + DV:base_v + 2 * DV], in_gate[2 * pair_index + 1], forget_gate[2 * pair_index + 1])
        columns.append(head_norm(out_one))
        columns.append(head_norm(out_two))
    normed = jnp.concatenate(columns, 1)
    mixed_heads = (normed * head_gain * jax.nn.sigmoid(out_gate.astype(jnp.float32))).astype(jnp.bfloat16)
    group_width = MIX // N_TP
    summed = jnp.zeros((SEQUENCE_TOKENS, D), jnp.float32)
    for group in range(N_TP):
        partial_sum = jnp.dot(mixed_heads[:, group * group_width:(group + 1) * group_width], out_weight[group * group_width:(group + 1) * group_width], preferred_element_type=jnp.float32).astype(jnp.bfloat16)
        summed = summed + lax.optimization_barrier(partial_sum).astype(jnp.float32)
    mixer_out = lax.optimization_barrier(summed.astype(jnp.bfloat16))
    first_norm = layer_norm(stream.astype(jnp.float32) + mixer_out.astype(jnp.float32), mix_gain).astype(jnp.bfloat16)
    hidden_width = FF // N_TP

    def mlp_block(row_block):
        hidden = jnp.square(jax.nn.relu(jnp.dot(row_block, up_weight, preferred_element_type=jnp.float32))).astype(jnp.bfloat16)
        total = jnp.zeros((row_block.shape[0], D), jnp.float32)
        for group in range(N_TP):
            partial_sum = jnp.dot(hidden[:, group * hidden_width:(group + 1) * hidden_width], down_weight[group * hidden_width:(group + 1) * hidden_width], preferred_element_type=jnp.float32).astype(jnp.bfloat16)
            total = total + lax.optimization_barrier(partial_sum).astype(jnp.float32)
        mlp_out = lax.optimization_barrier(total.astype(jnp.bfloat16))
        return layer_norm(row_block.astype(jnp.float32) + mlp_out.astype(jnp.float32), out_gain).astype(jnp.bfloat16)
    blocks = first_norm.reshape(SEQUENCE_TOKENS // TOK_DEV, TOK_DEV, D)
    return lax.map(mlp_block, blocks).reshape(SEQUENCE_TOKENS, D)
```

```python
import functools

import jax
import jax.numpy as jnp
from jax import lax
from jax.experimental import pallas as pl
from jax.experimental.pallas import tpu as pltpu
from jax.sharding import Mesh
from jax.sharding import PartitionSpec as P

NEG_BIG = -1e30
EPS = 1e-05
META = 8
f32, bf16 = jnp.float32, jnp.bfloat16
MESH = pl.DeviceIdType.MESH


def dg(a, b, ca, cb):
    return lax.dot_general(a, b, (((ca,), (cb,)), ((), ())), preferred_element_type=f32)


def three(a):
    hi = a.astype(bf16)
    rest = a - hi.astype(f32)
    mid = rest.astype(bf16)
    return hi, mid, (rest - mid.astype(f32)).astype(bf16)


def left_dot(a, b, ca, cb):
    hi, mid, lo = three(a)
    return dg(hi, b, ca, cb) + (dg(mid, b, ca, cb) + dg(lo, b, ca, cb))


def right_dot(a, b, ca, cb):
    hi, mid, lo = three(b)
    return dg(a, hi, ca, cb) + (dg(a, mid, ca, cb) + dg(a, lo, ca, cb))


def remote(src, dst, ssem, rsem, target):
    return pltpu.make_async_remote_copy(
        src_ref=src, dst_ref=dst, send_sem=ssem, recv_sem=rsem, device_id=target, device_id_type=MESH
    )


class Ring:
    def __init__(self, axis, n, block, half, ssem, rsem):
        self.axis, self.n, self.block, self.half = axis, n, block, half
        self.ssem, self.rsem = ssem, rsem
        self.me = lax.axis_index(axis)
        self.steps = n // 2
        self.taken = set()

    def part(self, way, step, distance):
        away = self.n - distance if way == 0 else distance
        index = lax.rem(self.me + away, self.n)
        return self.block(index) if step < self.steps else self.half(index, way)

    def copy(self, way, step, distance):
        ref = self.part(way, step, distance)
        target = lax.rem(self.me + (1 if way == 0 else self.n - 1), self.n)
        return remote(
            ref, ref, self.ssem.at[way, step - 1], self.rsem.at[way, step - 1], {self.axis: target}
        )

    def send(self, step):
        if step <= self.steps:
            for way in (0, 1):
                self.copy(way, step, step - 1).start()

    def take(self, step):
        if 1 <= step <= self.steps and step not in self.taken:
            self.taken.add(step)
            for way in (0, 1):
                self.copy(way, step, step).wait_recv()

    def advance(self, step):
        self.take(step - 1)
        self.send(step)

    def drain(self):
        for step in range(1, self.steps + 1):
            for way in (0, 1):
                self.copy(way, step, step - 1).wait_send()


class Direct:
    def __init__(self, axis, n, source, slots, ssem, rsem):
        self.axis, self.n, self.source, self.slots = axis, n, source, slots
        self.ssem, self.rsem = ssem, rsem
        self.me = lax.axis_index(axis)

    def copy(self, d, slot):
        peer = lax.rem(self.me + d, self.n)
        return remote(
            self.source(peer), self.slots(slot), self.ssem.at[d], self.rsem.at[d], {self.axis: peer}
        )

    def send(self):
        for d in range(1, self.n):
            self.copy(d, self.me).start()

    def take(self):
        for d in range(1, self.n):
            self.copy(d, lax.rem(self.me + self.n - d, self.n)).wait_recv()

    def drain(self):
        for d in range(1, self.n):
            self.copy(d, self.me).wait_send()


def normed(rows, gain):
    center = jnp.mean(rows, -1, keepdims=True)
    away = rows - center
    spread = jnp.mean(away * away, -1, keepdims=True)
    return away * lax.rsqrt(spread + EPS) * gain


def kernel(
    sizes,
    q1_ref, k1_ref, q2_ref, k2_ref, v_ref, og_ref, ig_ref, fg_ref, hg_ref, ow_ref,
    stream_ref, mg_ref, up_ref, down_ref, outg_ref,
    out_ref,
    up_all, down_all, st_send, e1, e2_send, e2, f_send, cin,
    rs_send, rs1, x_all, hidden, rs2_send, rs2, stream_own,
    local_sem, ysend, yrecv, zsend, zrecv, bsend, brecv,
    p1send, p1recv, p2send, p2recv, tsend, trecv,
):
    NZ, NY, TP = sizes
    iz, iy, it = lax.axis_index("z"), lax.axis_index("y"), lax.axis_index("tp")
    T, KA = q1_ref.shape
    KB = k2_ref.shape[1]
    DV = v_ref.shape[1] // 2
    KEYS = KA + KB
    SH = KEYS // NY
    OWN = T // TP
    D = ow_ref.shape[1]
    RW = up_ref.shape[0]
    FD = up_ref.shape[1]

    barrier = pltpu.get_barrier_semaphore()
    peers = 0
    for axis, n in (("y", NY), ("z", NZ), ("tp", TP)):
        for d in range(1, n):
            peer = lax.rem(lax.axis_index(axis) + d, n)
            pl.semaphore_signal(barrier, inc=1, device_id={axis: peer}, device_id_type=MESH)
            peers += 1

    up_copy = pltpu.make_async_copy(up_ref, up_all.at[iz, iy], local_sem.at[0])
    down_copy = pltpu.make_async_copy(down_ref, down_all.at[iz, iy], local_sem.at[1])
    stream_copy = pltpu.make_async_copy(
        stream_ref.at[pl.ds(pl.multiple_of(it * OWN, OWN), OWN), :], stream_own, local_sem.at[2]
    )
    up_copy.start()
    down_copy.start()
    stream_copy.start()

    row_i = lax.broadcasted_iota(jnp.int32, (T, T), 0)
    col_i = lax.broadcasted_iota(jnp.int32, (T, T), 1)
    upto = jnp.where(row_i <= col_i, 1.0, 0.0).astype(bf16)
    log_forget = -jnp.log1p(jnp.exp(-fg_ref[...]))
    ig = ig_ref[...]
    cum = left_dot(log_forget, upto, 1, 0)
    total = cum[:, T - 1 : T]
    weight_log = total - cum + ig
    peak = jnp.max(weight_log, axis=1, keepdims=True)
    weight = jnp.exp(weight_log - peak)
    turned = jnp.transpose(jnp.concatenate([cum, weight, cum, weight], axis=0))
    weighted1 = turned[:, 2:3] * (k1_ref[...].astype(f32) * (KA ** -0.5))
    weighted2 = turned[:, 3:4] * (k2_ref[...].astype(f32) * (KB ** -0.5))
    v1, v2 = v_ref[:, :DV], v_ref[:, DV:]
    state = jnp.concatenate(
        [left_dot(weighted1, v1, 0, 0), left_dot(weighted2, v2, 0, 0)], axis=0
    )
    n1 = jnp.sum(weighted1, axis=0, keepdims=True)
    n2 = jnp.sum(weighted2, axis=0, keepdims=True)
    n2 = jnp.concatenate([n2, jnp.zeros((1, KA - KB), f32)], axis=1)
    ones = jnp.ones((1, KA), f32)
    meta = jnp.concatenate(
        [n1, n2, total * ones, peak * ones, jnp.zeros((META - 6, KA), f32)], axis=0
    )
    for j in range(NY):
        st_send[j, :SH] = state[j * SH : (j + 1) * SH]
        st_send[j, SH:] = meta
    e1[pl.ds(iy, 1)] = st_send[pl.ds(iy, 1)]

    pl.semaphore_wait(barrier, peers)

    first_hop = Direct("y", NY, lambda j: st_send.at[j], lambda s: e1.at[s], ysend, yrecv)
    first_hop.send()

    rows = RW // 2
    up1 = Ring("y", NY, lambda b: up_all.at[iz, b],
               lambda b, h: up_all.at[iz, b, h * rows : (h + 1) * rows], p1send.at[0], p1recv.at[0])
    down1 = Ring("z", NZ, lambda b: down_all.at[b, iy],
                 lambda b, h: down_all.at[b, iy, h * rows : (h + 1) * rows], p1send.at[1], p1recv.at[1])
    hy, hz = max(NY // 2, 1), max(NZ // 2, 1)
    up2 = Ring("z", NZ, lambda b: up_all.at[b],
               lambda b, h: up_all.at[b, h * hy : (h + 1) * hy], p2send.at[0], p2recv.at[0])
    down2 = Ring("y", NY, lambda b: down_all.at[:, b],
                 lambda b, h: down_all.at[h * hz : (h + 1) * hz, b], p2send.at[1], p2recv.at[1])

    up_copy.wait()
    down_copy.wait()
    up1.send(1)
    down1.send(1)

    causal = row_i >= col_i
    local = []
    for h, (q_ref, k_ref, vh) in enumerate(((q1_ref, k1_ref, v1), (q2_ref, k2_ref, v2))):
        gaps = turned[:, h : h + 1] - cum[h : h + 1] + ig[h : h + 1]
        gaps = jnp.where(causal, gaps, -jnp.inf)
        top = jnp.max(gaps, axis=1, keepdims=True)
        scores = dg(q_ref[...], k_ref[...], 1, 1) * (k_ref.shape[1] ** -0.5)
        scores = scores * jnp.exp(gaps - top)
        local.append((top, left_dot(scores, vh, 1, 0), jnp.sum(scores, axis=1, keepdims=True)))

    up1.advance(2)
    down1.advance(2)

    key_row = lax.broadcasted_iota(jnp.int32, (SH, KA), 0) + iy * SH

    def spread(pair):
        return jnp.where(key_row < KA, pair[0:1], pair[1:2])

    def combine(early, late):
        decay_e, cell_e, norm_e, peak_e = early
        decay_l, cell_l, norm_l, peak_l = late
        moved = decay_l + peak_e
        ceiling = jnp.maximum(moved, peak_l)
        keep, fresh = jnp.exp(moved - ceiling), jnp.exp(peak_l - ceiling)
        return (
            decay_e + decay_l,
            spread(keep) * cell_e + spread(fresh) * cell_l,
            keep * norm_e + fresh * norm_l,
            ceiling,
        )

    def loaded(ref, j):
        return (ref[j, SH + 2 : SH + 4], ref[j, :SH], ref[j, SH : SH + 2], ref[j, SH + 4 : SH + 6])

    nothing = (
        jnp.zeros((2, KA), f32), jnp.zeros((SH, DV), f32), jnp.zeros((2, KA), f32),
        jnp.full((2, KA), NEG_BIG, f32),
    )
    first_hop.take()
    running, inside = nothing, []
    for j in range(NY):
        inside.append(running)
        running = combine(running, loaded(e1, j))
    e2_send[:SH] = running[1]
    e2_send[SH:] = jnp.concatenate(
        [running[2], running[0], running[3], jnp.zeros((META - 6, KA), f32)], axis=0
    )
    e2[pl.ds(iz, 1)] = e2_send[...][None]
    second_hop = Direct("z", NZ, lambda j: e2_send, lambda s: e2.at[s], zsend, zrecv)
    second_hop.send()
    up1.advance(3)
    down1.advance(3)
    up1.advance(4)
    down1.advance(4)
    second_hop.take()
    before = nothing
    for k in range(NZ):
        later = combine(before, loaded(e2, k))
        before = jax.tree.map(lambda new, old: jnp.where(k < iz, new, old), later, before)
    norm_in, peak_in = jnp.zeros((2, KA), f32), jnp.zeros((2, KA), f32)
    for j in range(NY):
        _, cell_j, norm_j, peak_j = combine(before, inside[j])
        f_send[j] = cell_j
        norm_in = jnp.where(iy == j, norm_j, norm_in)
        peak_in = jnp.where(iy == j, peak_j, peak_in)
    cin[pl.ds(iy, 1)] = f_send[pl.ds(iy, 1)]
    third_hop = Direct("y", NY, lambda j: f_send.at[j], lambda s: cin.at[s], bsend, brecv)
    third_hop.send()
    up1.take(up1.steps)
    down1.take(down1.steps)
    up2.send(1)
    down2.send(1)
    third_hop.take()

    cell_in = cin[...].reshape(KEYS, DV)
    columns = []
    for h, (q_ref, cell) in enumerate(((q1_ref, cell_in[:KA]), (q2_ref, cell_in[KA:]))):
        q = q_ref[...]
        width = q.shape[1]
        top, own_num, own_den = local[h]
        carried = turned[:, h : h + 1] + peak_in[h : h + 1, 0:1]
        ceiling = jnp.maximum(carried, top)
        keep, fresh = jnp.exp(carried - ceiling), jnp.exp(top - ceiling)
        num = keep * right_dot(q, cell, 1, 0) + fresh * own_num
        den = keep * jnp.sum(q.astype(f32) * norm_in[h : h + 1, :width], axis=1, keepdims=True)
        den = den + fresh * own_den
        cell_out = num / jnp.maximum(jnp.abs(den), jnp.exp(-ceiling))
        center = jnp.mean(cell_out, -1, keepdims=True)
        away = cell_out - center
        var = jnp.mean(away * away, -1, keepdims=True)
        columns.append(away * lax.rsqrt(var + EPS))
    gate = 1.0 / (1.0 + jnp.exp(-og_ref[...].astype(f32)))
    mixed = (jnp.concatenate(columns, axis=1) * hg_ref[...] * gate).astype(bf16)
    wide = min(D, 512)
    for c in range(0, D, wide):
        part = dg(mixed, ow_ref[:, c : c + wide], 1, 0).astype(bf16)
        rs_send[:, :, c : c + wide] = part.reshape(TP, OWN, wide)
    rs1[pl.ds(it, 1)] = rs_send[pl.ds(it, 1)]
    out_proj = Direct("tp", TP, lambda j: rs_send.at[j], lambda s: rs1.at[s], tsend.at[0], trecv.at[0])
    out_proj.send()
    up2.advance(2)
    down2.advance(2)
    stream_copy.wait()
    out_proj.take()
    mixer = jnp.sum(rs1[...].astype(f32), axis=0).astype(bf16).astype(f32)
    first = normed(stream_own[...].astype(f32) + mixer, mg_ref[...]).astype(bf16)
    x_all[pl.ds(it, 1)] = first[None]
    rows_out = Direct("tp", TP, lambda j: x_all.at[it], lambda s: x_all.at[s], tsend.at[1], trecv.at[1])
    rows_out.send()
    up2.advance(3)
    down2.advance(3)
    rows_out.take()
    up2.advance(4)
    down2.advance(4)
    up2.take(up2.steps)

    wide_f = min(FD, 256)
    for c in range(0, FD, wide_f):
        x = x_all[...].reshape(T, D)
        w = up_all[:, :, :, c : c + wide_f].reshape(D, wide_f)
        act = jnp.maximum(dg(x, w, 1, 0), 0.0)
        hidden[:, c : c + wide_f] = (act * act).astype(bf16)
    down2.take(down2.steps)
    wide_d = NY * RW
    for z in range(NZ):
        w = down_all[z].reshape(wide_d, FD)
        part = dg(hidden[...], w, 1, 1).astype(bf16)
        rs2_send[:, :, z * wide_d : (z + 1) * wide_d] = part.reshape(TP, OWN, wide_d)
    rs2[pl.ds(it, 1)] = rs2_send[pl.ds(it, 1)]
    mlp = Direct("tp", TP, lambda j: rs2_send.at[j], lambda s: rs2.at[s], tsend.at[2], trecv.at[2])
    mlp.send()
    for item in (first_hop, second_hop, third_hop, out_proj, rows_out, up1, down1, up2, down2):
        item.drain()
    mlp.take()
    mlp_out = jnp.sum(rs2[...].astype(f32), axis=0).astype(bf16).astype(f32)
    base = x_all[pl.ds(it, 1)].reshape(OWN, D).astype(f32)
    out_ref[...] = normed(base + mlp_out, outg_ref[...]).astype(bf16)
    mlp.drain()


def layer(
    sizes, query_one, key_one, query_two, key_two, values, out_gate, in_gate, forget_gate,
    head_gain, out_weight, stream, mix_gain, up_weight, down_weight, out_gain,
):
    NZ, NY, TP = sizes
    T, D = stream.shape
    OWN = T // TP
    RW, FD = up_weight.shape
    SH = (query_one.shape[1] + query_two.shape[1]) // NY
    KA = query_one.shape[1]
    sem = pltpu.SemaphoreType.DMA
    half = max(NY, NZ) // 2
    vmem, hbm = pl.BlockSpec(memory_space=pltpu.VMEM), pl.BlockSpec(memory_space=pl.ANY)
    return pl.pallas_call(
        functools.partial(kernel, sizes),
        out_shape=jax.ShapeDtypeStruct((OWN, D), bf16),
        in_specs=[vmem] * 10 + [hbm, vmem, hbm, hbm, vmem],
        out_specs=vmem,
        scratch_shapes=[
            pltpu.VMEM((NZ, NY, RW, FD), bf16),
            pltpu.VMEM((NZ, NY, RW, FD), bf16),
            pltpu.VMEM((NY, SH + META, KA), f32),
            pltpu.VMEM((NY, SH + META, KA), f32),
            pltpu.VMEM((SH + META, KA), f32),
            pltpu.VMEM((NZ, SH + META, KA), f32),
            pltpu.VMEM((NY, SH, KA), f32),
            pltpu.VMEM((NY, SH, KA), f32),
            pltpu.VMEM((TP, OWN, D), bf16),
            pltpu.VMEM((TP, OWN, D), bf16),
            pltpu.VMEM((TP, OWN, D), bf16),
            pltpu.VMEM((T, FD), bf16),
            pltpu.VMEM((TP, OWN, D), bf16),
            pltpu.VMEM((TP, OWN, D), bf16),
            pltpu.VMEM((OWN, D), bf16),
            sem((3,)),
            sem((NY,)), sem((NY,)), sem((NZ,)), sem((NZ,)), sem((NY,)), sem((NY,)),
            sem((2, 2, half)), sem((2, 2, half)), sem((2, 2, half)), sem((2, 2, half)),
            sem((3, TP)), sem((3, TP)),
        ],
        compiler_params=pltpu.CompilerParams(
            collective_id=0, has_side_effects=True, vmem_limit_bytes=40 * 1024 * 1024
        ),
    )(
        query_one, key_one, query_two, key_two, values, out_gate, in_gate, forget_gate,
        head_gain.reshape(1, -1), out_weight, stream, mix_gain.reshape(1, -1), up_weight,
        down_weight.T, out_gain.reshape(1, -1),
    )


def build(mesh, nz, ny):
    tp = mesh.shape["tp"]
    split = Mesh(mesh.devices.reshape(nz, ny, tp), ("z", "y", "tp"))
    SP = ("z", "y")
    return jax.shard_map(
        functools.partial(layer, (nz, ny, tp)),
        mesh=split,
        in_specs=(
            P(SP, "tp"), P(SP, "tp"), P(SP, "tp"), P(SP, "tp"), P(SP, "tp"), P(SP, "tp"),
            P("tp", SP), P("tp", SP), P("tp"), P("tp", None), P(SP, None), P(),
            P(SP, "tp"), P("tp", SP), P(),
        ),
        out_specs=P(("z", "y", "tp"), None),
        check_vma=False,
    )


def solution(mesh):
    return build(mesh, 8, 8)
```

```python
import contextlib
import functools

import jax
import jax.numpy as jnp
from jax import lax
from jax.experimental import pallas as pl
from jax.experimental.pallas import tpu as pltpu
from jax.sharding import Mesh
from jax.sharding import PartitionSpec as P

NEG_BIG = -1e30
EPS = 1e-05
META = 8
f32, bf16 = jnp.float32, jnp.bfloat16
MESH = pl.DeviceIdType.MESH
scope = contextlib.nullcontext


def dg(a, b, ca, cb):
    return lax.dot_general(a, b, (((ca,), (cb,)), ((), ())), preferred_element_type=f32)


def three(a):
    hi = a.astype(bf16)
    rest = a - hi.astype(f32)
    mid = rest.astype(bf16)
    return hi, mid, (rest - mid.astype(f32)).astype(bf16)


def left_dot(a, b, ca, cb):
    hi, mid, lo = three(a)
    return dg(hi, b, ca, cb) + (dg(mid, b, ca, cb) + dg(lo, b, ca, cb))


def right_dot(a, b, ca, cb):
    hi, mid, lo = three(b)
    return dg(a, hi, ca, cb) + (dg(a, mid, ca, cb) + dg(a, lo, ca, cb))


def remote(src, dst, ssem, rsem, target):
    return pltpu.make_async_remote_copy(
        src_ref=src, dst_ref=dst, send_sem=ssem, recv_sem=rsem, device_id=target, device_id_type=MESH
    )


class Ring:
    def __init__(self, axis, n, block, half, ssem, rsem):
        self.axis, self.n, self.block, self.half = axis, n, block, half
        self.ssem, self.rsem = ssem, rsem
        self.me = lax.axis_index(axis)
        self.steps = n // 2
        self.taken = set()

    def part(self, way, step, distance):
        away = self.n - distance if way == 0 else distance
        index = lax.rem(self.me + away, self.n)
        return self.block(index) if step < self.steps else self.half(index, way)

    def copy(self, way, step, distance):
        ref = self.part(way, step, distance)
        target = lax.rem(self.me + (1 if way == 0 else self.n - 1), self.n)
        return remote(
            ref, ref, self.ssem.at[way, step - 1], self.rsem.at[way, step - 1], {self.axis: target}
        )

    def send(self, step):
        if step <= self.steps:
            for way in (0, 1):
                self.copy(way, step, step - 1).start()

    def take(self, step):
        if 1 <= step <= self.steps and step not in self.taken:
            self.taken.add(step)
            for way in (0, 1):
                self.copy(way, step, step).wait_recv()

    def advance(self, step):
        self.take(step - 1)
        self.send(step)

    def drain(self):
        for step in range(1, self.steps + 1):
            for way in (0, 1):
                self.copy(way, step, step - 1).wait_send()


class Direct:
    def __init__(self, axis, n, source, slots, ssem, rsem):
        self.axis, self.n, self.source, self.slots = axis, n, source, slots
        self.ssem, self.rsem = ssem, rsem
        self.me = lax.axis_index(axis)

    def copy(self, d, slot):
        peer = lax.rem(self.me + d, self.n)
        return remote(
            self.source(peer), self.slots(slot), self.ssem.at[d], self.rsem.at[d], {self.axis: peer}
        )

    def send(self):
        for d in range(1, self.n):
            self.copy(d, self.me).start()

    def take(self):
        for d in range(1, self.n):
            self.copy(d, lax.rem(self.me + self.n - d, self.n)).wait_recv()

    def drain(self):
        for d in range(1, self.n):
            self.copy(d, self.me).wait_send()


class Wide:
    def __init__(self, first, axis, n, shard, pair, piece_sems, pair_sems):
        self.first, self.axis, self.n, self.shard, self.pair = first, axis, n, shard, pair
        self.piece_sems, self.pair_sems = piece_sems, pair_sems
        self.me = lax.axis_index(axis)
        self.steps = n // 2
        self.pairs = first.n // 2
        self.waited, self.sent = set(), []

    def source(self, way, distance):
        return lax.rem(self.me + (self.n - distance if way == 0 else distance), self.n)

    def target(self, way):
        return {self.axis: lax.rem(self.me + (1 if way == 0 else self.n - 1), self.n)}

    def piece(self, way, r, distance):
        ref = self.shard(lax.rem(self.first.me + r, self.first.n), self.source(way, distance))
        ssem, rsem = self.piece_sems
        return remote(ref, ref, ssem.at[way, r], rsem.at[way, r], self.target(way))

    def group(self, way, step, k, distance):
        q = lax.rem(lax.div(self.first.me, 2) + k, self.pairs)
        ref = self.pair(2 * q, self.source(way, distance))
        ssem, rsem = self.pair_sems
        return remote(ref, ref, ssem.at[way, step - 2, k], rsem.at[way, step - 2, k], self.target(way))

    def goes(self, way, step, index, count):
        if step < self.steps:
            return True
        return step == self.steps and (index < (count + 1) // 2) == (way == 0)

    def send_piece(self, r):
        for way in (0, 1):
            if self.goes(way, 1, r, self.first.n):
                copy = self.piece(way, r, 0)
                copy.start()
                self.sent.append(copy)

    def start(self):
        self.first.send(1)
        self.send_piece(0)

    def advance(self, step):
        if step <= self.first.steps:
            self.first.take(step)
            self.first.send(step + 1)
            for r in sorted({step, self.first.n - step}):
                self.send_piece(r)

    def take(self, step, k):
        if not 1 <= step <= self.steps or k >= self.pairs:
            return
        if step == 1:
            need = [("piece", r) for r in sorted({(2 * k + e) % self.first.n for e in (-1, 0, 1)})]
        else:
            need = [("pair", k)]
        for kind, i in need:
            if (kind, step, i) in self.waited:
                continue
            self.waited.add((kind, step, i))
            for way in (0, 1):
                if self.goes(way, step, i, self.first.n if kind == "piece" else self.pairs):
                    copy = self.piece(way, i, 1) if kind == "piece" else self.group(way, step, i, step)
                    copy.wait_recv()

    def forward(self, step, k):
        if step > self.steps or k >= self.pairs:
            return
        self.take(step - 1, k)
        for way in (0, 1):
            if self.goes(way, step, k, self.pairs):
                copy = self.group(way, step, k, step - 1)
                copy.start()
                self.sent.append(copy)

    def finish(self):
        for step in range(1, self.steps + 1):
            for k in range(self.pairs):
                self.take(step, k)

    def drain(self):
        self.first.drain()
        for copy in self.sent:
            copy.wait_send()


class TpSum:
    def __init__(self, chips, source, pair, chip_send, chip_recv, ssem, rsem):
        self.chips, self.source, self.pair = chips, source, pair
        self.chip_send, self.chip_recv, self.ssem, self.rsem = chip_send, chip_recv, ssem, rsem
        it = lax.axis_index("tp")
        self.chip, self.core = lax.div(it, 2), lax.rem(it, 2)

    def inner(self):
        other = 1 - self.core
        return remote(self.source.at[:, other], self.pair, self.ssem.at[0], self.rsem.at[0],
                      {"tp": self.chip * 2 + other})

    def outer(self, d, slot):
        peer = lax.rem(self.chip + d, self.chips)
        return remote(self.chip_send.at[peer], self.chip_recv.at[slot], self.ssem.at[d], self.rsem.at[d],
                      {"tp": peer * 2 + self.core})

    def start(self):
        self.inner().start()

    def between(self):
        self.inner().wait_recv()
        mine = self.source[:, pl.ds(self.core, 1)].astype(f32)
        both = mine.reshape(self.pair.shape) + self.pair[...].astype(f32)
        self.chip_send[...] = both.astype(bf16)
        for d in range(1, self.chips):
            self.outer(d, self.chip).start()
        self.chip_recv[pl.ds(self.chip, 1)] = self.chip_send[pl.ds(self.chip, 1)]

    def total(self):
        for d in range(1, self.chips):
            self.outer(d, lax.rem(self.chip + self.chips - d, self.chips)).wait_recv()
        return jnp.sum(self.chip_recv[...].astype(f32), axis=0)

    def drain(self):
        self.inner().wait_send()
        for d in range(1, self.chips):
            self.outer(d, self.chip).wait_send()


class TpGather:
    def __init__(self, chips, slots, ssem, rsem, psend, precv):
        self.chips, self.slots = chips, slots
        self.ssem, self.rsem, self.psend, self.precv = ssem, rsem, psend, precv
        it = lax.axis_index("tp")
        self.chip, self.core = lax.div(it, 2), lax.rem(it, 2)

    def outer(self, d, chip):
        ref = self.slots.at[chip, self.core]
        peer = lax.rem(self.chip + d, self.chips)
        return remote(ref, ref, self.ssem.at[d], self.rsem.at[d], {"tp": peer * 2 + self.core})

    def inner(self, d, core):
        ref = self.slots.at[lax.rem(self.chip + self.chips - d, self.chips), core]
        return remote(ref, ref, self.psend.at[d], self.precv.at[d], {"tp": self.chip * 2 + 1 - self.core})

    def start(self):
        for d in range(1, self.chips):
            self.outer(d, self.chip).start()
        self.inner(0, self.core).start()

    def relay(self):
        for d in sorted(range(1, self.chips), key=lambda d: min(d, self.chips - d)):
            self.outer(d, lax.rem(self.chip + self.chips - d, self.chips)).wait_recv()
            self.inner(d, self.core).start()

    def take(self):
        for d in range(self.chips):
            self.inner(d, 1 - self.core).wait_recv()

    def drain(self):
        for d in range(1, self.chips):
            self.outer(d, self.chip).wait_send()
        for d in range(self.chips):
            self.inner(d, self.core).wait_send()


def normed(rows, gain):
    center = jnp.mean(rows, -1, keepdims=True)
    away = rows - center
    spread = jnp.mean(away * away, -1, keepdims=True)
    return away * lax.rsqrt(spread + EPS) * gain


def kernel(
    sizes,
    q1_hbm, k1_hbm, q2_hbm, k2_hbm, v_hbm, og_hbm, ig_hbm, fg_hbm, hg_hbm, ow_hbm,
    stream_ref, mg_hbm, up_ref, down_ref, outg_hbm,
    out_ref,
    q1_ref, k1_ref, q2_ref, k2_ref, v_ref, og_ref, ig_ref, fg_ref, hg_ref, ow_ref, mg_ref, outg_ref,
    up_all, down_all, st_send, e1, e2_send, e2, f_send, cin,
    parts, pair, chip_send, chip_recv, x_all, hidden, parts2, pair2, chip_send2, chip_recv2, stream_own,
    local_sem, ysend, yrecv, zsend, zrecv, bsend, brecv,
    p1send, p1recv, p2send, p2recv, p3send, p3recv, tsend, trecv,
):
    NZ, NY, TP = sizes
    X = TP // 2
    iz, iy, it = lax.axis_index("z"), lax.axis_index("y"), lax.axis_index("tp")
    chip, core = lax.div(it, 2), lax.rem(it, 2)
    T, KA = q1_ref.shape
    KB = k2_ref.shape[0]
    DV = v_ref.shape[1] // 2
    KEYS = KA + KB
    SH = KEYS // NY
    OWN = T // TP
    D = ow_ref.shape[1]
    RW, FD = up_ref.shape

    barrier = pltpu.get_barrier_semaphore()
    peers = 0
    greeted = [{axis: lax.rem(lax.axis_index(axis) + d, n)} for axis, n in (("y", NY), ("z", NZ)) for d in range(1, n)]
    greeted += [{"tp": lax.rem(chip + d, X) * 2 + core} for d in range(1, X)] + [{"tp": chip * 2 + 1 - core}]
    for peer in greeted:
        pl.semaphore_signal(barrier, inc=1, device_id=peer, device_id_type=MESH)

    loads = []
    for src, dst in (
        (fg_hbm, fg_ref), (ig_hbm, ig_ref), (k1_hbm, k1_ref), (k2_hbm, k2_ref), (v_hbm, v_ref),
        (up_ref, up_all.at[iz, iy]), (down_ref, down_all.at[iz, iy]),
        (q1_hbm, q1_ref), (q2_hbm, q2_ref), (og_hbm, og_ref), (hg_hbm, hg_ref), (ow_hbm, ow_ref),
        (stream_ref.at[pl.ds(pl.multiple_of(it * OWN, OWN), OWN), :], stream_own),
        (mg_hbm, mg_ref), (outg_hbm, outg_ref),
    ):
        copy = pltpu.make_async_copy(src, dst, local_sem.at[len(loads)])
        copy.start()
        loads.append(copy)

    with scope("local"):
        row_i = lax.broadcasted_iota(jnp.int32, (T, T), 0)
        col_i = lax.broadcasted_iota(jnp.int32, (T, T), 1)
        upto = jnp.where(row_i <= col_i, 1.0, 0.0).astype(bf16)
        for i in range(5):
            loads[i].wait()
        log_forget = -jnp.log1p(jnp.exp(-fg_ref[...]))
        ig = ig_ref[...]
        cum = left_dot(log_forget, upto, 1, 0)
        total = cum[:, T - 1 : T]
        weight_log = total - cum + ig
        peak = jnp.max(weight_log, axis=1, keepdims=True)
        weight = jnp.exp(weight_log - peak)
        scaled1, scaled2 = weight[0:1] * (KA ** -0.5), weight[1:2] * (KB ** -0.5)
        v1, v2 = v_ref[:, :DV], v_ref[:, DV:]
        k1, k2 = k1_ref[...], k2_ref[...]
        state = jnp.concatenate(
            [
                left_dot(jnp.transpose(k1.astype(f32)) * scaled1, v1, 1, 0),
                left_dot(k2.astype(f32) * scaled2, v2, 1, 0),
            ],
            axis=0,
        )
        n1 = left_dot(scaled1, k1, 1, 0)
        n2 = left_dot(scaled2, k2, 1, 1)
        n2 = jnp.concatenate([n2, jnp.zeros((1, KA - KB), f32)], axis=1)
        ones = jnp.ones((1, KA), f32)
        meta = jnp.concatenate(
            [n1, n2, total * ones, peak * ones, jnp.zeros((META - 6, KA), f32)], axis=0
        )
        for j in range(NY):
            st_send[j, :SH] = state[j * SH : (j + 1) * SH]
            st_send[j, SH:] = meta
        e1[pl.ds(iy, 1)] = st_send[pl.ds(iy, 1)]

    with scope("barrier"):
        pl.semaphore_wait(barrier, len(greeted))

    first_hop = Direct("y", NY, lambda j: st_send.at[j], lambda s: e1.at[s], ysend, yrecv)
    first_hop.send()

    rows = RW // 2
    up1 = Ring("y", NY, lambda b: up_all.at[iz, b],
               lambda b, h: up_all.at[iz, b, h * rows : (h + 1) * rows], p1send.at[0], p1recv.at[0])
    down1 = Ring("z", NZ, lambda b: down_all.at[b, iy],
                 lambda b, h: down_all.at[b, iy, h * rows : (h + 1) * rows], p1send.at[1], p1recv.at[1])
    up2 = Wide(up1, "z", NZ, lambda b, z: up_all.at[z, b], lambda b, z: up_all.at[z, pl.ds(b, 2)],
               (p2send.at[0], p2recv.at[0]), (p3send.at[0], p3recv.at[0]))
    down2 = Wide(down1, "y", NY, lambda b, y: down_all.at[b, y], lambda b, y: down_all.at[pl.ds(b, 2), y],
                 (p2send.at[1], p2recv.at[1]), (p3send.at[1], p3recv.at[1]))

    def advance(step):
        up2.advance(step)
        down2.advance(step)

    def forward(step, *ks):
        for k in ks:
            up2.forward(step, k)
            down2.forward(step, k)

    loads[5].wait()
    loads[6].wait()
    up2.start()
    down2.start()

    with scope("scores"):
        turned = jnp.transpose(jnp.concatenate([cum, cum, cum, cum], axis=0))
        causal = row_i >= col_i
        loads[7].wait()
        loads[8].wait()
        q1, q2 = q1_ref[...], jnp.transpose(q2_ref[...].astype(f32)).astype(bf16)
        local = []
        for h, (q, k, over, width, vh) in enumerate(((q1, k1, 1, KA, v1), (q2, k2, 0, KB, v2))):
            gaps = turned[:, h : h + 1] - cum[h : h + 1] + ig[h : h + 1]
            gaps = jnp.where(causal, gaps, -jnp.inf)
            top = jnp.max(gaps, axis=1, keepdims=True)
            scores = dg(q, k, 1, over) * (width ** -0.5)
            scores = scores * jnp.exp(gaps - top)
            local.append((top, left_dot(scores, vh, 1, 0), jnp.sum(scores, axis=1, keepdims=True)))

    with scope("adv12"):
        advance(1)
        advance(2)

    key_row = lax.broadcasted_iota(jnp.int32, (SH, KA), 0) + iy * SH

    def spread(both):
        return jnp.where(key_row < KA, both[0:1], both[1:2])

    def combine(early, late):
        decay_e, cell_e, norm_e, peak_e = early
        decay_l, cell_l, norm_l, peak_l = late
        moved = decay_l + peak_e
        ceiling = jnp.maximum(moved, peak_l)
        keep, fresh = jnp.exp(moved - ceiling), jnp.exp(peak_l - ceiling)
        return (
            decay_e + decay_l,
            spread(keep) * cell_e + spread(fresh) * cell_l,
            keep * norm_e + fresh * norm_l,
            ceiling,
        )

    def loaded(ref, j):
        return (ref[j, SH + 2 : SH + 4], ref[j, :SH], ref[j, SH : SH + 2], ref[j, SH + 4 : SH + 6])

    nothing = (
        jnp.zeros((2, KA), f32), jnp.zeros((SH, DV), f32), jnp.zeros((2, KA), f32),
        jnp.full((2, KA), NEG_BIG, f32),
    )
    with scope("e1take"):
        first_hop.take()
    with scope("e1comb"):
        running, inside = nothing, []
        for j in range(NY):
            inside.append(running)
            running = combine(running, loaded(e1, j))
        e2_send[:SH] = running[1]
        e2_send[SH:] = jnp.concatenate(
            [running[2], running[0], running[3], jnp.zeros((META - 6, KA), f32)], axis=0
        )
        e2[pl.ds(iz, 1)] = e2_send[...][None]
    second_hop = Direct("z", NZ, lambda j: e2_send, lambda s: e2.at[s], zsend, zrecv)
    second_hop.send()
    with scope("adv34"):
        advance(3)
        advance(4)
    with scope("e2take"):
        second_hop.take()
    with scope("e2comb"):
        before = nothing
        for k in range(NZ):
            later = combine(before, loaded(e2, k))
            before = jax.tree.map(lambda new, old: jnp.where(k < iz, new, old), later, before)
        norm_in, peak_in = jnp.zeros((2, KA), f32), jnp.zeros((2, KA), f32)
        for j in range(NY):
            _, cell_j, norm_j, peak_j = combine(before, inside[j])
            f_send[j] = cell_j
            norm_in = jnp.where(iy == j, norm_j, norm_in)
            peak_in = jnp.where(iy == j, peak_j, peak_in)
        cin[pl.ds(iy, 1)] = f_send[pl.ds(iy, 1)]
    third_hop = Direct("y", NY, lambda j: f_send.at[j], lambda s: cin.at[s], bsend, brecv)
    third_hop.send()
    with scope("fwd2a"):
        forward(2, 0, 1, 3)
    with scope("e3take"):
        third_hop.take()

    with scope("cell"):
        for i in range(9, 15):
            loads[i].wait()
        cell_in = cin[...].reshape(KEYS, DV)
        columns = []
        for h, (q, width, cell) in enumerate(((q1, KA, cell_in[:KA]), (q2, KB, cell_in[KA:]))):
            top, own_num, own_den = local[h]
            carried = turned[:, h : h + 1] + peak_in[h : h + 1, 0:1]
            ceiling = jnp.maximum(carried, top)
            keep, fresh = jnp.exp(carried - ceiling), jnp.exp(top - ceiling)
            num = keep * right_dot(q, cell, 1, 0) + fresh * own_num
            den = keep * jnp.sum(q.astype(f32) * norm_in[h : h + 1, :width], axis=1, keepdims=True)
            den = den + fresh * own_den
            cell_out = num / jnp.maximum(jnp.abs(den), jnp.exp(-ceiling))
            center = jnp.mean(cell_out, -1, keepdims=True)
            away = cell_out - center
            var = jnp.mean(away * away, -1, keepdims=True)
            columns.append(away * lax.rsqrt(var + EPS))
        gate = 1.0 / (1.0 + jnp.exp(-og_ref[...].astype(f32)))
        mixed = (jnp.concatenate(columns, axis=1) * hg_ref[...] * gate).astype(bf16)
        wide = min(D, 512)
        for c in range(0, D, wide):
            part = dg(mixed, ow_ref[:, c : c + wide], 1, 0).astype(bf16)
            parts[:, :, :, c : c + wide] = part.reshape(X, 2, OWN, wide)
    out_proj = TpSum(X, parts, pair, chip_send, chip_recv, tsend.at[0], trecv.at[0])
    out_proj.start()
    with scope("fwd2b"):
        forward(2, 2)
    with scope("rs1mid"):
        out_proj.between()
    with scope("fwd3a"):
        forward(3, 0, 1)
    with scope("rs1take"):
        mixer = out_proj.total().astype(bf16).astype(f32)
    with scope("norm1"):
        first = normed(stream_own[...].astype(f32) + mixer, mg_ref[...]).astype(bf16)
        x_all[pl.ds(chip, 1), pl.ds(core, 1)] = first[None, None]
    rows_out = TpGather(X, x_all, tsend.at[1], trecv.at[1], tsend.at[2], trecv.at[2])
    rows_out.start()
    with scope("fwd3b"):
        forward(3, 3, 2)
    with scope("agrelay"):
        rows_out.relay()
    with scope("fwd4"):
        forward(4, 0, 1, 3, 2)
    with scope("agtake"):
        rows_out.take()
    with scope("upwait"):
        up2.finish()

    with scope("mlp1"):
        wide_f = min(FD, 256)
        for c in range(0, FD, wide_f):
            x = x_all[...].reshape(T, D)
            w = up_all[:, :, :, c : c + wide_f].reshape(D, wide_f)
            act = jnp.maximum(dg(x, w, 1, 0), 0.0)
            hidden[:, c : c + wide_f] = (act * act).astype(bf16)
    with scope("downwait"):
        down2.finish()
    with scope("mlp2"):
        wide_d = NY * RW
        for z in range(NZ):
            w = down_all[z].reshape(wide_d, FD)
            part = dg(hidden[...], w, 1, 1).astype(bf16)
            parts2[:, :, :, z * wide_d : (z + 1) * wide_d] = part.reshape(X, 2, OWN, wide_d)
    mlp = TpSum(X, parts2, pair2, chip_send2, chip_recv2, tsend.at[3], trecv.at[3])
    mlp.start()
    with scope("drain"):
        for item in (first_hop, second_hop, third_hop, out_proj, rows_out, up2, down2):
            item.drain()
    with scope("rs2mid"):
        mlp.between()
    with scope("rs2take"):
        mlp_out = mlp.total().astype(bf16).astype(f32)
    with scope("norm2"):
        base = x_all[pl.ds(chip, 1), pl.ds(core, 1)].reshape(OWN, D).astype(f32)
        out_ref[...] = normed(base + mlp_out, outg_ref[...]).astype(bf16)
    mlp.drain()


def layer(
    sizes, query_one, key_one, query_two, key_two, values, out_gate, in_gate, forget_gate,
    head_gain, out_weight, stream, mix_gain, up_weight, down_weight, out_gain,
):
    NZ, NY, TP = sizes
    X = TP // 2
    T, D = stream.shape
    OWN = T // TP
    RW, FD = up_weight.shape
    SH = (query_one.shape[1] + query_two.shape[1]) // NY
    KA = query_one.shape[1]
    sem = pltpu.SemaphoreType.DMA
    half = max(NY, NZ) // 2
    operands = (
        query_one, key_one, query_two.T, key_two.T, values, out_gate, in_gate, forget_gate,
        head_gain.reshape(1, -1), out_weight, stream, mix_gain.reshape(1, -1), up_weight,
        down_weight.T, out_gain.reshape(1, -1),
    )
    copied = [operands[i] for i in (0, 1, 2, 3, 4, 5, 6, 7, 8, 9, 11, 14)]
    exchange = [
        pltpu.VMEM((X, 2, OWN, D), bf16),
        pltpu.VMEM((X, OWN, D), bf16),
        pltpu.VMEM((X, OWN, D), bf16),
        pltpu.VMEM((X, OWN, D), bf16),
    ]
    return pl.pallas_call(
        functools.partial(kernel, sizes),
        out_shape=jax.ShapeDtypeStruct((OWN, D), bf16),
        in_specs=[pl.BlockSpec(memory_space=pl.ANY)] * len(operands),
        out_specs=pl.BlockSpec(memory_space=pltpu.VMEM),
        scratch_shapes=[pltpu.VMEM(a.shape, a.dtype) for a in copied]
        + [
            pltpu.VMEM((NZ, NY, RW, FD), bf16),
            pltpu.VMEM((NZ, NY, RW, FD), bf16),
            pltpu.VMEM((NY, SH + META, KA), f32),
            pltpu.VMEM((NY, SH + META, KA), f32),
            pltpu.VMEM((SH + META, KA), f32),
            pltpu.VMEM((NZ, SH + META, KA), f32),
            pltpu.VMEM((NY, SH, KA), f32),
            pltpu.VMEM((NY, SH, KA), f32),
        ]
        + exchange
        + [pltpu.VMEM((X, 2, OWN, D), bf16), pltpu.VMEM((T, FD), bf16)]
        + exchange
        + [
            pltpu.VMEM((OWN, D), bf16),
            sem((15,)),
            sem((NY,)), sem((NY,)), sem((NZ,)), sem((NZ,)), sem((NY,)), sem((NY,)),
            sem((2, 2, half)), sem((2, 2, half)),
            sem((2, 2, 2 * half)), sem((2, 2, 2 * half)),
            sem((2, 2, half, half)), sem((2, 2, half, half)),
            sem((4, X + 1)), sem((4, X + 1)),
        ],
        compiler_params=pltpu.CompilerParams(
            collective_id=0, has_side_effects=True, vmem_limit_bytes=60000 * 1024
        ),
    )(*operands)


def build(mesh, nz, ny):
    tp = mesh.shape["tp"]
    split = Mesh(mesh.devices.reshape(nz, ny, tp), ("z", "y", "tp"))
    SP = ("z", "y")
    return jax.shard_map(
        functools.partial(layer, (nz, ny, tp)),
        mesh=split,
        in_specs=(
            P(SP, "tp"), P(SP, "tp"), P(SP, "tp"), P(SP, "tp"), P(SP, "tp"), P(SP, "tp"),
            P("tp", SP), P("tp", SP), P("tp"), P("tp", None), P(SP, None), P(),
            P(SP, "tp"), P("tp", SP), P(),
        ),
        out_specs=P(("z", "y", "tp"), None),
        check_vma=False,
    )


def solution(mesh):
    return build(mesh, 8, 8)
```

```python
import contextlib
import functools
import itertools

import jax
import jax.numpy as jnp
from jax import lax
from jax.experimental import pallas as pl
from jax.experimental.pallas import tpu as pltpu
from jax.sharding import Mesh
from jax.sharding import PartitionSpec as P

NEG_BIG = -1e30
EPS = 1e-05
META = 8
f32, bf16 = jnp.float32, jnp.bfloat16
MESH = pl.DeviceIdType.MESH
LAG = 3
scope = contextlib.nullcontext


def dg(a, b, ca, cb):
    return lax.dot_general(a, b, (((ca,), (cb,)), ((), ())), preferred_element_type=f32)


def three(a):
    hi = a.astype(bf16)
    rest = a - hi.astype(f32)
    mid = rest.astype(bf16)
    return hi, mid, (rest - mid.astype(f32)).astype(bf16)


def left_dot(a, b, ca, cb):
    hi, mid, lo = three(a)
    return dg(hi, b, ca, cb) + (dg(mid, b, ca, cb) + dg(lo, b, ca, cb))


def right_dot(a, b, ca, cb):
    hi, mid, lo = three(b)
    return dg(a, hi, ca, cb) + (dg(a, mid, ca, cb) + dg(a, lo, ca, cb))


def remote(src, dst, ssem, rsem, target):
    return pltpu.make_async_remote_copy(
        src_ref=src, dst_ref=dst, send_sem=ssem, recv_sem=rsem, device_id=target, device_id_type=MESH
    )


class Gather:
    def __init__(self, axes, sizes, shard, spans, send_sems, first_recv, second_recv):
        self.axes, self.sizes, self.shard, self.spans = axes, sizes, shard, spans
        self.send_sems, self.first_recv, self.second_recv = send_sems, first_recv, second_recv
        self.me = [lax.axis_index(axis) for axis in axes]
        self.steps = [n // 2 for n in sizes]
        self.waited = set()

    def at(self, axis, offset):
        return lax.rem(self.me[axis] + offset % self.sizes[axis], self.sizes[axis])

    def away(self, axis, way, distance):
        return self.at(axis, -distance if way == 0 else distance)

    def target(self, axis, way):
        return {self.axes[axis]: self.at(axis, 1 if way == 0 else -1)}

    def first_ways(self, step):
        return (0, 1) if step < self.steps[0] else (1,)

    def second_ways(self, step, r):
        if step < self.steps[1]:
            return (0, 1)
        return (0,) if r < (self.sizes[0] + 1) // 2 else (1,)

    def ranked(self, rank):
        return sorted({rank, (self.sizes[0] - rank) % self.sizes[0]})

    def send_first(self, step):
        if step <= self.steps[0]:
            for way in self.first_ways(step):
                ref = self.shard(self.away(0, way, step - 1), self.me[1])
                remote(ref, ref, self.send_sems.at[0], self.first_recv.at[step - 1], self.target(0, way)).start()

    def take_first(self, step):
        if step <= self.steps[0] and step not in self.waited:
            self.waited.add(step)
            ref = self.spans[0](len(self.first_ways(step)))
            remote(ref, ref, self.send_sems.at[0], self.first_recv.at[step - 1], self.target(0, 0)).wait_recv()

    def send(self, step, rank):
        for r in self.ranked(rank):
            for way in self.second_ways(step, r):
                ref = self.shard(self.at(0, r), self.away(1, way, step - 1))
                remote(ref, ref, self.send_sems.at[1], self.second_recv.at[step - 1, rank],
                       self.target(1, way)).start()

    def take(self, step, rank):
        if (step, rank) not in self.waited:
            self.waited.add((step, rank))
            ref = self.spans[0](sum(len(self.second_ways(step, r)) for r in self.ranked(rank)))
            remote(ref, ref, self.send_sems.at[1], self.second_recv.at[step - 1, rank],
                   self.target(1, 0)).wait_recv()

    def stage(self, stage):
        def one():
            if stage:
                self.take_first(stage)
            self.send_first(stage + 1)

        def further(step, rank):
            if step > 1:
                self.take(step - 1, rank)
            self.send(step, rank)

        actions = [one]
        for step in range(1, self.steps[1] + 1):
            if 0 <= stage - step + 1 <= self.steps[0]:
                actions.append(functools.partial(further, step, stage - step + 1))
        return actions

    def finish(self):
        for step in range(1, self.steps[0] + 1):
            self.take_first(step)
        for step in range(1, self.steps[1] + 1):
            for rank in range(self.steps[0] + 1):
                self.take(step, rank)

    def near(self, axis, reach):
        for step in range(1, self.steps[0] + 1):
            if axis == 1 or step <= reach:
                self.take_first(step)
        for step in range(1, self.steps[1] + 1):
            for rank in range(self.steps[0] + 1):
                if (step if axis == 1 else rank) <= reach:
                    self.take(step, rank)

    def drain(self):
        for sem, ref in ((0, self.spans[1]), (1, self.spans[2])):
            remote(ref, ref, self.send_sems.at[sem], self.first_recv.at[0], self.target(0, 0)).wait_send()


class Direct:
    def __init__(self, axis, n, source, slots, span, sems):
        self.axis, self.n, self.source, self.slots, self.span, self.sems = axis, n, source, slots, span, sems
        self.me = lax.axis_index(axis)

    def send(self):
        for d in range(1, self.n):
            peer = lax.rem(self.me + d, self.n)
            remote(self.source(peer), self.slots.at[self.me], self.sems.at[0], self.sems.at[1],
                   {self.axis: peer}).start()

    def whole(self):
        return remote(self.span, self.span, self.sems.at[0], self.sems.at[1], {self.axis: lax.rem(self.me + 1, self.n)})

    def take(self):
        self.whole().wait_recv()

    def drain(self):
        self.whole().wait_send()


class TpSum:
    def __init__(self, chips, source, pair, chip_send, chip_recv, sems):
        self.chips, self.source, self.pair = chips, source, pair
        self.chip_send, self.chip_recv, self.sems = chip_send, chip_recv, sems
        it = lax.axis_index("tp")
        self.chip, self.core = lax.div(it, 2), lax.rem(it, 2)

    def inner(self):
        other = 1 - self.core
        return remote(self.source.at[:, other], self.pair, self.sems.at[0], self.sems.at[1],
                      {"tp": self.chip * 2 + other})

    def outer(self):
        ref = self.chip_recv.at[0 : self.chips - 1]
        peer = lax.rem(self.chip + 1, self.chips)
        return remote(ref, ref, self.sems.at[2], self.sems.at[3], {"tp": peer * 2 + self.core})

    def start(self):
        self.inner().start()

    def between(self):
        self.inner().wait_recv()
        mine = self.source[:, pl.ds(self.core, 1)].astype(f32)
        both = mine.reshape(self.pair.shape) + self.pair[...].astype(f32)
        self.chip_send[...] = both.astype(bf16)
        for d in range(1, self.chips):
            peer = lax.rem(self.chip + d, self.chips)
            remote(self.chip_send.at[peer], self.chip_recv.at[self.chip], self.sems.at[2], self.sems.at[3],
                   {"tp": peer * 2 + self.core}).start()
        self.chip_recv[pl.ds(self.chip, 1)] = self.chip_send[pl.ds(self.chip, 1)]

    def total(self):
        if self.chips > 1:
            self.outer().wait_recv()
        return jnp.sum(self.chip_recv[...].astype(f32), axis=0)

    def drain(self):
        self.inner().wait_send()
        if self.chips > 1:
            self.outer().wait_send()


class TpGather:
    def __init__(self, chips, slots, sems, chip_sems):
        self.chips, self.slots, self.sems, self.chip_sems = chips, slots, sems, chip_sems
        it = lax.axis_index("tp")
        self.chip, self.core = lax.div(it, 2), lax.rem(it, 2)

    def outer(self, d, ref):
        peer = lax.rem(self.chip + d, self.chips)
        return remote(ref, ref, self.sems.at[0], self.chip_sems.at[d], {"tp": peer * 2 + self.core})

    def inner(self, ref):
        return remote(ref, ref, self.sems.at[1], self.sems.at[2], {"tp": self.chip * 2 + 1 - self.core})

    def start(self):
        for d in range(1, self.chips):
            self.outer(d, self.slots.at[self.chip, self.core]).start()
        self.inner(self.slots.at[self.chip, self.core]).start()

    def relay(self):
        for d in sorted(range(1, self.chips), key=lambda d: min(d, self.chips - d)):
            ref = self.slots.at[lax.rem(self.chip + self.chips - d, self.chips), self.core]
            self.outer(d, ref).wait_recv()
            self.inner(ref).start()

    def take(self):
        self.inner(self.slots.at[:, 0]).wait_recv()

    def drain(self):
        if self.chips > 1:
            self.outer(1, self.slots.at[0 : self.chips - 1, 0]).wait_send()
        self.inner(self.slots.at[:, 0]).wait_send()


def normed(rows, gain):
    center = jnp.mean(rows, -1, keepdims=True)
    away = rows - center
    spread = jnp.mean(away * away, -1, keepdims=True)
    return away * lax.rsqrt(spread + EPS) * gain


def early_blocks(nz):
    return sum(min(s, nz - s) <= nz // 2 - 2 for s in range(nz))


def kernel(
    sizes,
    q1_hbm, k1_hbm, q2_hbm, k2_hbm, v_hbm, og_hbm, ig_hbm, fg_hbm, hg_hbm, ow_hbm,
    stream_ref, mg_hbm, up_ref, down_ref, outg_hbm,
    out_ref,
    q1_ref, k1_ref, q2_ref, k2_ref, v_ref, og_ref, ig_ref, fg_ref, hg_ref, ow_ref, mg_ref, outg_ref,
    up_all, down_all, st_send, e1, e2_send, e2, f_send, cin,
    parts, pair, chip_send, chip_recv, x_all, hidden, parts_a, pair_a, send_a, recv_a, parts_b, pair_b, send_b, recv_b, mlp_sum, stream_own,
    local_sem, hop, gsend, g1recv, g2recv, tsems, rowsems,
):
    NZ, NY, TP = sizes
    X = TP // 2
    iz, iy, it = lax.axis_index("z"), lax.axis_index("y"), lax.axis_index("tp")
    chip, core = lax.div(it, 2), lax.rem(it, 2)
    T, KA = q1_ref.shape
    KB = k2_ref.shape[0]
    DV = v_ref.shape[1] // 2
    KEYS = KA + KB
    SH = KEYS // NY
    OWN = T // TP
    D = ow_ref.shape[1]
    RW, FD = up_ref.shape

    barrier = pltpu.get_barrier_semaphore()
    peers = 0
    greeted = [{axis: lax.rem(lax.axis_index(axis) + d, n)} for axis, n in (("y", NY), ("z", NZ)) for d in range(1, n)]
    greeted += [{"tp": lax.rem(chip + d, X) * 2 + core} for d in range(1, X)] + [{"tp": chip * 2 + 1 - core}]
    for peer in greeted:
        pl.semaphore_signal(barrier, inc=1, device_id=peer, device_id_type=MESH)

    loads = []
    for src, dst in (
        (up_ref, up_all.at[iz, iy]), (down_ref, down_all.at[iz, iy]),
        (fg_hbm, fg_ref), (ig_hbm, ig_ref), (k1_hbm, k1_ref), (k2_hbm, k2_ref), (v_hbm, v_ref),
        (q1_hbm, q1_ref), (q2_hbm, q2_ref), (og_hbm, og_ref), (hg_hbm, hg_ref), (ow_hbm, ow_ref),
        (stream_ref.at[pl.ds(pl.multiple_of(it * OWN, OWN), OWN), :], stream_own),
        (mg_hbm, mg_ref), (outg_hbm, outg_ref),
    ):
        copy = pltpu.make_async_copy(src, dst, local_sem.at[len(loads)])
        copy.start()
        loads.append(copy)

    half = RW // 2

    def gather(weights, low, sems, first_recv, second_recv):
        part = slice(0, half) if low else slice(half, RW)
        if low:
            axes, sizes = ("y", "z"), (NY, NZ)
            shard = lambda a, b: weights.at[b, a, part]
            spans = (lambda n: weights.at[0, 0:n, part] if n <= NY else weights.at[0:2, 0 : n // 2, part],
                     weights.at[0, 0 : NY - 1, part], weights.at[0 : NZ - 1, :, part])
        else:
            axes, sizes = ("z", "y"), (NZ, NY)
            shard = lambda a, b: weights.at[a, b, part]
            spans = (lambda n: weights.at[0, 0:n, part] if n <= NY else weights.at[0:2, 0 : n // 2, part],
                     weights.at[0 : NZ - 1, 0, part], weights.at[:, 0 : NY - 1, part])
        return Gather(axes, sizes, shard, spans, sems, first_recv, second_recv)

    ups = [gather(up_all, i == 0, gsend.at[i], g1recv.at[i], g2recv.at[i]) for i in range(2)]
    downs = [gather(down_all, i == 0, gsend.at[2 + i], g1recv.at[2 + i], g2recv.at[2 + i]) for i in range(2)]

    def stage(number, part=None):
        late = number if number < 2 else number - LAG
        lists = [item.stage(number) for item in ups]
        if number < 2 or late >= 2:
            lists += [item.stage(late) for item in downs]
        rows = list(itertools.zip_longest(*lists))
        cut = (len(rows) + 1) // 2
        with scope(f"stage{number}{part}"):
            for row in rows[:cut] if part == 0 else rows[cut:] if part == 1 else rows:
                for action in row:
                    if action is not None:
                        action()

    loads[0].wait()
    loads[1].wait()
    with scope("barrier"):
        pl.semaphore_wait(barrier, len(greeted))
    stage(0)

    with scope("local"):
        row_i = lax.broadcasted_iota(jnp.int32, (T, T), 0)
        col_i = lax.broadcasted_iota(jnp.int32, (T, T), 1)
        upto = jnp.where(row_i <= col_i, 1.0, 0.0).astype(bf16)
        for i in range(2, 7):
            loads[i].wait()
        log_forget = -jnp.log1p(jnp.exp(-fg_ref[...]))
        ig = ig_ref[...]
        cum = left_dot(log_forget, upto, 1, 0)
        total = cum[:, T - 1 : T]
        weight_log = total - cum + ig
        peak = jnp.max(weight_log, axis=1, keepdims=True)
        weight = jnp.exp(weight_log - peak)
        scaled1, scaled2 = weight[0:1] * (KA ** -0.5), weight[1:2] * (KB ** -0.5)
        v1, v2 = v_ref[:, :DV], v_ref[:, DV:]
        k1, k2 = k1_ref[...], k2_ref[...]
        state = jnp.concatenate(
            [
                left_dot(jnp.transpose(k1.astype(f32)) * scaled1, v1, 1, 0),
                left_dot(k2.astype(f32) * scaled2, v2, 1, 0),
            ],
            axis=0,
        )
        n1 = left_dot(scaled1, k1, 1, 0)
        n2 = left_dot(scaled2, k2, 1, 1)
        n2 = jnp.concatenate([n2, jnp.zeros((1, KA - KB), f32)], axis=1)
        ones = jnp.ones((1, KA), f32)
        meta = jnp.concatenate(
            [n1, n2, total * ones, peak * ones, jnp.zeros((META - 6, KA), f32)], axis=0
        )
        for j in range(NY):
            st_send[j, :SH] = state[j * SH : (j + 1) * SH]
            st_send[j, SH:] = meta
        e1[pl.ds(iy, 1)] = st_send[pl.ds(iy, 1)]

    first_hop = Direct("y", NY, lambda j: st_send.at[j], e1, e1.at[0 : NY - 1], hop.at[0])
    first_hop.send()

    with scope("scores"):
        turned = jnp.transpose(jnp.concatenate([cum, cum, cum, cum], axis=0))
        causal = row_i >= col_i
        loads[7].wait()
        loads[8].wait()
        q1, q2 = q1_ref[...], jnp.transpose(q2_ref[...].astype(f32)).astype(bf16)
        local = []
        for h, (q, k, over, width, vh) in enumerate(((q1, k1, 1, KA, v1), (q2, k2, 0, KB, v2))):
            gaps = turned[:, h : h + 1] - cum[h : h + 1] + ig[h : h + 1]
            gaps = jnp.where(causal, gaps, -jnp.inf)
            top = jnp.max(gaps, axis=1, keepdims=True)
            scores = dg(q, k, 1, over) * (width ** -0.5)
            scores = scores * jnp.exp(gaps - top)
            local.append((top, left_dot(scores, vh, 1, 0), jnp.sum(scores, axis=1, keepdims=True)))

    stage(1)

    key_row = lax.broadcasted_iota(jnp.int32, (SH, KA), 0) + iy * SH

    def spread(both):
        return jnp.where(key_row < KA, both[0:1], both[1:2])

    def combine(early, late):
        decay_e, cell_e, norm_e, peak_e = early
        decay_l, cell_l, norm_l, peak_l = late
        moved = decay_l + peak_e
        ceiling = jnp.maximum(moved, peak_l)
        keep, fresh = jnp.exp(moved - ceiling), jnp.exp(peak_l - ceiling)
        return (
            decay_e + decay_l,
            spread(keep) * cell_e + spread(fresh) * cell_l,
            keep * norm_e + fresh * norm_l,
            ceiling,
        )

    def loaded(ref, j):
        return (ref[j, SH + 2 : SH + 4], ref[j, :SH], ref[j, SH : SH + 2], ref[j, SH + 4 : SH + 6])

    nothing = (
        jnp.zeros((2, KA), f32), jnp.zeros((SH, DV), f32), jnp.zeros((2, KA), f32),
        jnp.full((2, KA), NEG_BIG, f32),
    )
    with scope("e1take"):
        first_hop.take()
    with scope("e1comb"):
        running, inside = nothing, []
        for j in range(NY):
            inside.append(running)
            running = combine(running, loaded(e1, j))
        e2_send[:SH] = running[1]
        e2_send[SH:] = jnp.concatenate(
            [running[2], running[0], running[3], jnp.zeros((META - 6, KA), f32)], axis=0
        )
        e2[pl.ds(iz, 1)] = e2_send[...][None]
    second_hop = Direct("z", NZ, lambda j: e2_send, e2, e2.at[0 : NZ - 1], hop.at[1])
    second_hop.send()
    stage(2)
    with scope("e2take"):
        second_hop.take()
    with scope("e2comb"):
        before = nothing
        for k in range(NZ):
            later = combine(before, loaded(e2, k))
            before = jax.tree.map(lambda new, old: jnp.where(k < iz, new, old), later, before)
        norm_in, peak_in = jnp.zeros((2, KA), f32), jnp.zeros((2, KA), f32)
        for j in range(NY):
            _, cell_j, norm_j, peak_j = combine(before, inside[j])
            f_send[j] = cell_j
            norm_in = jnp.where(iy == j, norm_j, norm_in)
            peak_in = jnp.where(iy == j, peak_j, peak_in)
        cin[pl.ds(iy, 1)] = f_send[pl.ds(iy, 1)]
    third_hop = Direct("y", NY, lambda j: f_send.at[j], cin, cin.at[0 : NY - 1], hop.at[2])
    third_hop.send()
    stage(3)
    stage(4)
    with scope("e3take"):
        third_hop.take()

    with scope("cell"):
        for i in range(9, 15):
            loads[i].wait()
        cell_in = cin[...].reshape(KEYS, DV)
        columns = []
        for h, (q, width, cell) in enumerate(((q1, KA, cell_in[:KA]), (q2, KB, cell_in[KA:]))):
            top, own_num, own_den = local[h]
            carried = turned[:, h : h + 1] + peak_in[h : h + 1, 0:1]
            ceiling = jnp.maximum(carried, top)
            keep, fresh = jnp.exp(carried - ceiling), jnp.exp(top - ceiling)
            num = keep * right_dot(q, cell, 1, 0) + fresh * own_num
            den = keep * jnp.sum(q.astype(f32) * norm_in[h : h + 1, :width], axis=1, keepdims=True)
            den = den + fresh * own_den
            cell_out = num / jnp.maximum(jnp.abs(den), jnp.exp(-ceiling))
            center = jnp.mean(cell_out, -1, keepdims=True)
            away = cell_out - center
            var = jnp.mean(away * away, -1, keepdims=True)
            columns.append(away * lax.rsqrt(var + EPS))
        gate = 1.0 / (1.0 + jnp.exp(-og_ref[...].astype(f32)))
        mixed = (jnp.concatenate(columns, axis=1) * hg_ref[...] * gate).astype(bf16)
        wide = min(D, 512)
        for c in range(0, D, wide):
            part = dg(mixed, ow_ref[:, c : c + wide], 1, 0).astype(bf16)
            parts[:, :, :, c : c + wide] = part.reshape(X, 2, OWN, wide)
    out_proj = TpSum(X, parts, pair, chip_send, chip_recv, tsems.at[0])
    out_proj.start()
    stage(5, 0)
    with scope("rs1mid"):
        out_proj.between()
    stage(5, 1)
    with scope("rs1take"):
        mixer = out_proj.total().astype(bf16).astype(f32)
    with scope("norm1"):
        first = normed(stream_own[...].astype(f32) + mixer, mg_ref[...]).astype(bf16)
        x_all[pl.ds(chip, 1), pl.ds(core, 1)] = first[None, None]
    rows_out = TpGather(X, x_all, tsems.at[1], rowsems)
    rows_out.start()
    stage(6, 0)
    with scope("agrelay"):
        rows_out.relay()
    stage(6, 1)
    with scope("agtake"):
        rows_out.take()
    last = max(NY, NZ) - 1 + LAG
    stage(7)
    stage(8)
    with scope("upwait"):
        for item in ups:
            item.finish()
    with scope("mlp1"):
        wide_f = min(FD, 256)
        for c in range(0, FD, wide_f):
            x = x_all[...].reshape(T, D)
            w = up_all[:, :, :, c : c + wide_f].reshape(D, wide_f)
            act = jnp.maximum(dg(x, w, 1, 0), 0.0)
            hidden[:, c : c + wide_f] = (act * act).astype(bf16)
    for number in range(9, last + 1):
        stage(number)

    wide_d = NY * RW

    def columns(shift):
        return lax.rem(iz + shift, NZ)

    def second(shifts, store):
        for i, shift in enumerate(shifts):
            w = down_all[pl.ds(columns(shift), 1)].reshape(wide_d, FD)
            store[:, :, i] = dg(hidden[...], w, 1, 1).astype(bf16).reshape(X, 2, OWN, wide_d)

    shifts = sorted(range(NZ), key=lambda s: min(s, NZ - s))
    early = early_blocks(NZ)
    sums = []
    if early:
        with scope("mlp2a"):
            for item, axis in zip(downs, (1, 0)):
                item.near(axis, NZ // 2 - 2)
            second(shifts[:early], parts_a)
        sums.append((TpSum(X, parts_a, pair_a, send_a, recv_a, tsems.at[2]), shifts[:early]))
        sums[-1][0].start()
    with scope("downwait"):
        for item in downs:
            item.finish()
    with scope("mlp2b"):
        second(shifts[early:], parts_b)
    sums.append((TpSum(X, parts_b, pair_b, send_b, recv_b, tsems.at[3]), shifts[early:]))
    sums[-1][0].start()
    with scope("rs2mid"):
        for item, _ in sums:
            item.between()
    with scope("drain"):
        for item in (first_hop, second_hop, third_hop, out_proj, rows_out, *ups, *downs):
            item.drain()
    with scope("rs2take"):
        for item, where in sums:
            total_of = item.total()
            for i, shift in enumerate(where):
                mlp_sum[:, pl.ds(pl.multiple_of(columns(shift) * wide_d, wide_d), wide_d)] = total_of[i]
        mlp_out = mlp_sum[...].astype(bf16).astype(f32)
    with scope("norm2"):
        base = x_all[pl.ds(chip, 1), pl.ds(core, 1)].reshape(OWN, D).astype(f32)
        out_ref[...] = normed(base + mlp_out, outg_ref[...]).astype(bf16)
    with scope("lastdrain"):
        for item, _ in sums:
            item.drain()


def layer(
    sizes, query_one, key_one, query_two, key_two, values, out_gate, in_gate, forget_gate,
    head_gain, out_weight, stream, mix_gain, up_weight, down_weight, out_gain,
):
    NZ, NY, TP = sizes
    X = TP // 2
    T, D = stream.shape
    OWN = T // TP
    RW, FD = up_weight.shape
    SH = (query_one.shape[1] + query_two.shape[1]) // NY
    KA = query_one.shape[1]
    sem = pltpu.SemaphoreType.DMA
    half = max(NY, NZ) // 2
    early = early_blocks(NZ)
    operands = (
        query_one, key_one, query_two.T, key_two.T, values, out_gate, in_gate, forget_gate,
        head_gain.reshape(1, -1), out_weight, stream, mix_gain.reshape(1, -1), up_weight,
        down_weight.T, out_gain.reshape(1, -1),
    )
    copied = [operands[i] for i in (0, 1, 2, 3, 4, 5, 6, 7, 8, 9, 11, 14)]

    def exchange(*inner):
        return [pltpu.VMEM((X, 2) + inner, bf16)] + [pltpu.VMEM((X,) + inner, bf16)] * 3

    return pl.pallas_call(
        functools.partial(kernel, sizes),
        out_shape=jax.ShapeDtypeStruct((OWN, D), bf16),
        in_specs=[pl.BlockSpec(memory_space=pltpu.HBM)] * len(operands),
        out_specs=pl.BlockSpec(memory_space=pltpu.VMEM),
        scratch_shapes=[pltpu.VMEM(a.shape, a.dtype) for a in copied]
        + [
            pltpu.VMEM((NZ, NY, RW, FD), bf16),
            pltpu.VMEM((NZ, NY, RW, FD), bf16),
            pltpu.VMEM((NY, SH + META, KA), f32),
            pltpu.VMEM((NY, SH + META, KA), f32),
            pltpu.VMEM((SH + META, KA), f32),
            pltpu.VMEM((NZ, SH + META, KA), f32),
            pltpu.VMEM((NY, SH, KA), f32),
            pltpu.VMEM((NY, SH, KA), f32),
        ]
        + exchange(OWN, D)
        + [pltpu.VMEM((X, 2, OWN, D), bf16), pltpu.VMEM((T, FD), bf16)]
        + exchange(max(early, 1), OWN, NY * RW)
        + exchange(NZ - early, OWN, NY * RW)
        + [
            pltpu.VMEM((OWN, D), f32),
            pltpu.VMEM((OWN, D), bf16),
            sem((15,)),
            sem((3, 2)), sem((4, 2)), sem((4, half)), sem((4, half, half + 1)), sem((4, 4)), sem((X,)),
        ],
        compiler_params=pltpu.CompilerParams(
            collective_id=0, has_side_effects=True, vmem_limit_bytes=60000 * 1024
        ),
    )(*operands)


def build(mesh, nz, ny):
    tp = mesh.shape["tp"]
    split = Mesh(mesh.devices.reshape(nz, ny, tp), ("z", "y", "tp"))
    SP = ("z", "y")
    return jax.shard_map(
        functools.partial(layer, (nz, ny, tp)),
        mesh=split,
        in_specs=(
            P(SP, "tp"), P(SP, "tp"), P(SP, "tp"), P(SP, "tp"), P(SP, "tp"), P(SP, "tp"),
            P("tp", SP), P("tp", SP), P("tp"), P("tp", None), P(SP, None), P(),
            P(SP, "tp"), P("tp", SP), P(),
        ),
        out_specs=P(("z", "y", "tp"), None),
        check_vma=False,
    )


def solution(mesh):
    return build(mesh, 8, 8)
```

```python
import contextlib
import functools
import itertools

import jax
import jax.numpy as jnp
from jax import lax
from jax.experimental import pallas as pl
from jax.experimental.pallas import tpu as pltpu
from jax.sharding import Mesh
from jax.sharding import PartitionSpec as P

NEG_BIG = -1e30
EPS = 1e-05
META = 8
f32, bf16 = jnp.float32, jnp.bfloat16
MESH = pl.DeviceIdType.MESH
LAG = 2
scope = contextlib.nullcontext


def dg(a, b, ca, cb):
    return lax.dot_general(a, b, (((ca,), (cb,)), ((), ())), preferred_element_type=f32)


def three(a):
    hi = a.astype(bf16)
    rest = a - hi.astype(f32)
    mid = rest.astype(bf16)
    return hi, mid, (rest - mid.astype(f32)).astype(bf16)


def left_dot(a, b, ca, cb):
    hi, mid, lo = three(a)
    return dg(hi, b, ca, cb) + (dg(mid, b, ca, cb) + dg(lo, b, ca, cb))


def right_dot(a, b, ca, cb):
    hi, mid, lo = three(b)
    return dg(a, hi, ca, cb) + (dg(a, mid, ca, cb) + dg(a, lo, ca, cb))


def remote(src, dst, ssem, rsem, target):
    return pltpu.make_async_remote_copy(
        src_ref=src, dst_ref=dst, send_sem=ssem, recv_sem=rsem, device_id=target, device_id_type=MESH
    )


class Gather:
    def __init__(self, axes, sizes, shard, spans, send_sems, first_recv, second_recv):
        self.axes, self.sizes, self.shard, self.spans = axes, sizes, shard, spans
        self.send_sems, self.first_recv, self.second_recv = send_sems, first_recv, second_recv
        self.me = [lax.axis_index(axis) for axis in axes]
        self.steps = [n // 2 for n in sizes]
        self.waited = set()

    def at(self, axis, offset):
        return lax.rem(self.me[axis] + offset % self.sizes[axis], self.sizes[axis])

    def away(self, axis, way, distance):
        return self.at(axis, -distance if way == 0 else distance)

    def target(self, axis, way):
        return {self.axes[axis]: self.at(axis, 1 if way == 0 else -1)}

    def first_ways(self, step):
        return (0, 1) if step < self.steps[0] else (1,)

    def second_ways(self, step, r):
        if step < self.steps[1]:
            return (0, 1)
        return (0,) if r < (self.sizes[0] + 1) // 2 else (1,)

    def ranked(self, rank):
        return sorted({rank, (self.sizes[0] - rank) % self.sizes[0]})

    def send_first(self, step):
        if step <= self.steps[0]:
            for way in self.first_ways(step):
                ref = self.shard(self.away(0, way, step - 1), self.me[1])
                remote(ref, ref, self.send_sems.at[0], self.first_recv.at[step - 1], self.target(0, way)).start()

    def take_first(self, step):
        if step <= self.steps[0] and step not in self.waited:
            self.waited.add(step)
            ref = self.spans[0](len(self.first_ways(step)))
            remote(ref, ref, self.send_sems.at[0], self.first_recv.at[step - 1], self.target(0, 0)).wait_recv()

    def send(self, step, rank):
        for r in self.ranked(rank):
            for way in self.second_ways(step, r):
                ref = self.shard(self.at(0, r), self.away(1, way, step - 1))
                remote(ref, ref, self.send_sems.at[1], self.second_recv.at[step - 1, rank],
                       self.target(1, way)).start()

    def take(self, step, rank):
        if (step, rank) not in self.waited:
            self.waited.add((step, rank))
            ref = self.spans[0](sum(len(self.second_ways(step, r)) for r in self.ranked(rank)))
            remote(ref, ref, self.send_sems.at[1], self.second_recv.at[step - 1, rank],
                   self.target(1, 0)).wait_recv()

    def stage(self, stage):
        def one():
            if stage:
                self.take_first(stage)
            self.send_first(stage + 1)

        def further(step, rank):
            if step > 1:
                self.take(step - 1, rank)
            self.send(step, rank)

        actions = [one]
        for step in range(1, self.steps[1] + 1):
            if 0 <= stage - step + 1 <= self.steps[0]:
                actions.append(functools.partial(further, step, stage - step + 1))
        return actions

    def finish(self):
        for step in range(1, self.steps[0] + 1):
            self.take_first(step)
        for step in range(1, self.steps[1] + 1):
            for rank in range(self.steps[0] + 1):
                self.take(step, rank)

    def near(self, axis, reach):
        for step in range(1, self.steps[0] + 1):
            if axis == 1 or step <= reach:
                self.take_first(step)
        for step in range(1, self.steps[1] + 1):
            for rank in range(self.steps[0] + 1):
                if (step if axis == 1 else rank) <= reach:
                    self.take(step, rank)

    def drain(self):
        for sem, ref in ((0, self.spans[1]), (1, self.spans[2])):
            remote(ref, ref, self.send_sems.at[sem], self.first_recv.at[0], self.target(0, 0)).wait_send()


class Direct:
    def __init__(self, axis, n, source, slots, span, sems):
        self.axis, self.n, self.source, self.slots, self.span, self.sems = axis, n, source, slots, span, sems
        self.me = lax.axis_index(axis)

    def send(self):
        for d in range(1, self.n):
            peer = lax.rem(self.me + d, self.n)
            remote(self.source(peer), self.slots.at[self.me], self.sems.at[0], self.sems.at[1],
                   {self.axis: peer}).start()

    def whole(self):
        return remote(self.span, self.span, self.sems.at[0], self.sems.at[1], {self.axis: lax.rem(self.me + 1, self.n)})

    def take(self):
        self.whole().wait_recv()

    def drain(self):
        self.whole().wait_send()


class TpSum:
    def __init__(self, chips, source, pair, chip_send, chip_recv, sems):
        self.chips, self.source, self.pair = chips, source, pair
        self.chip_send, self.chip_recv, self.sems = chip_send, chip_recv, sems
        it = lax.axis_index("tp")
        self.chip, self.core = lax.div(it, 2), lax.rem(it, 2)

    def inner(self):
        other = 1 - self.core
        return remote(self.source.at[:, other], self.pair, self.sems.at[0], self.sems.at[1],
                      {"tp": self.chip * 2 + other})

    def outer(self):
        ref = self.chip_recv.at[0 : self.chips - 1]
        peer = lax.rem(self.chip + 1, self.chips)
        return remote(ref, ref, self.sems.at[2], self.sems.at[3], {"tp": peer * 2 + self.core})

    def start(self):
        self.inner().start()

    def between(self):
        self.inner().wait_recv()
        mine = self.source[:, pl.ds(self.core, 1)].astype(f32)
        both = mine.reshape(self.pair.shape) + self.pair[...].astype(f32)
        self.chip_send[...] = both.astype(bf16)
        for d in range(1, self.chips):
            peer = lax.rem(self.chip + d, self.chips)
            remote(self.chip_send.at[peer], self.chip_recv.at[self.chip], self.sems.at[2], self.sems.at[3],
                   {"tp": peer * 2 + self.core}).start()
        self.chip_recv[pl.ds(self.chip, 1)] = self.chip_send[pl.ds(self.chip, 1)]

    def total(self):
        if self.chips > 1:
            self.outer().wait_recv()
        return jnp.sum(self.chip_recv[...].astype(f32), axis=0)

    def drain(self):
        self.inner().wait_send()
        if self.chips > 1:
            self.outer().wait_send()


class TpGather:
    def __init__(self, chips, slots, sems, chip_sems):
        self.chips, self.slots, self.sems, self.chip_sems = chips, slots, sems, chip_sems
        it = lax.axis_index("tp")
        self.chip, self.core = lax.div(it, 2), lax.rem(it, 2)

    def outer(self, d, ref):
        peer = lax.rem(self.chip + d, self.chips)
        return remote(ref, ref, self.sems.at[0], self.chip_sems.at[d], {"tp": peer * 2 + self.core})

    def inner(self, ref):
        return remote(ref, ref, self.sems.at[1], self.sems.at[2], {"tp": self.chip * 2 + 1 - self.core})

    def start(self):
        for d in range(1, self.chips):
            self.outer(d, self.slots.at[self.chip, self.core]).start()
        self.inner(self.slots.at[self.chip, self.core]).start()

    def relay(self):
        for d in sorted(range(1, self.chips), key=lambda d: min(d, self.chips - d)):
            ref = self.slots.at[lax.rem(self.chip + self.chips - d, self.chips), self.core]
            self.outer(d, ref).wait_recv()
            self.inner(ref).start()

    def take(self):
        self.inner(self.slots.at[:, 0]).wait_recv()

    def drain(self):
        if self.chips > 1:
            self.outer(1, self.slots.at[0 : self.chips - 1, 0]).wait_send()
        self.inner(self.slots.at[:, 0]).wait_send()


def normed(rows, gain):
    center = jnp.mean(rows, -1, keepdims=True)
    away = rows - center
    spread = jnp.mean(away * away, -1, keepdims=True)
    return away * lax.rsqrt(spread + EPS) * gain


def early_blocks(nz):
    return sum(min(s, nz - s) <= nz // 2 - 2 for s in range(nz))


def kernel(
    sizes,
    q1_hbm, k1_hbm, q2_hbm, k2_hbm, v_hbm, og_hbm, ig_hbm, fg_hbm, hg_hbm, ow_hbm,
    stream_ref, mg_hbm, up_ref, down_ref, outg_hbm,
    out_ref,
    q1_ref, k1_ref, q2_ref, k2_ref, v_ref, og_ref, ig_ref, fg_ref, hg_ref, ow_ref, mg_ref, outg_ref,
    up_all, down_all, st_send, e1, e2_send, e2, f_send, cin,
    parts, pair, chip_send, chip_recv, x_all, hidden, parts_a, pair_a, send_a, recv_a, parts_b, pair_b, send_b, recv_b, last_parts, last_recv, mlp_sum, stream_own,
    local_sem, hop, gsend, g1recv, g2recv, tsems, rowsems,
):
    NZ, NY, TP = sizes
    X = TP // 2
    iz, iy, it = lax.axis_index("z"), lax.axis_index("y"), lax.axis_index("tp")
    chip, core = lax.div(it, 2), lax.rem(it, 2)
    T, KA = q1_ref.shape
    KB = k2_ref.shape[0]
    DV = v_ref.shape[1] // 2
    KEYS = KA + KB
    SH = KEYS // NY
    OWN = T // TP
    D = ow_ref.shape[1]
    RW, FD = up_ref.shape

    barrier = pltpu.get_barrier_semaphore()
    peers = 0
    greeted = [{axis: lax.rem(lax.axis_index(axis) + d, n)} for axis, n in (("y", NY), ("z", NZ)) for d in range(1, n)]
    greeted += [{"tp": lax.rem(it + d, TP)} for d in range(1, TP)]
    for peer in greeted:
        pl.semaphore_signal(barrier, inc=1, device_id=peer, device_id_type=MESH)

    loads = []
    for src, dst in (
        (up_ref, up_all.at[iz, iy]), (down_ref, down_all.at[iz, iy]),
        (fg_hbm, fg_ref), (ig_hbm, ig_ref), (k1_hbm, k1_ref), (k2_hbm, k2_ref), (v_hbm, v_ref),
        (q1_hbm, q1_ref), (q2_hbm, q2_ref), (og_hbm, og_ref), (hg_hbm, hg_ref), (ow_hbm, ow_ref),
        (stream_ref.at[pl.ds(pl.multiple_of(it * OWN, OWN), OWN), :], stream_own),
        (mg_hbm, mg_ref), (outg_hbm, outg_ref),
    ):
        copy = pltpu.make_async_copy(src, dst, local_sem.at[len(loads)])
        copy.start()
        loads.append(copy)

    half = RW // 2

    def gather(weights, low, sems, first_recv, second_recv):
        part = slice(0, half) if low else slice(half, RW)
        if low:
            axes, sizes = ("y", "z"), (NY, NZ)
            shard = lambda a, b: weights.at[b, a, part]
            spans = (lambda n: weights.at[0, 0:n, part] if n <= NY else weights.at[0:2, 0 : n // 2, part],
                     weights.at[0, 0 : NY - 1, part], weights.at[0 : NZ - 1, :, part])
        else:
            axes, sizes = ("z", "y"), (NZ, NY)
            shard = lambda a, b: weights.at[a, b, part]
            spans = (lambda n: weights.at[0, 0:n, part] if n <= NY else weights.at[0:2, 0 : n // 2, part],
                     weights.at[0 : NZ - 1, 0, part], weights.at[:, 0 : NY - 1, part])
        return Gather(axes, sizes, shard, spans, sems, first_recv, second_recv)

    ups = [gather(up_all, i == 0, gsend.at[i], g1recv.at[i], g2recv.at[i]) for i in range(2)]
    downs = [gather(down_all, i == 0, gsend.at[2 + i], g1recv.at[2 + i], g2recv.at[2 + i]) for i in range(2)]

    def stage(number, part=None):
        late = number if number < 2 else number - LAG
        lists = [item.stage(number) for item in ups]
        if number < 2 or late >= 2:
            lists += [item.stage(late) for item in downs]
        rows = list(itertools.zip_longest(*lists))
        cut = (len(rows) + 1) // 2
        with scope(f"stage{number}{part}"):
            for row in rows[:cut] if part == 0 else rows[cut:] if part == 1 else rows:
                for action in row:
                    if action is not None:
                        action()

    loads[0].wait()
    loads[1].wait()
    with scope("barrier"):
        pl.semaphore_wait(barrier, len(greeted))
    stage(0)

    with scope("local"):
        row_i = lax.broadcasted_iota(jnp.int32, (T, T), 0)
        col_i = lax.broadcasted_iota(jnp.int32, (T, T), 1)
        upto = jnp.where(row_i <= col_i, 1.0, 0.0).astype(bf16)
        for i in range(2, 7):
            loads[i].wait()
        log_forget = -jnp.log1p(jnp.exp(-fg_ref[...]))
        ig = ig_ref[...]
        cum = left_dot(log_forget, upto, 1, 0)
        total = cum[:, T - 1 : T]
        weight_log = total - cum + ig
        peak = jnp.max(weight_log, axis=1, keepdims=True)
        weight = jnp.exp(weight_log - peak)
        scaled1, scaled2 = weight[0:1] * (KA ** -0.5), weight[1:2] * (KB ** -0.5)
        v1, v2 = v_ref[:, :DV], v_ref[:, DV:]
        k1, k2 = k1_ref[...], k2_ref[...]
        state = jnp.concatenate(
            [
                left_dot(jnp.transpose(k1.astype(f32)) * scaled1, v1, 1, 0),
                left_dot(k2.astype(f32) * scaled2, v2, 1, 0),
            ],
            axis=0,
        )
        n1 = left_dot(scaled1, k1, 1, 0)
        n2 = left_dot(scaled2, k2, 1, 1)
        n2 = jnp.concatenate([n2, jnp.zeros((1, KA - KB), f32)], axis=1)
        ones = jnp.ones((1, KA), f32)
        meta = jnp.concatenate(
            [n1, n2, total * ones, peak * ones, jnp.zeros((META - 6, KA), f32)], axis=0
        )
        for j in range(NY):
            st_send[j, :SH] = state[j * SH : (j + 1) * SH]
            st_send[j, SH:] = meta
        e1[pl.ds(iy, 1)] = st_send[pl.ds(iy, 1)]

    first_hop = Direct("y", NY, lambda j: st_send.at[j], e1, e1.at[0 : NY - 1], hop.at[0])
    first_hop.send()

    with scope("scores"):
        turned = jnp.transpose(jnp.concatenate([cum, cum, cum, cum], axis=0))
        causal = row_i >= col_i
        loads[7].wait()
        loads[8].wait()
        q1, q2 = q1_ref[...], jnp.transpose(q2_ref[...].astype(f32)).astype(bf16)
        local = []
        for h, (q, k, over, width, vh) in enumerate(((q1, k1, 1, KA, v1), (q2, k2, 0, KB, v2))):
            gaps = turned[:, h : h + 1] - cum[h : h + 1] + ig[h : h + 1]
            gaps = jnp.where(causal, gaps, -jnp.inf)
            top = jnp.max(gaps, axis=1, keepdims=True)
            scores = dg(q, k, 1, over) * (width ** -0.5)
            scores = scores * jnp.exp(gaps - top)
            local.append((top, left_dot(scores, vh, 1, 0), jnp.sum(scores, axis=1, keepdims=True)))

    stage(1)

    key_row = lax.broadcasted_iota(jnp.int32, (SH, KA), 0) + iy * SH

    def spread(both):
        return jnp.where(key_row < KA, both[0:1], both[1:2])

    def combine(early, late):
        decay_e, cell_e, norm_e, peak_e = early
        decay_l, cell_l, norm_l, peak_l = late
        moved = decay_l + peak_e
        ceiling = jnp.maximum(moved, peak_l)
        keep, fresh = jnp.exp(moved - ceiling), jnp.exp(peak_l - ceiling)
        return (
            decay_e + decay_l,
            spread(keep) * cell_e + spread(fresh) * cell_l,
            keep * norm_e + fresh * norm_l,
            ceiling,
        )

    def loaded(ref, j):
        return (ref[j, SH + 2 : SH + 4], ref[j, :SH], ref[j, SH : SH + 2], ref[j, SH + 4 : SH + 6])

    nothing = (
        jnp.zeros((2, KA), f32), jnp.zeros((SH, DV), f32), jnp.zeros((2, KA), f32),
        jnp.full((2, KA), NEG_BIG, f32),
    )
    stage(2)
    with scope("e1take"):
        first_hop.take()
    with scope("e1comb"):
        running, inside = nothing, []
        for j in range(NY):
            inside.append(running)
            running = combine(running, loaded(e1, j))
        e2_send[:SH] = running[1]
        e2_send[SH:] = jnp.concatenate(
            [running[2], running[0], running[3], jnp.zeros((META - 6, KA), f32)], axis=0
        )
        e2[pl.ds(iz, 1)] = e2_send[...][None]
    second_hop = Direct("z", NZ, lambda j: e2_send, e2, e2.at[0 : NZ - 1], hop.at[1])
    second_hop.send()
    stage(3)
    with scope("e2take"):
        second_hop.take()
    with scope("e2comb"):
        before = nothing
        for k in range(NZ):
            later = combine(before, loaded(e2, k))
            before = jax.tree.map(lambda new, old: jnp.where(k < iz, new, old), later, before)
        norm_in, peak_in = jnp.zeros((2, KA), f32), jnp.zeros((2, KA), f32)
        for j in range(NY):
            _, cell_j, norm_j, peak_j = combine(before, inside[j])
            f_send[j] = cell_j
            norm_in = jnp.where(iy == j, norm_j, norm_in)
            peak_in = jnp.where(iy == j, peak_j, peak_in)
        cin[pl.ds(iy, 1)] = f_send[pl.ds(iy, 1)]
    third_hop = Direct("y", NY, lambda j: f_send.at[j], cin, cin.at[0 : NY - 1], hop.at[2])
    third_hop.send()
    stage(4)
    stage(5, 0)
    with scope("e3take"):
        third_hop.take()

    with scope("cell"):
        for i in range(9, 15):
            loads[i].wait()
        cell_in = cin[...].reshape(KEYS, DV)
        columns = []
        for h, (q, width, cell) in enumerate(((q1, KA, cell_in[:KA]), (q2, KB, cell_in[KA:]))):
            top, own_num, own_den = local[h]
            carried = turned[:, h : h + 1] + peak_in[h : h + 1, 0:1]
            ceiling = jnp.maximum(carried, top)
            keep, fresh = jnp.exp(carried - ceiling), jnp.exp(top - ceiling)
            num = keep * right_dot(q, cell, 1, 0) + fresh * own_num
            den = keep * jnp.sum(q.astype(f32) * norm_in[h : h + 1, :width], axis=1, keepdims=True)
            den = den + fresh * own_den
            cell_out = num / jnp.maximum(jnp.abs(den), jnp.exp(-ceiling))
            center = jnp.mean(cell_out, -1, keepdims=True)
            away = cell_out - center
            var = jnp.mean(away * away, -1, keepdims=True)
            columns.append(away * lax.rsqrt(var + EPS))
        gate = 1.0 / (1.0 + jnp.exp(-og_ref[...].astype(f32)))
        mixed = (jnp.concatenate(columns, axis=1) * hg_ref[...] * gate).astype(bf16)
        wide = min(D, 512)
        for c in range(0, D, wide):
            part = dg(mixed, ow_ref[:, c : c + wide], 1, 0).astype(bf16)
            parts[:, :, :, c : c + wide] = part.reshape(X, 2, OWN, wide)
    out_proj = TpSum(X, parts, pair, chip_send, chip_recv, tsems.at[0])
    out_proj.start()
    stage(5, 1)
    with scope("rs1mid"):
        out_proj.between()
    stage(6)
    with scope("rs1take"):
        mixer = out_proj.total().astype(bf16).astype(f32)
    with scope("norm1"):
        first = normed(stream_own[...].astype(f32) + mixer, mg_ref[...]).astype(bf16)
        x_all[pl.ds(chip, 1), pl.ds(core, 1)] = first[None, None]
    rows_out = TpGather(X, x_all, tsems.at[1], rowsems)
    rows_out.start()
    stage(7)
    with scope("agrelay"):
        rows_out.relay()
    for number in range(8, 7 + LAG):
        stage(number)
    with scope("agtake"):
        rows_out.take()
    with scope("upwait"):
        for item in ups:
            item.finish()
    with scope("mlp1"):
        wide_f = min(FD, 256)
        for c in range(0, FD, wide_f):
            x = x_all[...].reshape(T, D)
            w = up_all[:, :, :, c : c + wide_f].reshape(D, wide_f)
            act = jnp.maximum(dg(x, w, 1, 0), 0.0)
            hidden[:, c : c + wide_f] = (act * act).astype(bf16)

    wide_d = NY * RW

    def columns(shift):
        return lax.rem(iz + shift, NZ)

    def second(shift):
        w = down_all[pl.ds(columns(shift), 1)].reshape(wide_d, FD)
        return dg(hidden[...], w, 1, 1).astype(bf16)

    shifts = sorted(range(NZ), key=lambda s: min(s, NZ - s))
    early = early_blocks(NZ)
    sums, at = [], 0
    for count, reach, refs, sems in (
        (early, NZ // 2 - 2, (parts_a, pair_a, send_a, recv_a), tsems.at[2]),
        (NZ - 1 - early, NZ // 2 - 1, (parts_b, pair_b, send_b, recv_b), tsems.at[3]),
    ):
        if count:
            with scope(f"mlp2 {reach}"):
                for item, axis in zip(downs, (1, 0)):
                    item.near(axis, reach)
                for i in range(count):
                    refs[0][:, :, i] = second(shifts[at + i]).reshape(X, 2, OWN, wide_d)
            sums.append((TpSum(X, *refs, sems), shifts[at : at + count]))
            sums[-1][0].start()
        at += count
        if not sums or len(sums) == 1 and count == early:
            stage(7 + LAG)
    with scope("rs2mid"):
        for item, _ in sums:
            item.between()
    with scope("downwait"):
        for item in downs:
            item.finish()
    with scope("mlp2 last"):
        last_parts[...] = second(shifts[-1]).reshape(TP, OWN, wide_d)
    last_sum = Direct("tp", TP, lambda j: last_parts.at[j], last_recv, last_recv.at[0 : TP - 1], hop.at[3])
    last_sum.send()
    last_recv[pl.ds(it, 1)] = last_parts[pl.ds(it, 1)]
    with scope("drain"):
        for item in (first_hop, second_hop, third_hop, out_proj, rows_out, *ups, *downs):
            item.drain()

    def put(shift, value):
        mlp_sum[:, pl.ds(pl.multiple_of(columns(shift) * wide_d, wide_d), wide_d)] = value

    with scope("rs2take"):
        for item, where in sums:
            total_of = item.total()
            for i, shift in enumerate(where):
                put(shift, total_of[i])
    with scope("rs2last"):
        last_sum.take()
        put(shifts[-1], jnp.sum(last_recv[...].astype(f32), axis=0))
        mlp_out = mlp_sum[...].astype(bf16).astype(f32)
    with scope("norm2"):
        base = x_all[pl.ds(chip, 1), pl.ds(core, 1)].reshape(OWN, D).astype(f32)
        out_ref[...] = normed(base + mlp_out, outg_ref[...]).astype(bf16)
    with scope("lastdrain"):
        for item, _ in sums:
            item.drain()
        last_sum.drain()


def layer(
    sizes, query_one, key_one, query_two, key_two, values, out_gate, in_gate, forget_gate,
    head_gain, out_weight, stream, mix_gain, up_weight, down_weight, out_gain,
):
    NZ, NY, TP = sizes
    X = TP // 2
    T, D = stream.shape
    OWN = T // TP
    RW, FD = up_weight.shape
    SH = (query_one.shape[1] + query_two.shape[1]) // NY
    KA = query_one.shape[1]
    sem = pltpu.SemaphoreType.DMA
    half = max(NY, NZ) // 2
    early = early_blocks(NZ)
    operands = (
        query_one, key_one, query_two.T, key_two.T, values, out_gate, in_gate, forget_gate,
        head_gain.reshape(1, -1), out_weight, stream, mix_gain.reshape(1, -1), up_weight,
        down_weight.T, out_gain.reshape(1, -1),
    )
    copied = [operands[i] for i in (0, 1, 2, 3, 4, 5, 6, 7, 8, 9, 11, 14)]

    def exchange(*inner):
        return [pltpu.VMEM((X, 2) + inner, bf16)] + [pltpu.VMEM((X,) + inner, bf16)] * 3

    return pl.pallas_call(
        functools.partial(kernel, sizes),
        out_shape=jax.ShapeDtypeStruct((OWN, D), bf16),
        in_specs=[pl.BlockSpec(memory_space=pltpu.HBM)] * len(operands),
        out_specs=pl.BlockSpec(memory_space=pltpu.VMEM),
        scratch_shapes=[pltpu.VMEM(a.shape, a.dtype) for a in copied]
        + [
            pltpu.VMEM((NZ, NY, RW, FD), bf16),
            pltpu.VMEM((NZ, NY, RW, FD), bf16),
            pltpu.VMEM((NY, SH + META, KA), f32),
            pltpu.VMEM((NY, SH + META, KA), f32),
            pltpu.VMEM((SH + META, KA), f32),
            pltpu.VMEM((NZ, SH + META, KA), f32),
            pltpu.VMEM((NY, SH, KA), f32),
            pltpu.VMEM((NY, SH, KA), f32),
        ]
        + exchange(OWN, D)
        + [pltpu.VMEM((X, 2, OWN, D), bf16), pltpu.VMEM((T, FD), bf16)]
        + exchange(max(early, 1), OWN, NY * RW)
        + exchange(max(NZ - 1 - early, 1), OWN, NY * RW)
        + [
            pltpu.VMEM((TP, OWN, NY * RW), bf16),
            pltpu.VMEM((TP, OWN, NY * RW), bf16),
            pltpu.VMEM((OWN, D), f32),
            pltpu.VMEM((OWN, D), bf16),
            sem((15,)),
            sem((4, 2)), sem((4, 2)), sem((4, half)), sem((4, half, half + 1)), sem((4, 4)), sem((X,)),
        ],
        compiler_params=pltpu.CompilerParams(
            collective_id=0, has_side_effects=True, vmem_limit_bytes=60000 * 1024
        ),
    )(*operands)


def build(mesh, nz, ny):
    tp = mesh.shape["tp"]
    split = Mesh(mesh.devices.reshape(nz, ny, tp), ("z", "y", "tp"))
    SP = ("z", "y")
    return jax.shard_map(
        functools.partial(layer, (nz, ny, tp)),
        mesh=split,
        in_specs=(
            P(SP, "tp"), P(SP, "tp"), P(SP, "tp"), P(SP, "tp"), P(SP, "tp"), P(SP, "tp"),
            P("tp", SP), P("tp", SP), P("tp"), P("tp", None), P(SP, None), P(),
            P(SP, "tp"), P("tp", SP), P(),
        ),
        out_specs=P(("z", "y", "tp"), None),
        check_vma=False,
    )


def solution(mesh):
    return build(mesh, 8, 8)
```

```python
import contextlib
import functools
import itertools

import jax
import jax.numpy as jnp
from jax import lax
from jax.experimental import pallas as pl
from jax.experimental.pallas import tpu as pltpu
from jax.sharding import Mesh
from jax.sharding import PartitionSpec as P

NEG_BIG = -1e30
EPS = 1e-05
META = 8
f32, bf16 = jnp.float32, jnp.bfloat16
MESH = pl.DeviceIdType.MESH
LATER = {
    0: ((1, 0),),
    1: ((1, 1),),
    4: ((1, 2), (1, 3), (1, 4), (2, 0)),
    5: ((2, 1), (2, 2), (2, 3), (3, 0)),
    6: ((2, 4), (3, 1), (3, 2), (4, 0)),
    7: ((3, 3), (3, 4), (4, 1), (4, 2)),
    8: ((4, 3), (4, 4)),
}
scope = contextlib.nullcontext


def dg(a, b, ca, cb):
    return lax.dot_general(a, b, (((ca,), (cb,)), ((), ())), preferred_element_type=f32)


def three(a):
    hi = a.astype(bf16)
    rest = a - hi.astype(f32)
    mid = rest.astype(bf16)
    return hi, mid, (rest - mid.astype(f32)).astype(bf16)


def left_dot(a, b, ca, cb):
    hi, mid, lo = three(a)
    return dg(hi, b, ca, cb) + (dg(mid, b, ca, cb) + dg(lo, b, ca, cb))


def right_dot(a, b, ca, cb):
    hi, mid, lo = three(b)
    return dg(a, hi, ca, cb) + (dg(a, mid, ca, cb) + dg(a, lo, ca, cb))


def remote(src, dst, ssem, rsem, target):
    return pltpu.make_async_remote_copy(
        src_ref=src, dst_ref=dst, send_sem=ssem, recv_sem=rsem, device_id=target, device_id_type=MESH
    )


class Gather:
    def __init__(self, axes, sizes, shard, spans, send_sems, first_recv, second_recv):
        self.axes, self.sizes, self.shard, self.spans = axes, sizes, shard, spans
        self.send_sems, self.first_recv, self.second_recv = send_sems, first_recv, second_recv
        self.me = [lax.axis_index(axis) for axis in axes]
        self.steps = [n // 2 for n in sizes]
        self.twins, self.waited = 1, set()

    def twin(self, other):
        if self.sizes == other.sizes:
            self.twins, self.first_recv, self.second_recv = 2, other.first_recv, other.second_recv
            other.twins, other.waited = 2, self.waited

    def at(self, axis, offset):
        return lax.rem(self.me[axis] + offset % self.sizes[axis], self.sizes[axis])

    def away(self, axis, way, distance):
        return self.at(axis, -distance if way == 0 else distance)

    def target(self, axis, way):
        return {self.axes[axis]: self.at(axis, 1 if way == 0 else -1)}

    def first_ways(self, step):
        return (0, 1) if step < self.steps[0] else (1,)

    def second_ways(self, step, r):
        if step < self.steps[1]:
            return (0, 1)
        return (0,) if r < (self.sizes[0] + 1) // 2 else (1,)

    def ranked(self, rank):
        return sorted({rank, (self.sizes[0] - rank) % self.sizes[0]})

    def send_first(self, step):
        if step <= self.steps[0]:
            for way in self.first_ways(step):
                ref = self.shard(self.away(0, way, step - 1), self.me[1])
                remote(ref, ref, self.send_sems.at[0], self.first_recv.at[step - 1], self.target(0, way)).start()

    def take_first(self, step):
        if step <= self.steps[0] and step not in self.waited:
            self.waited.add(step)
            ref = self.spans[0](self.twins * len(self.first_ways(step)))
            remote(ref, ref, self.send_sems.at[0], self.first_recv.at[step - 1], self.target(0, 0)).wait_recv()

    def send(self, step, rank):
        for r in self.ranked(rank):
            for way in self.second_ways(step, r):
                ref = self.shard(self.at(0, r), self.away(1, way, step - 1))
                remote(ref, ref, self.send_sems.at[1], self.second_recv.at[step - 1, rank],
                       self.target(1, way)).start()

    def take(self, step, rank):
        if (step, rank) not in self.waited:
            self.waited.add((step, rank))
            ref = self.spans[0](self.twins * sum(len(self.second_ways(step, r)) for r in self.ranked(rank)))
            remote(ref, ref, self.send_sems.at[1], self.second_recv.at[step - 1, rank],
                   self.target(1, 0)).wait_recv()

    def one(self, stage):
        if stage:
            self.take_first(stage)
        self.send_first(stage + 1)

    def further(self, step, rank):
        if step > 1:
            self.take(step - 1, rank)
        self.send(step, rank)

    def stage(self, stage, order=None):
        if order is None:
            order = [(step, stage - step + 1) for step in range(1, self.steps[1] + 1)]
        return [functools.partial(self.one, stage)] + [
            functools.partial(self.further, step, rank)
            for step, rank in order
            if step <= self.steps[1] and 0 <= rank <= self.steps[0]
        ]

    def finish(self):
        for step in range(1, self.steps[0] + 1):
            self.take_first(step)
        for step in range(1, self.steps[1] + 1):
            for rank in range(self.steps[0] + 1):
                self.take(step, rank)

    def near(self, axis, reach):
        for step in range(1, self.steps[0] + 1):
            if axis == 1 or step <= reach:
                self.take_first(step)
        for step in range(1, self.steps[1] + 1):
            for rank in range(self.steps[0] + 1):
                if (step if axis == 1 else rank) <= reach:
                    self.take(step, rank)

    def drain(self):
        for sem, ref in ((0, self.spans[1]), (1, self.spans[2])):
            remote(ref, ref, self.send_sems.at[sem], self.first_recv.at[0], self.target(0, 0)).wait_send()


class Direct:
    def __init__(self, axis, n, source, slots, span, sems):
        self.axis, self.n, self.source, self.slots, self.span, self.sems = axis, n, source, slots, span, sems
        self.me = lax.axis_index(axis)

    def send(self):
        for d in range(1, self.n):
            peer = lax.rem(self.me + d, self.n)
            remote(self.source(peer), self.slots.at[self.me], self.sems.at[0], self.sems.at[1],
                   {self.axis: peer}).start()

    def whole(self):
        return remote(self.span, self.span, self.sems.at[0], self.sems.at[1], {self.axis: lax.rem(self.me + 1, self.n)})

    def take(self):
        self.whole().wait_recv()

    def drain(self):
        self.whole().wait_send()


class TpSum:
    def __init__(self, chips, source, pair, chip_send, chip_recv, sems):
        self.chips, self.source, self.pair = chips, source, pair
        self.chip_send, self.chip_recv, self.sems = chip_send, chip_recv, sems
        it = lax.axis_index("tp")
        self.chip, self.core = lax.div(it, 2), lax.rem(it, 2)

    def inner(self):
        other = 1 - self.core
        return remote(self.source.at[:, other], self.pair, self.sems.at[0], self.sems.at[1],
                      {"tp": self.chip * 2 + other})

    def outer(self):
        ref = self.chip_recv.at[0 : self.chips - 1]
        peer = lax.rem(self.chip + 1, self.chips)
        return remote(ref, ref, self.sems.at[2], self.sems.at[3], {"tp": peer * 2 + self.core})

    def start(self):
        self.inner().start()

    def between(self):
        self.inner().wait_recv()
        mine = self.source[:, pl.ds(self.core, 1)].astype(f32)
        both = mine.reshape(self.pair.shape) + self.pair[...].astype(f32)
        self.chip_send[...] = both.astype(bf16)
        for d in range(1, self.chips):
            peer = lax.rem(self.chip + d, self.chips)
            remote(self.chip_send.at[peer], self.chip_recv.at[self.chip], self.sems.at[2], self.sems.at[3],
                   {"tp": peer * 2 + self.core}).start()
        self.chip_recv[pl.ds(self.chip, 1)] = self.chip_send[pl.ds(self.chip, 1)]

    def total(self):
        if self.chips > 1:
            self.outer().wait_recv()
        return jnp.sum(self.chip_recv[...].astype(f32), axis=0)

    def drain(self):
        self.inner().wait_send()
        if self.chips > 1:
            self.outer().wait_send()


class TpGather:
    def __init__(self, chips, slots, sems, chip_sems):
        self.chips, self.slots, self.sems, self.chip_sems = chips, slots, sems, chip_sems
        it = lax.axis_index("tp")
        self.chip, self.core = lax.div(it, 2), lax.rem(it, 2)

    def outer(self, d, ref):
        peer = lax.rem(self.chip + d, self.chips)
        return remote(ref, ref, self.sems.at[0], self.chip_sems.at[d], {"tp": peer * 2 + self.core})

    def inner(self, ref):
        return remote(ref, ref, self.sems.at[1], self.sems.at[2], {"tp": self.chip * 2 + 1 - self.core})

    def start(self):
        for d in range(1, self.chips):
            self.outer(d, self.slots.at[self.chip, self.core]).start()
        self.inner(self.slots.at[self.chip, self.core]).start()

    def relay(self):
        for d in sorted(range(1, self.chips), key=lambda d: min(d, self.chips - d)):
            ref = self.slots.at[lax.rem(self.chip + self.chips - d, self.chips), self.core]
            self.outer(d, ref).wait_recv()
            self.inner(ref).start()

    def take(self):
        self.inner(self.slots.at[:, 0]).wait_recv()

    def drain(self):
        if self.chips > 1:
            self.outer(1, self.slots.at[0 : self.chips - 1, 0]).wait_send()
        self.inner(self.slots.at[:, 0]).wait_send()


def normed(rows, gain):
    center = jnp.mean(rows, -1, keepdims=True)
    away = rows - center
    spread = jnp.mean(away * away, -1, keepdims=True)
    return away * lax.rsqrt(spread + EPS) * gain


def early_blocks(nz):
    return sum(min(s, nz - s) <= nz // 2 - 2 for s in range(nz))


def kernel(
    sizes,
    q1_hbm, k1_hbm, q2_hbm, k2_hbm, v_hbm, og_hbm, ig_hbm, fg_hbm, hg_hbm, ow_hbm,
    stream_ref, mg_hbm, up_ref, down_ref, outg_hbm,
    out_ref,
    q1_ref, k1_ref, q2_ref, k2_ref, v_ref, og_ref, ig_ref, fg_ref, hg_ref, ow_ref, mg_ref, outg_ref,
    up_all, down_all, st_send, e1, e2_send, e2, f_send, cin,
    parts, pair, chip_send, chip_recv, x_all, hidden, parts_a, pair_a, send_a, recv_a, parts_b, recv_b, last_parts, last_recv, mlp_sum, stream_own,
    local_sem, hop, gsend, g1recv, g2recv, tsems, rowsems,
):
    NZ, NY, TP = sizes
    X = TP // 2
    iz, iy, it = lax.axis_index("z"), lax.axis_index("y"), lax.axis_index("tp")
    chip, core = lax.div(it, 2), lax.rem(it, 2)
    T, KA = q1_ref.shape
    KB = k2_ref.shape[0]
    DV = v_ref.shape[1] // 2
    KEYS = KA + KB
    SH = KEYS // NY
    OWN = T // TP
    D = ow_ref.shape[1]
    RW, FD = up_ref.shape

    barrier = pltpu.get_barrier_semaphore()
    peers = 0
    greeted = [{axis: lax.rem(lax.axis_index(axis) + d, n)} for axis, n in (("y", NY), ("z", NZ)) for d in range(1, n)]
    greeted += [{"tp": lax.rem(it + d, TP)} for d in range(1, TP)]
    for peer in greeted:
        pl.semaphore_signal(barrier, inc=1, device_id=peer, device_id_type=MESH)

    loads = []
    for src, dst in (
        (up_ref, up_all.at[iz, iy]), (down_ref, down_all.at[iz, iy]),
        (fg_hbm, fg_ref), (ig_hbm, ig_ref), (k1_hbm, k1_ref), (k2_hbm, k2_ref), (v_hbm, v_ref),
        (q1_hbm, q1_ref), (q2_hbm, q2_ref), (og_hbm, og_ref), (hg_hbm, hg_ref), (ow_hbm, ow_ref),
        (stream_ref.at[pl.ds(pl.multiple_of(it * OWN, OWN), OWN), :], stream_own),
        (mg_hbm, mg_ref), (outg_hbm, outg_ref),
    ):
        copy = pltpu.make_async_copy(src, dst, local_sem.at[len(loads)])
        copy.start()
        loads.append(copy)

    half = RW // 2
    HALVES = 1 if NY == NZ else 2

    def gather(weights, low, sems, first_recv, second_recv):
        part = slice(0, half) if low else slice(half, RW)
        if low:
            axes, sizes = ("y", "z"), (NY, NZ)
            shard = lambda a, b: weights.at[b, a, part]
            spans = (lambda n: weights.at[0 : -(-n // NY), 0 : min(n, NY), part],
                     weights.at[0, 0 : NY - 1, part], weights.at[0 : NZ - 1, :, part])
        else:
            axes, sizes = ("z", "y"), (NZ, NY)
            shard = lambda a, b: weights.at[a, b, part]
            spans = (lambda n: weights.at[0 : -(-n // NY), 0 : min(n, NY), part],
                     weights.at[0 : NZ - 1, 0, part], weights.at[:, 0 : NY - 1, part])
        return Gather(axes, sizes, shard, spans, sems, first_recv, second_recv)

    ups = [gather(up_all, i == 0, gsend.at[i], g1recv.at[i % HALVES], g2recv.at[i % HALVES]) for i in range(2)]
    downs = [gather(down_all, i == 0, gsend.at[2 + i], g1recv.at[HALVES + i % HALVES], g2recv.at[HALVES + i % HALVES]) for i in range(2)]

    for low, high in (ups, downs):
        low.twin(high)

    def stage(number, part=None):
        lists = [item.stage(number) for item in ups] + [item.stage(number, LATER.get(number, ())) for item in downs]
        rows = list(itertools.zip_longest(*lists))
        cut = (len(rows) + 1) // 2
        with scope(f"stage{number}{part}"):
            for row in rows[:cut] if part == 0 else rows[cut:] if part == 1 else rows:
                for action in row:
                    if action is not None:
                        action()

    loads[0].wait()
    loads[1].wait()
    with scope("barrier"):
        pl.semaphore_wait(barrier, len(greeted))
    stage(0)

    with scope("local"):
        row_i = lax.broadcasted_iota(jnp.int32, (T, T), 0)
        col_i = lax.broadcasted_iota(jnp.int32, (T, T), 1)
        upto = jnp.where(row_i <= col_i, 1.0, 0.0).astype(bf16)
        for i in range(2, 7):
            loads[i].wait()
        log_forget = -jnp.log1p(jnp.exp(-fg_ref[...]))
        ig = ig_ref[...]
        cum = left_dot(log_forget, upto, 1, 0)
        total = cum[:, T - 1 : T]
        weight_log = total - cum + ig
        peak = jnp.max(weight_log, axis=1, keepdims=True)
        weight = jnp.exp(weight_log - peak)
        scaled1, scaled2 = weight[0:1] * (KA ** -0.5), weight[1:2] * (KB ** -0.5)
        v1, v2 = v_ref[:, :DV], v_ref[:, DV:]
        k1, k2 = k1_ref[...], k2_ref[...]
        state = jnp.concatenate(
            [
                left_dot(jnp.transpose(k1.astype(f32)) * scaled1, v1, 1, 0),
                left_dot(k2.astype(f32) * scaled2, v2, 1, 0),
            ],
            axis=0,
        )
        n1 = left_dot(scaled1, k1, 1, 0)
        n2 = left_dot(scaled2, k2, 1, 1)
        n2 = jnp.concatenate([n2, jnp.zeros((1, KA - KB), f32)], axis=1)
        ones = jnp.ones((1, KA), f32)
        meta = jnp.concatenate(
            [n1, n2, total * ones, peak * ones, jnp.zeros((META - 6, KA), f32)], axis=0
        )
        for j in range(NY):
            st_send[j, :SH] = state[j * SH : (j + 1) * SH]
            st_send[j, SH:] = meta
        e1[pl.ds(iy, 1)] = st_send[pl.ds(iy, 1)]

    first_hop = Direct("y", NY, lambda j: st_send.at[j], e1, e1.at[0 : NY - 1], hop.at[0])
    first_hop.send()

    with scope("scores"):
        turned = jnp.transpose(jnp.concatenate([cum, cum, cum, cum], axis=0))
        causal = row_i >= col_i
        loads[7].wait()
        loads[8].wait()
        q1, q2 = q1_ref[...], jnp.transpose(q2_ref[...].astype(f32)).astype(bf16)
        local = []
        for h, (q, k, over, width, vh) in enumerate(((q1, k1, 1, KA, v1), (q2, k2, 0, KB, v2))):
            gaps = turned[:, h : h + 1] - cum[h : h + 1] + ig[h : h + 1]
            gaps = jnp.where(causal, gaps, -jnp.inf)
            top = jnp.max(gaps, axis=1, keepdims=True)
            scores = dg(q, k, 1, over) * (width ** -0.5)
            scores = scores * jnp.exp(gaps - top)
            local.append((top, left_dot(scores, vh, 1, 0), jnp.sum(scores, axis=1, keepdims=True)))

    stage(1)

    key_row = lax.broadcasted_iota(jnp.int32, (SH, KA), 0) + iy * SH

    def spread(both):
        return jnp.where(key_row < KA, both[0:1], both[1:2])

    def combine(early, late):
        decay_e, cell_e, norm_e, peak_e = early
        decay_l, cell_l, norm_l, peak_l = late
        moved = decay_l + peak_e
        ceiling = jnp.maximum(moved, peak_l)
        keep, fresh = jnp.exp(moved - ceiling), jnp.exp(peak_l - ceiling)
        return (
            decay_e + decay_l,
            spread(keep) * cell_e + spread(fresh) * cell_l,
            keep * norm_e + fresh * norm_l,
            ceiling,
        )

    def loaded(ref, j):
        return (ref[j, SH + 2 : SH + 4], ref[j, :SH], ref[j, SH : SH + 2], ref[j, SH + 4 : SH + 6])

    nothing = (
        jnp.zeros((2, KA), f32), jnp.zeros((SH, DV), f32), jnp.zeros((2, KA), f32),
        jnp.full((2, KA), NEG_BIG, f32),
    )
    stage(2)
    with scope("e1take"):
        first_hop.take()
    with scope("e1comb"):
        running, inside = nothing, []
        for j in range(NY):
            inside.append(running)
            running = combine(running, loaded(e1, j))
        e2_send[:SH] = running[1]
        e2_send[SH:] = jnp.concatenate(
            [running[2], running[0], running[3], jnp.zeros((META - 6, KA), f32)], axis=0
        )
        e2[pl.ds(iz, 1)] = e2_send[...][None]
    second_hop = Direct("z", NZ, lambda j: e2_send, e2, e2.at[0 : NZ - 1], hop.at[1])
    second_hop.send()
    stage(3)
    with scope("e2take"):
        second_hop.take()
    with scope("e2comb"):
        before = nothing
        for k in range(NZ):
            later = combine(before, loaded(e2, k))
            before = jax.tree.map(lambda new, old: jnp.where(k < iz, new, old), later, before)
        norm_in, peak_in = jnp.zeros((2, KA), f32), jnp.zeros((2, KA), f32)
        for j in range(NY):
            _, cell_j, norm_j, peak_j = combine(before, inside[j])
            f_send[j] = cell_j
            norm_in = jnp.where(iy == j, norm_j, norm_in)
            peak_in = jnp.where(iy == j, peak_j, peak_in)
        cin[pl.ds(iy, 1)] = f_send[pl.ds(iy, 1)]
    third_hop = Direct("y", NY, lambda j: f_send.at[j], cin, cin.at[0 : NY - 1], hop.at[2])
    third_hop.send()
    stage(4)
    stage(5, 0)
    with scope("e3take"):
        third_hop.take()

    with scope("cell"):
        for i in range(9, 15):
            loads[i].wait()
        cell_in = cin[...].reshape(KEYS, DV)
        columns = []
        for h, (q, width, cell) in enumerate(((q1, KA, cell_in[:KA]), (q2, KB, cell_in[KA:]))):
            top, own_num, own_den = local[h]
            carried = turned[:, h : h + 1] + peak_in[h : h + 1, 0:1]
            ceiling = jnp.maximum(carried, top)
            keep, fresh = jnp.exp(carried - ceiling), jnp.exp(top - ceiling)
            num = keep * right_dot(q, cell, 1, 0) + fresh * own_num
            den = keep * jnp.sum(q.astype(f32) * norm_in[h : h + 1, :width], axis=1, keepdims=True)
            den = den + fresh * own_den
            cell_out = num / jnp.maximum(jnp.abs(den), jnp.exp(-ceiling))
            center = jnp.mean(cell_out, -1, keepdims=True)
            away = cell_out - center
            var = jnp.mean(away * away, -1, keepdims=True)
            columns.append(away * lax.rsqrt(var + EPS))
        gate = 1.0 / (1.0 + jnp.exp(-og_ref[...].astype(f32)))
        mixed = (jnp.concatenate(columns, axis=1) * hg_ref[...] * gate).astype(bf16)
        wide = min(D, 512)
        for c in range(0, D, wide):
            part = dg(mixed, ow_ref[:, c : c + wide], 1, 0).astype(bf16)
            parts[:, :, :, c : c + wide] = part.reshape(X, 2, OWN, wide)
    out_proj = TpSum(X, parts, pair, chip_send, chip_recv, tsems.at[0])
    out_proj.start()
    stage(5, 1)
    with scope("rs1mid"):
        out_proj.between()
    stage(6)
    with scope("rs1take"):
        mixer = out_proj.total().astype(bf16).astype(f32)
    with scope("norm1"):
        first = normed(stream_own[...].astype(f32) + mixer, mg_ref[...]).astype(bf16)
        x_all[pl.ds(chip, 1), pl.ds(core, 1)] = first[None, None]
    rows_out = TpGather(X, x_all, tsems.at[1], rowsems)
    rows_out.start()
    stage(7)
    with scope("agrelay"):
        rows_out.relay()
    stage(8)
    with scope("agtake"):
        rows_out.take()
    with scope("upwait"):
        for item in ups:
            item.finish()
    with scope("mlp1"):
        wide_f = min(FD, 256)
        for c in range(0, FD, wide_f):
            x = x_all[...].reshape(T, D)
            w = up_all[:, :, :, c : c + wide_f].reshape(D, wide_f)
            act = jnp.maximum(dg(x, w, 1, 0), 0.0)
            hidden[:, c : c + wide_f] = (act * act).astype(bf16)

    wide_d = NY * RW

    def columns(shift):
        return lax.rem(iz + shift, NZ)

    def second(shift):
        w = down_all[pl.ds(columns(shift), 1)].reshape(wide_d, FD)
        return dg(hidden[...], w, 1, 1).astype(bf16)

    shifts = sorted(range(NZ), key=lambda s: min(s, NZ - s))
    early = early_blocks(NZ)
    sums = []
    later = NZ - 1 - early
    if early:
        with scope("mlp2a"):
            for i in range(early):
                shift = shifts[i]
                for item, axis in zip(downs, (1, 0)):
                    item.near(axis, min(shift, NZ - shift))
                parts_a[:, :, i] = second(shift).reshape(X, 2, OWN, wide_d)
        sums.append(TpSum(X, parts_a, pair_a, send_a, recv_a, tsems.at[2]))
        sums[-1].start()
    with scope("mlp2b"):
        for item, axis in zip(downs, (1, 0)):
            item.near(axis, NZ // 2 - 1)
        for i in range(later):
            parts_b[:, i] = second(shifts[early + i]).reshape(TP, OWN, wide_d)
    later_sum = Direct("tp", TP, lambda j: parts_b.at[j], recv_b, recv_b.at[0 : TP - 1], hop.at[4])
    later_sum.send()
    recv_b[pl.ds(it, 1)] = parts_b[pl.ds(it, 1)]
    with scope("downwait"):
        for item in downs:
            item.finish()
    with scope("mlp2 last"):
        last_parts[...] = second(shifts[-1]).reshape(TP, OWN, wide_d)
    last_sum = Direct("tp", TP, lambda j: last_parts.at[j], last_recv, last_recv.at[0 : TP - 1], hop.at[3])
    last_sum.send()
    with scope("rs2mid"):
        for item in sums:
            item.between()
    last_recv[pl.ds(it, 1)] = last_parts[pl.ds(it, 1)]
    with scope("drain"):
        for item in (first_hop, second_hop, third_hop, out_proj, rows_out, *ups, *downs):
            item.drain()

    def put(shift, value):
        mlp_sum[:, pl.ds(pl.multiple_of(columns(shift) * wide_d, wide_d), wide_d)] = value

    with scope("rs2take"):
        for item in sums:
            total_of = item.total()
            for i in range(early):
                put(shifts[i], total_of[i])
    with scope("rs2later"):
        later_sum.take()
        total_of = jnp.sum(recv_b[...].astype(f32), axis=0)
        for i in range(later):
            put(shifts[early + i], total_of[i])
    with scope("rs2last"):
        last_sum.take()
        put(shifts[-1], jnp.sum(last_recv[...].astype(f32), axis=0))
        mlp_out = mlp_sum[...].astype(bf16).astype(f32)
    with scope("norm2"):
        base = x_all[pl.ds(chip, 1), pl.ds(core, 1)].reshape(OWN, D).astype(f32)
        out_ref[...] = normed(base + mlp_out, outg_ref[...]).astype(bf16)
    with scope("lastdrain"):
        for item in (*sums, later_sum, last_sum):
            item.drain()


def layer(
    sizes, query_one, key_one, query_two, key_two, values, out_gate, in_gate, forget_gate,
    head_gain, out_weight, stream, mix_gain, up_weight, down_weight, out_gain,
):
    NZ, NY, TP = sizes
    X = TP // 2
    T, D = stream.shape
    OWN = T // TP
    RW, FD = up_weight.shape
    SH = (query_one.shape[1] + query_two.shape[1]) // NY
    KA = query_one.shape[1]
    sem = pltpu.SemaphoreType.DMA
    half = max(NY, NZ) // 2
    trees = 2 if NY == NZ else 4
    early = early_blocks(NZ)
    operands = (
        query_one, key_one, query_two.T, key_two.T, values, out_gate, in_gate, forget_gate,
        head_gain.reshape(1, -1), out_weight, stream, mix_gain.reshape(1, -1), up_weight,
        down_weight.T, out_gain.reshape(1, -1),
    )
    copied = [operands[i] for i in (0, 1, 2, 3, 4, 5, 6, 7, 8, 9, 11, 14)]

    def exchange(*inner):
        return [pltpu.VMEM((X, 2) + inner, bf16)] + [pltpu.VMEM((X,) + inner, bf16)] * 3

    return pl.pallas_call(
        functools.partial(kernel, sizes),
        out_shape=jax.ShapeDtypeStruct((OWN, D), bf16),
        in_specs=[pl.BlockSpec(memory_space=pltpu.HBM)] * len(operands),
        out_specs=pl.BlockSpec(memory_space=pltpu.VMEM),
        scratch_shapes=[pltpu.VMEM(a.shape, a.dtype) for a in copied]
        + [
            pltpu.VMEM((NZ, NY, RW, FD), bf16),
            pltpu.VMEM((NZ, NY, RW, FD), bf16),
            pltpu.VMEM((NY, SH + META, KA), f32),
            pltpu.VMEM((NY, SH + META, KA), f32),
            pltpu.VMEM((SH + META, KA), f32),
            pltpu.VMEM((NZ, SH + META, KA), f32),
            pltpu.VMEM((NY, SH, KA), f32),
            pltpu.VMEM((NY, SH, KA), f32),
        ]
        + exchange(OWN, D)
        + [pltpu.VMEM((X, 2, OWN, D), bf16), pltpu.VMEM((T, FD), bf16)]
        + exchange(max(early, 1), OWN, NY * RW)
        + [
            pltpu.VMEM((TP, NZ - 1 - early, OWN, NY * RW), bf16),
            pltpu.VMEM((TP, NZ - 1 - early, OWN, NY * RW), bf16),
            pltpu.VMEM((TP, OWN, NY * RW), bf16),
            pltpu.VMEM((TP, OWN, NY * RW), bf16),
            pltpu.VMEM((OWN, D), f32),
            pltpu.VMEM((OWN, D), bf16),
            sem((15,)),
            sem((5, 2)), sem((4, 2)), sem((trees, half)), sem((trees, half, half + 1)), sem((3, 4)), sem((X,)),
        ],
        compiler_params=pltpu.CompilerParams(
            collective_id=0, has_side_effects=True, vmem_limit_bytes=60000 * 1024
        ),
    )(*operands)


def build(mesh, nz, ny):
    tp = mesh.shape["tp"]
    split = Mesh(mesh.devices.reshape(nz, ny, tp), ("z", "y", "tp"))
    SP = ("z", "y")
    return jax.shard_map(
        functools.partial(layer, (nz, ny, tp)),
        mesh=split,
        in_specs=(
            P(SP, "tp"), P(SP, "tp"), P(SP, "tp"), P(SP, "tp"), P(SP, "tp"), P(SP, "tp"),
            P("tp", SP), P("tp", SP), P("tp"), P("tp", None), P(SP, None), P(),
            P(SP, "tp"), P("tp", SP), P(),
        ),
        out_specs=P(("z", "y", "tp"), None),
        check_vma=False,
    )


def solution(mesh):
    return build(mesh, 8, 8)
```

```python
import contextlib
import functools
import itertools

import jax
import jax.numpy as jnp
from jax import lax
from jax.experimental import pallas as pl
from jax.experimental.pallas import tpu as pltpu
from jax.sharding import Mesh
from jax.sharding import PartitionSpec as P

NEG_BIG = -1e30
EPS = 1e-05
META = 8
f32, bf16 = jnp.float32, jnp.bfloat16
MESH = pl.DeviceIdType.MESH
LATER = {
    0: ((1, 0),),
    1: ((1, 1),),
    4: ((1, 2), (1, 3), (1, 4), (2, 0)),
    5: ((2, 1), (2, 2), (2, 3), (3, 0)),
    6: ((2, 4), (3, 1), (3, 2), (4, 0)),
    7: ((3, 3), (3, 4), (4, 1), (4, 2)),
    8: ((4, 3), (4, 4)),
}
scope = contextlib.nullcontext


def dg(a, b, ca, cb):
    return lax.dot_general(a, b, (((ca,), (cb,)), ((), ())), preferred_element_type=f32)


def three(a):
    hi = a.astype(bf16)
    rest = a - hi.astype(f32)
    mid = rest.astype(bf16)
    return hi, mid, (rest - mid.astype(f32)).astype(bf16)


def left_dot(a, b, ca, cb):
    hi, mid, lo = three(a)
    return dg(hi, b, ca, cb) + (dg(mid, b, ca, cb) + dg(lo, b, ca, cb))


def right_dot(a, b, ca, cb):
    hi, mid, lo = three(b)
    return dg(a, hi, ca, cb) + (dg(a, mid, ca, cb) + dg(a, lo, ca, cb))


def remote(src, dst, ssem, rsem, target):
    return pltpu.make_async_remote_copy(
        src_ref=src, dst_ref=dst, send_sem=ssem, recv_sem=rsem, device_id=target, device_id_type=MESH
    )


class Gather:
    def __init__(self, axes, sizes, shard, spans, send_sems, first_recv, second_recv):
        self.axes, self.sizes, self.shard, self.spans = axes, sizes, shard, spans
        self.send_sems, self.first_recv, self.second_recv = send_sems, first_recv, second_recv
        self.me = [lax.axis_index(axis) for axis in axes]
        self.steps = [n // 2 for n in sizes]
        self.twins, self.waited = 1, set()

    def twin(self, other):
        if self.sizes == other.sizes:
            self.twins, self.first_recv, self.second_recv = 2, other.first_recv, other.second_recv
            other.twins, other.waited = 2, self.waited

    def at(self, axis, offset):
        return lax.rem(self.me[axis] + offset % self.sizes[axis], self.sizes[axis])

    def away(self, axis, way, distance):
        return self.at(axis, -distance if way == 0 else distance)

    def target(self, axis, way):
        return {self.axes[axis]: self.at(axis, 1 if way == 0 else -1)}

    def first_ways(self, step):
        return (0, 1) if step < self.steps[0] else (1,)

    def second_ways(self, step, r):
        if step < self.steps[1]:
            return (0, 1)
        return (0,) if r < (self.sizes[0] + 1) // 2 else (1,)

    def ranked(self, rank):
        return sorted({rank, (self.sizes[0] - rank) % self.sizes[0]})

    def send_first(self, step):
        if step <= self.steps[0]:
            for way in self.first_ways(step):
                ref = self.shard(self.away(0, way, step - 1), self.me[1])
                remote(ref, ref, self.send_sems.at[0], self.first_recv.at[step - 1], self.target(0, way)).start()

    def take_first(self, step):
        if step <= self.steps[0] and step not in self.waited:
            self.waited.add(step)
            ref = self.spans[0](self.twins * len(self.first_ways(step)))
            remote(ref, ref, self.send_sems.at[0], self.first_recv.at[step - 1], self.target(0, 0)).wait_recv()

    def send(self, step, rank):
        for r in self.ranked(rank):
            for way in self.second_ways(step, r):
                ref = self.shard(self.at(0, r), self.away(1, way, step - 1))
                remote(ref, ref, self.send_sems.at[1], self.second_recv.at[step - 1, rank],
                       self.target(1, way)).start()

    def take(self, step, rank):
        if (step, rank) not in self.waited:
            self.waited.add((step, rank))
            ref = self.spans[0](self.twins * sum(len(self.second_ways(step, r)) for r in self.ranked(rank)))
            remote(ref, ref, self.send_sems.at[1], self.second_recv.at[step - 1, rank],
                   self.target(1, 0)).wait_recv()

    def one(self, stage):
        if stage:
            self.take_first(stage)
        self.send_first(stage + 1)

    def further(self, step, rank):
        if step > 1:
            self.take(step - 1, rank)
        self.send(step, rank)

    def stage(self, stage, order=None):
        if order is None:
            order = [(step, stage - step + 1) for step in range(1, self.steps[1] + 1)]
        return [functools.partial(self.one, stage)] + [
            functools.partial(self.further, step, rank)
            for step, rank in order
            if step <= self.steps[1] and 0 <= rank <= self.steps[0]
        ]

    def finish(self):
        for step in range(1, self.steps[0] + 1):
            self.take_first(step)
        for step in range(1, self.steps[1] + 1):
            for rank in range(self.steps[0] + 1):
                self.take(step, rank)

    def near(self, axis, reach):
        for step in range(1, self.steps[0] + 1):
            if axis == 1 or step <= reach:
                self.take_first(step)
        for step in range(1, self.steps[1] + 1):
            for rank in range(self.steps[0] + 1):
                if (step if axis == 1 else rank) <= reach:
                    self.take(step, rank)

    def drain(self):
        for sem, ref in ((0, self.spans[1]), (1, self.spans[2])):
            remote(ref, ref, self.send_sems.at[sem], self.first_recv.at[0], self.target(0, 0)).wait_send()


class Direct:
    def __init__(self, axis, n, source, slots, span, sems):
        self.axis, self.n, self.source, self.slots, self.span, self.sems = axis, n, source, slots, span, sems
        self.me = lax.axis_index(axis)

    def send(self):
        for d in range(1, self.n):
            peer = lax.rem(self.me + d, self.n)
            remote(self.source(peer), self.slots.at[self.me], self.sems.at[0], self.sems.at[1],
                   {self.axis: peer}).start()

    def whole(self):
        return remote(self.span, self.span, self.sems.at[0], self.sems.at[1], {self.axis: lax.rem(self.me + 1, self.n)})

    def take(self):
        self.whole().wait_recv()

    def drain(self):
        self.whole().wait_send()


class TpSum:
    def __init__(self, chips, source, pair, chip_send, chip_recv, sems):
        self.chips, self.source, self.pair = chips, source, pair
        self.chip_send, self.chip_recv, self.sems = chip_send, chip_recv, sems
        it = lax.axis_index("tp")
        self.chip, self.core = lax.div(it, 2), lax.rem(it, 2)

    def inner(self):
        other = 1 - self.core
        return remote(self.source.at[:, other], self.pair, self.sems.at[0], self.sems.at[1],
                      {"tp": self.chip * 2 + other})

    def outer(self):
        ref = self.chip_recv.at[0 : self.chips - 1]
        peer = lax.rem(self.chip + 1, self.chips)
        return remote(ref, ref, self.sems.at[2], self.sems.at[3], {"tp": peer * 2 + self.core})

    def start(self):
        self.inner().start()

    def between(self):
        self.inner().wait_recv()
        mine = self.source[:, pl.ds(self.core, 1)].astype(f32)
        both = mine.reshape(self.pair.shape) + self.pair[...].astype(f32)
        self.chip_send[...] = both.astype(bf16)
        for d in range(1, self.chips):
            peer = lax.rem(self.chip + d, self.chips)
            remote(self.chip_send.at[peer], self.chip_recv.at[self.chip], self.sems.at[2], self.sems.at[3],
                   {"tp": peer * 2 + self.core}).start()
        self.chip_recv[pl.ds(self.chip, 1)] = self.chip_send[pl.ds(self.chip, 1)]

    def total(self):
        if self.chips > 1:
            self.outer().wait_recv()
        return jnp.sum(self.chip_recv[...].astype(f32), axis=0)

    def drain(self):
        self.inner().wait_send()
        if self.chips > 1:
            self.outer().wait_send()


class TpGather:
    def __init__(self, chips, slots, sems, chip_sems):
        self.chips, self.slots, self.sems, self.chip_sems = chips, slots, sems, chip_sems
        it = lax.axis_index("tp")
        self.chip, self.core = lax.div(it, 2), lax.rem(it, 2)

    def outer(self, d, ref):
        peer = lax.rem(self.chip + d, self.chips)
        return remote(ref, ref, self.sems.at[0], self.chip_sems.at[d], {"tp": peer * 2 + self.core})

    def inner(self, ref):
        return remote(ref, ref, self.sems.at[1], self.sems.at[2], {"tp": self.chip * 2 + 1 - self.core})

    def start(self):
        for d in range(1, self.chips):
            self.outer(d, self.slots.at[self.chip, self.core]).start()
        self.inner(self.slots.at[self.chip, self.core]).start()

    def relay(self):
        for d in sorted(range(1, self.chips), key=lambda d: min(d, self.chips - d)):
            ref = self.slots.at[lax.rem(self.chip + self.chips - d, self.chips), self.core]
            self.outer(d, ref).wait_recv()
            self.inner(ref).start()

    def take(self):
        self.inner(self.slots.at[:, 0]).wait_recv()

    def drain(self):
        if self.chips > 1:
            self.outer(1, self.slots.at[0 : self.chips - 1, 0]).wait_send()
        self.inner(self.slots.at[:, 0]).wait_send()


def normed(rows, gain):
    center = jnp.mean(rows, -1, keepdims=True)
    away = rows - center
    spread = jnp.mean(away * away, -1, keepdims=True)
    return away * lax.rsqrt(spread + EPS) * gain


def early_blocks(nz):
    return sum(min(s, nz - s) <= nz // 2 - 2 for s in range(nz))


def kernel(
    sizes,
    q1_hbm, k1_hbm, q2_hbm, k2_hbm, v_hbm, og_hbm, ig_hbm, fg_hbm, hg_hbm, ow_hbm,
    stream_ref, mg_hbm, up_ref, down_ref, outg_hbm,
    out_ref,
    q1_ref, k1_ref, q2_ref, k2_ref, v_ref, og_ref, ig_ref, fg_ref, hg_ref, ow_ref, mg_ref, outg_ref,
    up_all, down_all, st_send, e1, e2_send, e2, f_send, cin,
    parts, pair, chip_send, chip_recv, x_all, hidden, parts_a, pair_a, send_a, recv_a, parts_b, recv_b, last_parts, last_recv, mlp_sum, stream_own,
    local_sem, hop, gsend, g1recv, g2recv, tsems, rowsems,
):
    NZ, NY, TP = sizes
    X = TP // 2
    iz, iy, it = lax.axis_index("z"), lax.axis_index("y"), lax.axis_index("tp")
    chip, core = lax.div(it, 2), lax.rem(it, 2)
    T, KA = q1_ref.shape
    KB = k2_ref.shape[0]
    DV = v_ref.shape[1] // 2
    KEYS = KA + KB
    SH = KEYS // NY
    OWN = T // TP
    D = ow_ref.shape[1]
    RW, FD = up_ref.shape

    barrier = pltpu.get_barrier_semaphore()
    peers = 0
    greeted = [{axis: lax.rem(lax.axis_index(axis) + d, n)} for axis, n in (("y", NY), ("z", NZ)) for d in range(1, n)]
    greeted += [{"tp": lax.rem(it + d, TP)} for d in range(1, TP)]
    for peer in greeted:
        pl.semaphore_signal(barrier, inc=1, device_id=peer, device_id_type=MESH)

    loads = []
    for src, dst in (
        (up_ref, up_all.at[iz, iy]), (down_ref, down_all.at[iz, iy]),
        (fg_hbm, fg_ref), (ig_hbm, ig_ref), (k1_hbm, k1_ref), (k2_hbm, k2_ref), (v_hbm, v_ref),
        (q1_hbm, q1_ref), (q2_hbm, q2_ref), (og_hbm, og_ref), (hg_hbm, hg_ref), (ow_hbm, ow_ref),
        (stream_ref.at[pl.ds(pl.multiple_of(it * OWN, OWN), OWN), :], stream_own),
        (mg_hbm, mg_ref), (outg_hbm, outg_ref),
    ):
        copy = pltpu.make_async_copy(src, dst, local_sem.at[len(loads)])
        copy.start()
        loads.append(copy)

    half = RW // 2
    HALVES = 1 if NY == NZ else 2

    def gather(weights, low, sems, first_recv, second_recv):
        part = slice(0, half) if low else slice(half, RW)
        if low:
            axes, sizes = ("y", "z"), (NY, NZ)
            shard = lambda a, b: weights.at[b, a, part]
            spans = (lambda n: weights.at[0 : -(-n // NY), 0 : min(n, NY), part],
                     weights.at[0, 0 : NY - 1, part], weights.at[0 : NZ - 1, :, part])
        else:
            axes, sizes = ("z", "y"), (NZ, NY)
            shard = lambda a, b: weights.at[a, b, part]
            spans = (lambda n: weights.at[0 : -(-n // NY), 0 : min(n, NY), part],
                     weights.at[0 : NZ - 1, 0, part], weights.at[:, 0 : NY - 1, part])
        return Gather(axes, sizes, shard, spans, sems, first_recv, second_recv)

    ups = [gather(up_all, i == 0, gsend.at[i], g1recv.at[i % HALVES], g2recv.at[i % HALVES]) for i in range(2)]
    downs = [gather(down_all, i == 0, gsend.at[2 + i], g1recv.at[HALVES + i % HALVES], g2recv.at[HALVES + i % HALVES]) for i in range(2)]

    for low, high in (ups, downs):
        low.twin(high)

    def stage(number, part=None):
        lists = [item.stage(number) for item in ups] + [item.stage(number, LATER.get(number, ())) for item in downs]
        rows = list(itertools.zip_longest(*lists))
        cut = (len(rows) + 1) // 2 if number < 7 else len(rows) - 1
        with scope(f"stage{number}{part}"):
            for row in rows[:cut] if part == 0 else rows[cut:] if part == 1 else rows:
                for action in row:
                    if action is not None:
                        action()

    loads[0].wait()
    loads[1].wait()
    with scope("barrier"):
        pl.semaphore_wait(barrier, len(greeted))
    stage(0)

    with scope("local"):
        row_i = lax.broadcasted_iota(jnp.int32, (T, T), 0)
        col_i = lax.broadcasted_iota(jnp.int32, (T, T), 1)
        upto = jnp.where(row_i <= col_i, 1.0, 0.0).astype(bf16)
        for i in range(2, 7):
            loads[i].wait()
        log_forget = -jnp.log1p(jnp.exp(-fg_ref[...]))
        ig = ig_ref[...]
        cum = left_dot(log_forget, upto, 1, 0)
        total = cum[:, T - 1 : T]
        weight_log = total - cum + ig
        peak = jnp.max(weight_log, axis=1, keepdims=True)
        weight = jnp.exp(weight_log - peak)
        scaled1, scaled2 = weight[0:1] * (KA ** -0.5), weight[1:2] * (KB ** -0.5)
        v1, v2 = v_ref[:, :DV], v_ref[:, DV:]
        k1, k2 = k1_ref[...], k2_ref[...]
        state = jnp.concatenate(
            [
                left_dot(jnp.transpose(k1.astype(f32)) * scaled1, v1, 1, 0),
                left_dot(k2.astype(f32) * scaled2, v2, 1, 0),
            ],
            axis=0,
        )
        n1 = left_dot(scaled1, k1, 1, 0)
        n2 = left_dot(scaled2, k2, 1, 1)
        n2 = jnp.concatenate([n2, jnp.zeros((1, KA - KB), f32)], axis=1)
        ones = jnp.ones((1, KA), f32)
        meta = jnp.concatenate(
            [n1, n2, total * ones, peak * ones, jnp.zeros((META - 6, KA), f32)], axis=0
        )
        for j in range(NY):
            st_send[j, :SH] = state[j * SH : (j + 1) * SH]
            st_send[j, SH:] = meta
        e1[pl.ds(iy, 1)] = st_send[pl.ds(iy, 1)]

    first_hop = Direct("y", NY, lambda j: st_send.at[j], e1, e1.at[0 : NY - 1], hop.at[0])
    first_hop.send()

    with scope("scores"):
        turned = jnp.transpose(jnp.concatenate([cum, cum, cum, cum], axis=0))
        causal = row_i >= col_i
        loads[7].wait()
        loads[8].wait()
        q1, q2 = q1_ref[...], jnp.transpose(q2_ref[...].astype(f32)).astype(bf16)
        local = []
        for h, (q, k, over, width, vh) in enumerate(((q1, k1, 1, KA, v1), (q2, k2, 0, KB, v2))):
            gaps = turned[:, h : h + 1] - cum[h : h + 1] + ig[h : h + 1]
            gaps = jnp.where(causal, gaps, -jnp.inf)
            top = jnp.max(gaps, axis=1, keepdims=True)
            scores = dg(q, k, 1, over) * (width ** -0.5)
            scores = scores * jnp.exp(gaps - top)
            local.append((top, left_dot(scores, vh, 1, 0), jnp.sum(scores, axis=1, keepdims=True)))

    stage(1)

    key_row = lax.broadcasted_iota(jnp.int32, (SH, KA), 0) + iy * SH

    def spread(both):
        return jnp.where(key_row < KA, both[0:1], both[1:2])

    def combine(early, late):
        decay_e, cell_e, norm_e, peak_e = early
        decay_l, cell_l, norm_l, peak_l = late
        moved = decay_l + peak_e
        ceiling = jnp.maximum(moved, peak_l)
        keep, fresh = jnp.exp(moved - ceiling), jnp.exp(peak_l - ceiling)
        return (
            decay_e + decay_l,
            spread(keep) * cell_e + spread(fresh) * cell_l,
            keep * norm_e + fresh * norm_l,
            ceiling,
        )

    def loaded(ref, j):
        return (ref[j, SH + 2 : SH + 4], ref[j, :SH], ref[j, SH : SH + 2], ref[j, SH + 4 : SH + 6])

    nothing = (
        jnp.zeros((2, KA), f32), jnp.zeros((SH, DV), f32), jnp.zeros((2, KA), f32),
        jnp.full((2, KA), NEG_BIG, f32),
    )
    stage(2)
    with scope("e1take"):
        first_hop.take()
    with scope("e1comb"):
        running, inside = nothing, []
        for j in range(NY):
            inside.append(running)
            running = combine(running, loaded(e1, j))
        e2_send[:SH] = running[1]
        e2_send[SH:] = jnp.concatenate(
            [running[2], running[0], running[3], jnp.zeros((META - 6, KA), f32)], axis=0
        )
        e2[pl.ds(iz, 1)] = e2_send[...][None]
    second_hop = Direct("z", NZ, lambda j: e2_send, e2, e2.at[0 : NZ - 1], hop.at[1])
    second_hop.send()
    stage(3)
    with scope("e2take"):
        second_hop.take()
    with scope("e2comb"):
        before = nothing
        for k in range(NZ):
            later = combine(before, loaded(e2, k))
            before = jax.tree.map(lambda new, old: jnp.where(k < iz, new, old), later, before)
        norm_in, peak_in = jnp.zeros((2, KA), f32), jnp.zeros((2, KA), f32)
        for j in range(NY):
            _, cell_j, norm_j, peak_j = combine(before, inside[j])
            f_send[j] = cell_j
            norm_in = jnp.where(iy == j, norm_j, norm_in)
            peak_in = jnp.where(iy == j, peak_j, peak_in)
        cin[pl.ds(iy, 1)] = f_send[pl.ds(iy, 1)]
    third_hop = Direct("y", NY, lambda j: f_send.at[j], cin, cin.at[0 : NY - 1], hop.at[2])
    third_hop.send()
    stage(4)
    stage(5, 0)
    with scope("e3take"):
        third_hop.take()

    with scope("cell"):
        for i in range(9, 15):
            loads[i].wait()
        cell_in = cin[...].reshape(KEYS, DV)
        columns = []
        for h, (q, width, cell) in enumerate(((q1, KA, cell_in[:KA]), (q2, KB, cell_in[KA:]))):
            top, own_num, own_den = local[h]
            carried = turned[:, h : h + 1] + peak_in[h : h + 1, 0:1]
            ceiling = jnp.maximum(carried, top)
            keep, fresh = jnp.exp(carried - ceiling), jnp.exp(top - ceiling)
            num = keep * right_dot(q, cell, 1, 0) + fresh * own_num
            den = keep * jnp.sum(q.astype(f32) * norm_in[h : h + 1, :width], axis=1, keepdims=True)
            den = den + fresh * own_den
            cell_out = num / jnp.maximum(jnp.abs(den), jnp.exp(-ceiling))
            center = jnp.mean(cell_out, -1, keepdims=True)
            away = cell_out - center
            var = jnp.mean(away * away, -1, keepdims=True)
            columns.append(away * lax.rsqrt(var + EPS))
        gate = 1.0 / (1.0 + jnp.exp(-og_ref[...].astype(f32)))
        mixed = (jnp.concatenate(columns, axis=1) * hg_ref[...] * gate).astype(bf16)
        wide = min(D, 512)
        for c in range(0, D, wide):
            part = dg(mixed, ow_ref[:, c : c + wide], 1, 0).astype(bf16)
            parts[:, :, :, c : c + wide] = part.reshape(X, 2, OWN, wide)
    out_proj = TpSum(X, parts, pair, chip_send, chip_recv, tsems.at[0])
    out_proj.start()
    stage(5, 1)
    with scope("rs1mid"):
        out_proj.between()
    stage(6)
    with scope("rs1take"):
        mixer = out_proj.total().astype(bf16).astype(f32)
    with scope("norm1"):
        first = normed(stream_own[...].astype(f32) + mixer, mg_ref[...]).astype(bf16)
        x_all[pl.ds(chip, 1), pl.ds(core, 1)] = first[None, None]
    rows_out = TpGather(X, x_all, tsems.at[1], rowsems)
    rows_out.start()
    stage(7, 0)
    with scope("agrelay"):
        rows_out.relay()
    stage(7, 1)
    stage(8)
    with scope("agtake"):
        rows_out.take()
    with scope("upwait"):
        for item in ups:
            item.finish()
    with scope("mlp1"):
        wide_f = min(FD, 256)
        for c in range(0, FD, wide_f):
            x = x_all[...].reshape(T, D)
            w = up_all[:, :, :, c : c + wide_f].reshape(D, wide_f)
            act = jnp.maximum(dg(x, w, 1, 0), 0.0)
            hidden[:, c : c + wide_f] = (act * act).astype(bf16)

    wide_d = NY * RW

    def columns(shift):
        return lax.rem(iz + shift, NZ)

    def second(shift):
        w = down_all[pl.ds(columns(shift), 1)].reshape(wide_d, FD)
        return dg(hidden[...], w, 1, 1).astype(bf16)

    shifts = sorted(range(NZ), key=lambda s: min(s, NZ - s))
    early = early_blocks(NZ)
    sums = []
    later = NZ - 1 - early
    if early:
        with scope("mlp2a"):
            for i in range(early):
                shift = shifts[i]
                for item, axis in zip(downs, (1, 0)):
                    item.near(axis, min(shift, NZ - shift))
                parts_a[:, :, i] = second(shift).reshape(X, 2, OWN, wide_d)
        sums.append(TpSum(X, parts_a, pair_a, send_a, recv_a, tsems.at[2]))
        sums[-1].start()
    with scope("mlp2b"):
        for item, axis in zip(downs, (1, 0)):
            item.near(axis, NZ // 2 - 1)
        for i in range(later):
            parts_b[:, i] = second(shifts[early + i]).reshape(TP, OWN, wide_d)
    later_sum = Direct("tp", TP, lambda j: parts_b.at[j], recv_b, recv_b.at[0 : TP - 1], hop.at[4])
    later_sum.send()
    recv_b[pl.ds(it, 1)] = parts_b[pl.ds(it, 1)]
    with scope("downwait"):
        for item in downs:
            item.finish()
    with scope("mlp2 last"):
        last_parts[...] = second(shifts[-1]).reshape(TP, OWN, wide_d)
    last_sum = Direct("tp", TP, lambda j: last_parts.at[j], last_recv, last_recv.at[0 : TP - 1], hop.at[3])
    last_sum.send()
    with scope("rs2mid"):
        for item in sums:
            item.between()
    last_recv[pl.ds(it, 1)] = last_parts[pl.ds(it, 1)]
    with scope("drain"):
        for item in (first_hop, second_hop, third_hop, out_proj, rows_out, *ups, *downs):
            item.drain()

    def put(shift, value):
        mlp_sum[:, pl.ds(pl.multiple_of(columns(shift) * wide_d, wide_d), wide_d)] = value

    with scope("rs2take"):
        for item in sums:
            total_of = item.total()
            for i in range(early):
                put(shifts[i], total_of[i])
    with scope("rs2later"):
        later_sum.take()
        total_of = jnp.sum(recv_b[...].astype(f32), axis=0)
        for i in range(later):
            put(shifts[early + i], total_of[i])
    with scope("rs2last"):
        last_sum.take()
        put(shifts[-1], jnp.sum(last_recv[...].astype(f32), axis=0))
        mlp_out = mlp_sum[...].astype(bf16).astype(f32)
    with scope("norm2"):
        base = x_all[pl.ds(chip, 1), pl.ds(core, 1)].reshape(OWN, D).astype(f32)
        out_ref[...] = normed(base + mlp_out, outg_ref[...]).astype(bf16)
    with scope("lastdrain"):
        for item in (*sums, later_sum, last_sum):
            item.drain()


def layer(
    sizes, query_one, key_one, query_two, key_two, values, out_gate, in_gate, forget_gate,
    head_gain, out_weight, stream, mix_gain, up_weight, down_weight, out_gain,
):
    NZ, NY, TP = sizes
    X = TP // 2
    T, D = stream.shape
    OWN = T // TP
    RW, FD = up_weight.shape
    SH = (query_one.shape[1] + query_two.shape[1]) // NY
    KA = query_one.shape[1]
    sem = pltpu.SemaphoreType.DMA
    half = max(NY, NZ) // 2
    trees = 2 if NY == NZ else 4
    early = early_blocks(NZ)
    operands = (
        query_one, key_one, query_two.T, key_two.T, values, out_gate, in_gate, forget_gate,
        head_gain.reshape(1, -1), out_weight, stream, mix_gain.reshape(1, -1), up_weight,
        down_weight.T, out_gain.reshape(1, -1),
    )
    copied = [operands[i] for i in (0, 1, 2, 3, 4, 5, 6, 7, 8, 9, 11, 14)]

    def exchange(*inner):
        return [pltpu.VMEM((X, 2) + inner, bf16)] + [pltpu.VMEM((X,) + inner, bf16)] * 3

    return pl.pallas_call(
        functools.partial(kernel, sizes),
        out_shape=jax.ShapeDtypeStruct((OWN, D), bf16),
        in_specs=[pl.BlockSpec(memory_space=pltpu.HBM)] * len(operands),
        out_specs=pl.BlockSpec(memory_space=pltpu.VMEM),
        scratch_shapes=[pltpu.VMEM(a.shape, a.dtype) for a in copied]
        + [
            pltpu.VMEM((NZ, NY, RW, FD), bf16),
            pltpu.VMEM((NZ, NY, RW, FD), bf16),
            pltpu.VMEM((NY, SH + META, KA), f32),
            pltpu.VMEM((NY, SH + META, KA), f32),
            pltpu.VMEM((SH + META, KA), f32),
            pltpu.VMEM((NZ, SH + META, KA), f32),
            pltpu.VMEM((NY, SH, KA), f32),
            pltpu.VMEM((NY, SH, KA), f32),
        ]
        + exchange(OWN, D)
        + [pltpu.VMEM((X, 2, OWN, D), bf16), pltpu.VMEM((T, FD), bf16)]
        + exchange(max(early, 1), OWN, NY * RW)
        + [
            pltpu.VMEM((TP, NZ - 1 - early, OWN, NY * RW), bf16),
            pltpu.VMEM((TP, NZ - 1 - early, OWN, NY * RW), bf16),
            pltpu.VMEM((TP, OWN, NY * RW), bf16),
            pltpu.VMEM((TP, OWN, NY * RW), bf16),
            pltpu.VMEM((OWN, D), f32),
            pltpu.VMEM((OWN, D), bf16),
            sem((15,)),
            sem((5, 2)), sem((4, 2)), sem((trees, half)), sem((trees, half, half + 1)), sem((3, 4)), sem((X,)),
        ],
        compiler_params=pltpu.CompilerParams(
            collective_id=0, has_side_effects=True, vmem_limit_bytes=60000 * 1024
        ),
    )(*operands)


def build(mesh, nz, ny):
    tp = mesh.shape["tp"]
    split = Mesh(mesh.devices.reshape(nz, ny, tp), ("z", "y", "tp"))
    SP = ("z", "y")
    return jax.shard_map(
        functools.partial(layer, (nz, ny, tp)),
        mesh=split,
        in_specs=(
            P(SP, "tp"), P(SP, "tp"), P(SP, "tp"), P(SP, "tp"), P(SP, "tp"), P(SP, "tp"),
            P("tp", SP), P("tp", SP), P("tp"), P("tp", None), P(SP, None), P(),
            P(SP, "tp"), P("tp", SP), P(),
        ),
        out_specs=P(("z", "y", "tp"), None),
        check_vma=False,
    )


def solution(mesh):
    return build(mesh, 8, 8)
```

```python
import contextlib
import functools
import itertools

import jax
import jax.numpy as jnp
from jax import lax
from jax.experimental import pallas as pl
from jax.experimental.pallas import tpu as pltpu
from jax.sharding import Mesh
from jax.sharding import PartitionSpec as P

NEG_BIG = -1e30
EPS = 1e-05
META = 8
f32, bf16 = jnp.float32, jnp.bfloat16
MESH = pl.DeviceIdType.MESH
LATER = {
    0: ((1, 0),),
    1: ((1, 1),),
    4: ((1, 2), (1, 3), (1, 4), (2, 0)),
    5: ((2, 1), (2, 2), (2, 3), (3, 0)),
    6: ((2, 4), (3, 1), (3, 2), (4, 0)),
    7: ((3, 3), (3, 4), (4, 1), (4, 2)),
    8: ((4, 3), (4, 4)),
}
scope = contextlib.nullcontext


def dg(a, b, ca, cb):
    return lax.dot_general(a, b, (((ca,), (cb,)), ((), ())), preferred_element_type=f32)


def three(a):
    hi = a.astype(bf16)
    rest = a - hi.astype(f32)
    mid = rest.astype(bf16)
    return hi, mid, (rest - mid.astype(f32)).astype(bf16)


def left_dot(a, b, ca, cb):
    hi, mid, lo = three(a)
    return dg(hi, b, ca, cb) + (dg(mid, b, ca, cb) + dg(lo, b, ca, cb))


def right_dot(a, b, ca, cb):
    hi, mid, lo = three(b)
    return dg(a, hi, ca, cb) + (dg(a, mid, ca, cb) + dg(a, lo, ca, cb))


def remote(src, dst, ssem, rsem, target):
    return pltpu.make_async_remote_copy(
        src_ref=src, dst_ref=dst, send_sem=ssem, recv_sem=rsem, device_id=target, device_id_type=MESH
    )


class Gather:
    def __init__(self, axes, sizes, shard, spans, send_sems, first_recv, second_recv):
        self.axes, self.sizes, self.shard, self.spans = axes, sizes, shard, spans
        self.send_sems, self.first_recv, self.second_recv = send_sems, first_recv, second_recv
        self.me = [lax.axis_index(axis) for axis in axes]
        self.steps = [n // 2 for n in sizes]
        self.twins, self.waited = 1, set()

    def twin(self, other):
        if self.sizes == other.sizes:
            self.twins, self.first_recv, self.second_recv = 2, other.first_recv, other.second_recv
            other.twins, other.waited = 2, self.waited

    def at(self, axis, offset):
        return lax.rem(self.me[axis] + offset % self.sizes[axis], self.sizes[axis])

    def away(self, axis, way, distance):
        return self.at(axis, -distance if way == 0 else distance)

    def target(self, axis, way):
        return {self.axes[axis]: self.at(axis, 1 if way == 0 else -1)}

    def first_ways(self, step):
        return (0, 1) if step < self.steps[0] else (1,)

    def second_ways(self, step, r):
        if step < self.steps[1]:
            return (0, 1)
        return (0,) if r < (self.sizes[0] + 1) // 2 else (1,)

    def ranked(self, rank):
        return sorted({rank, (self.sizes[0] - rank) % self.sizes[0]})

    def send_first(self, step):
        if step <= self.steps[0]:
            for way in self.first_ways(step):
                ref = self.shard(self.away(0, way, step - 1), self.me[1])
                remote(ref, ref, self.send_sems.at[0], self.first_recv.at[step - 1], self.target(0, way)).start()

    def take_first(self, step):
        if step <= self.steps[0] and step not in self.waited:
            self.waited.add(step)
            ref = self.spans[0](self.twins * len(self.first_ways(step)))
            remote(ref, ref, self.send_sems.at[0], self.first_recv.at[step - 1], self.target(0, 0)).wait_recv()

    def send(self, step, rank):
        for r in self.ranked(rank):
            for way in self.second_ways(step, r):
                ref = self.shard(self.at(0, r), self.away(1, way, step - 1))
                remote(ref, ref, self.send_sems.at[1], self.second_recv.at[step - 1, rank],
                       self.target(1, way)).start()

    def take(self, step, rank):
        if (step, rank) not in self.waited:
            self.waited.add((step, rank))
            ref = self.spans[0](self.twins * sum(len(self.second_ways(step, r)) for r in self.ranked(rank)))
            remote(ref, ref, self.send_sems.at[1], self.second_recv.at[step - 1, rank],
                   self.target(1, 0)).wait_recv()

    def one(self, stage):
        if stage:
            self.take_first(stage)
        self.send_first(stage + 1)

    def further(self, step, rank):
        if step > 1:
            self.take(step - 1, rank)
        self.send(step, rank)

    def stage(self, stage, order=None):
        if order is None:
            order = [(step, stage - step + 1) for step in range(1, self.steps[1] + 1)]
        return [functools.partial(self.one, stage)] + [
            functools.partial(self.further, step, rank)
            for step, rank in order
            if step <= self.steps[1] and 0 <= rank <= self.steps[0]
        ]

    def finish(self):
        for step in range(1, self.steps[0] + 1):
            self.take_first(step)
        for step in range(1, self.steps[1] + 1):
            for rank in range(self.steps[0] + 1):
                self.take(step, rank)

    def near(self, axis, reach):
        for step in range(1, self.steps[0] + 1):
            if axis == 1 or step <= reach:
                self.take_first(step)
        for step in range(1, self.steps[1] + 1):
            for rank in range(self.steps[0] + 1):
                if (step if axis == 1 else rank) <= reach:
                    self.take(step, rank)

    def drain(self):
        for sem, ref in ((0, self.spans[1]), (1, self.spans[2])):
            remote(ref, ref, self.send_sems.at[sem], self.first_recv.at[0], self.target(0, 0)).wait_send()


class Direct:
    def __init__(self, axis, n, source, slots, span, sems):
        self.axis, self.n, self.source, self.slots, self.span, self.sems = axis, n, source, slots, span, sems
        self.me = lax.axis_index(axis)

    def send(self):
        for d in range(1, self.n):
            peer = lax.rem(self.me + d, self.n)
            remote(self.source(peer), self.slots.at[self.me], self.sems.at[0], self.sems.at[1],
                   {self.axis: peer}).start()

    def whole(self):
        return remote(self.span, self.span, self.sems.at[0], self.sems.at[1], {self.axis: lax.rem(self.me + 1, self.n)})

    def take(self):
        self.whole().wait_recv()

    def drain(self):
        self.whole().wait_send()


class TpSum:
    def __init__(self, chips, source, pair, chip_send, chip_recv, sems):
        self.chips, self.source, self.pair = chips, source, pair
        self.chip_send, self.chip_recv, self.sems = chip_send, chip_recv, sems
        it = lax.axis_index("tp")
        self.chip, self.core = lax.div(it, 2), lax.rem(it, 2)

    def inner(self):
        other = 1 - self.core
        return remote(self.source.at[:, other], self.pair, self.sems.at[0], self.sems.at[1],
                      {"tp": self.chip * 2 + other})

    def outer(self):
        ref = self.chip_recv.at[0 : self.chips - 1]
        peer = lax.rem(self.chip + 1, self.chips)
        return remote(ref, ref, self.sems.at[2], self.sems.at[3], {"tp": peer * 2 + self.core})

    def start(self):
        self.inner().start()

    def between(self):
        self.inner().wait_recv()
        mine = self.source[:, pl.ds(self.core, 1)].astype(f32)
        both = mine.reshape(self.pair.shape) + self.pair[...].astype(f32)
        self.chip_send[...] = both.astype(bf16)
        for d in range(1, self.chips):
            peer = lax.rem(self.chip + d, self.chips)
            remote(self.chip_send.at[peer], self.chip_recv.at[self.chip], self.sems.at[2], self.sems.at[3],
                   {"tp": peer * 2 + self.core}).start()
        self.chip_recv[pl.ds(self.chip, 1)] = self.chip_send[pl.ds(self.chip, 1)]

    def total(self):
        if self.chips > 1:
            self.outer().wait_recv()
        return jnp.sum(self.chip_recv[...].astype(f32), axis=0)

    def drain(self):
        self.inner().wait_send()
        if self.chips > 1:
            self.outer().wait_send()


class TpGather:
    def __init__(self, chips, slots, sems, chip_sems):
        self.chips, self.slots, self.sems, self.chip_sems = chips, slots, sems, chip_sems
        it = lax.axis_index("tp")
        self.chip, self.core = lax.div(it, 2), lax.rem(it, 2)

    def outer(self, d, ref):
        peer = lax.rem(self.chip + d, self.chips)
        return remote(ref, ref, self.sems.at[0], self.chip_sems.at[d], {"tp": peer * 2 + self.core})

    def inner(self, ref):
        return remote(ref, ref, self.sems.at[1], self.sems.at[2], {"tp": self.chip * 2 + 1 - self.core})

    def start(self):
        for d in range(1, self.chips):
            self.outer(d, self.slots.at[self.chip, self.core]).start()
        self.inner(self.slots.at[self.chip, self.core]).start()

    def relay(self):
        for d in sorted(range(1, self.chips), key=lambda d: min(d, self.chips - d)):
            ref = self.slots.at[lax.rem(self.chip + self.chips - d, self.chips), self.core]
            self.outer(d, ref).wait_recv()
            self.inner(ref).start()

    def take(self):
        self.inner(self.slots.at[:, 0]).wait_recv()

    def drain(self):
        if self.chips > 1:
            self.outer(1, self.slots.at[0 : self.chips - 1, 0]).wait_send()
        self.inner(self.slots.at[:, 0]).wait_send()


def normed(rows, gain):
    center = jnp.mean(rows, -1, keepdims=True)
    away = rows - center
    spread = jnp.mean(away * away, -1, keepdims=True)
    return away * lax.rsqrt(spread + EPS) * gain


def early_blocks(nz):
    return sum(min(s, nz - s) <= nz // 2 - 2 for s in range(nz))


def kernel(
    sizes,
    q1_hbm, k1_hbm, q2_hbm, k2_hbm, v_hbm, og_hbm, ig_hbm, fg_hbm, hg_hbm, ow_hbm,
    stream_ref, mg_hbm, up_ref, down_ref, outg_hbm,
    out_ref,
    q1_ref, k1_ref, q2_ref, k2_ref, v_ref, og_ref, ig_ref, fg_ref, hg_ref, ow_ref, mg_ref, outg_ref,
    up_all, down_all, st_send, e1, e2_send, e2, f_send, cin,
    parts, pair, chip_send, chip_recv, x_all, hidden, parts_a, pair_a, send_a, recv_a, parts_b, recv_b, last_parts, last_recv, mlp_sum, stream_own,
    local_sem, hop, gsend, g1recv, g2recv, tsems, rowsems,
):
    NZ, NY, TP = sizes
    X = TP // 2
    iz, iy, it = lax.axis_index("z"), lax.axis_index("y"), lax.axis_index("tp")
    chip, core = lax.div(it, 2), lax.rem(it, 2)
    T, KA = q1_ref.shape
    KB = k2_ref.shape[0]
    DV = v_ref.shape[1] // 2
    KEYS = KA + KB
    SH = KEYS // NY
    OWN = T // TP
    D = ow_ref.shape[1]
    RW, FD = up_ref.shape

    barrier = pltpu.get_barrier_semaphore()
    peers = 0
    greeted = [{axis: lax.rem(lax.axis_index(axis) + d, n)} for axis, n in (("y", NY), ("z", NZ)) for d in range(1, n)]
    greeted += [{"tp": lax.rem(it + d, TP)} for d in range(1, TP)]
    for peer in greeted:
        pl.semaphore_signal(barrier, inc=1, device_id=peer, device_id_type=MESH)

    loads = []
    for src, dst in (
        (up_ref, up_all.at[iz, iy]), (down_ref, down_all.at[iz, iy]),
        (fg_hbm, fg_ref), (ig_hbm, ig_ref), (k1_hbm, k1_ref), (k2_hbm, k2_ref), (v_hbm, v_ref),
        (q1_hbm, q1_ref), (q2_hbm, q2_ref), (og_hbm, og_ref), (hg_hbm, hg_ref), (ow_hbm, ow_ref),
        (stream_ref.at[pl.ds(pl.multiple_of(it * OWN, OWN), OWN), :], stream_own),
        (mg_hbm, mg_ref), (outg_hbm, outg_ref),
    ):
        copy = pltpu.make_async_copy(src, dst, local_sem.at[len(loads)])
        copy.start()
        loads.append(copy)

    half = RW // 2
    HALVES = 1 if NY == NZ else 2

    def gather(weights, low, sems, first_recv, second_recv):
        part = slice(0, half) if low else slice(half, RW)
        if low:
            axes, sizes = ("y", "z"), (NY, NZ)
            shard = lambda a, b: weights.at[b, a, part]
            spans = (lambda n: weights.at[0 : -(-n // NY), 0 : min(n, NY), part],
                     weights.at[0, 0 : NY - 1, part], weights.at[0 : NZ - 1, :, part])
        else:
            axes, sizes = ("z", "y"), (NZ, NY)
            shard = lambda a, b: weights.at[a, b, part]
            spans = (lambda n: weights.at[0 : -(-n // NY), 0 : min(n, NY), part],
                     weights.at[0 : NZ - 1, 0, part], weights.at[:, 0 : NY - 1, part])
        return Gather(axes, sizes, shard, spans, sems, first_recv, second_recv)

    ups = [gather(up_all, i == 0, gsend.at[i], g1recv.at[i % HALVES], g2recv.at[i % HALVES]) for i in range(2)]
    downs = [gather(down_all, i == 0, gsend.at[2 + i], g1recv.at[HALVES + i % HALVES], g2recv.at[HALVES + i % HALVES]) for i in range(2)]

    for low, high in (ups, downs):
        low.twin(high)

    def stage(number, part=None):
        lists = [item.stage(number) for item in ups] + [item.stage(number, LATER.get(number, ())) for item in downs]
        rows = list(itertools.zip_longest(*lists))
        cut = (len(rows) + 1) // 2
        with scope(f"stage{number}{part}"):
            for row in rows[:cut] if part == 0 else rows[cut:] if part == 1 else rows:
                for action in row:
                    if action is not None:
                        action()

    loads[0].wait()
    loads[1].wait()
    with scope("barrier"):
        pl.semaphore_wait(barrier, len(greeted))
    stage(0)

    with scope("local"):
        row_i = lax.broadcasted_iota(jnp.int32, (T, T), 0)
        col_i = lax.broadcasted_iota(jnp.int32, (T, T), 1)
        upto = jnp.where(row_i <= col_i, 1.0, 0.0).astype(bf16)
        for i in range(2, 7):
            loads[i].wait()
        log_forget = -jnp.log1p(jnp.exp(-fg_ref[...]))
        ig = ig_ref[...]
        cum = left_dot(log_forget, upto, 1, 0)
        total = cum[:, T - 1 : T]
        weight_log = total - cum + ig
        peak = jnp.max(weight_log, axis=1, keepdims=True)
        weight = jnp.exp(weight_log - peak)
        scaled1, scaled2 = weight[0:1] * (KA ** -0.5), weight[1:2] * (KB ** -0.5)
        v1, v2 = v_ref[:, :DV], v_ref[:, DV:]
        k1, k2 = k1_ref[...], k2_ref[...]
        state = jnp.concatenate(
            [
                left_dot(jnp.transpose(k1.astype(f32)) * scaled1, v1, 1, 0),
                left_dot(k2.astype(f32) * scaled2, v2, 1, 0),
            ],
            axis=0,
        )
        n1 = left_dot(scaled1, k1, 1, 0)
        n2 = left_dot(scaled2, k2, 1, 1)
        n2 = jnp.concatenate([n2, jnp.zeros((1, KA - KB), f32)], axis=1)
        ones = jnp.ones((1, KA), f32)
        meta = jnp.concatenate(
            [n1, n2, total * ones, peak * ones, jnp.zeros((META - 6, KA), f32)], axis=0
        )
        for j in range(NY):
            st_send[j, :SH] = state[j * SH : (j + 1) * SH]
            st_send[j, SH:] = meta
        e1[pl.ds(iy, 1)] = st_send[pl.ds(iy, 1)]

    first_hop = Direct("y", NY, lambda j: st_send.at[j], e1, e1.at[0 : NY - 1], hop.at[0])
    first_hop.send()

    with scope("scores"):
        turned = jnp.transpose(jnp.concatenate([cum, cum, cum, cum], axis=0))
        causal = row_i >= col_i
        loads[7].wait()
        loads[8].wait()
        q1, q2 = q1_ref[...], jnp.transpose(q2_ref[...].astype(f32)).astype(bf16)
        local = []
        for h, (q, k, over, width, vh) in enumerate(((q1, k1, 1, KA, v1), (q2, k2, 0, KB, v2))):
            gaps = turned[:, h : h + 1] - cum[h : h + 1] + ig[h : h + 1]
            gaps = jnp.where(causal, gaps, -jnp.inf)
            top = jnp.max(gaps, axis=1, keepdims=True)
            scores = dg(q, k, 1, over) * (width ** -0.5)
            scores = scores * jnp.exp(gaps - top)
            local.append((top, left_dot(scores, vh, 1, 0), jnp.sum(scores, axis=1, keepdims=True)))

    stage(1)

    key_row = lax.broadcasted_iota(jnp.int32, (SH, KA), 0) + iy * SH

    def spread(both):
        return jnp.where(key_row < KA, both[0:1], both[1:2])

    def combine(early, late):
        decay_e, cell_e, norm_e, peak_e = early
        decay_l, cell_l, norm_l, peak_l = late
        moved = decay_l + peak_e
        ceiling = jnp.maximum(moved, peak_l)
        keep, fresh = jnp.exp(moved - ceiling), jnp.exp(peak_l - ceiling)
        return (
            decay_e + decay_l,
            spread(keep) * cell_e + spread(fresh) * cell_l,
            keep * norm_e + fresh * norm_l,
            ceiling,
        )

    def loaded(ref, j):
        return (ref[j, SH + 2 : SH + 4], ref[j, :SH], ref[j, SH : SH + 2], ref[j, SH + 4 : SH + 6])

    nothing = (
        jnp.zeros((2, KA), f32), jnp.zeros((SH, DV), f32), jnp.zeros((2, KA), f32),
        jnp.full((2, KA), NEG_BIG, f32),
    )
    stage(2)
    with scope("e1take"):
        first_hop.take()
    with scope("e1comb"):
        running, inside = nothing, []
        for j in range(NY):
            inside.append(running)
            running = combine(running, loaded(e1, j))
        e2_send[:SH] = running[1]
        e2_send[SH:] = jnp.concatenate(
            [running[2], running[0], running[3], jnp.zeros((META - 6, KA), f32)], axis=0
        )
        e2[pl.ds(iz, 1)] = e2_send[...][None]
    second_hop = Direct("z", NZ, lambda j: e2_send, e2, e2.at[0 : NZ - 1], hop.at[1])
    second_hop.send()
    stage(3)
    with scope("e2take"):
        second_hop.take()
    with scope("e2comb"):
        before = nothing
        for k in range(NZ):
            later = combine(before, loaded(e2, k))
            before = jax.tree.map(lambda new, old: jnp.where(k < iz, new, old), later, before)
        norm_in, peak_in = jnp.zeros((2, KA), f32), jnp.zeros((2, KA), f32)
        for j in range(NY):
            _, cell_j, norm_j, peak_j = combine(before, inside[j])
            f_send[j] = cell_j
            norm_in = jnp.where(iy == j, norm_j, norm_in)
            peak_in = jnp.where(iy == j, peak_j, peak_in)
        cin[pl.ds(iy, 1)] = f_send[pl.ds(iy, 1)]
    third_hop = Direct("y", NY, lambda j: f_send.at[j], cin, cin.at[0 : NY - 1], hop.at[2])
    third_hop.send()
    stage(4)
    stage(5, 0)
    with scope("e3take"):
        third_hop.take()

    with scope("cell"):
        for i in range(9, 15):
            loads[i].wait()
        cell_in = cin[...].reshape(KEYS, DV)
        columns = []
        for h, (q, width, cell) in enumerate(((q1, KA, cell_in[:KA]), (q2, KB, cell_in[KA:]))):
            top, own_num, own_den = local[h]
            carried = turned[:, h : h + 1] + peak_in[h : h + 1, 0:1]
            ceiling = jnp.maximum(carried, top)
            keep, fresh = jnp.exp(carried - ceiling), jnp.exp(top - ceiling)
            num = keep * right_dot(q, cell, 1, 0) + fresh * own_num
            den = keep * jnp.sum(q.astype(f32) * norm_in[h : h + 1, :width], axis=1, keepdims=True)
            den = den + fresh * own_den
            cell_out = num / jnp.maximum(jnp.abs(den), jnp.exp(-ceiling))
            center = jnp.mean(cell_out, -1, keepdims=True)
            away = cell_out - center
            var = jnp.mean(away * away, -1, keepdims=True)
            columns.append(away * lax.rsqrt(var + EPS))
        gate = 1.0 / (1.0 + jnp.exp(-og_ref[...].astype(f32)))
        mixed = (jnp.concatenate(columns, axis=1) * hg_ref[...] * gate).astype(bf16)
        wide = min(D, 512)
        for c in range(0, D, wide):
            part = dg(mixed, ow_ref[:, c : c + wide], 1, 0).astype(bf16)
            parts[:, :, :, c : c + wide] = part.reshape(X, 2, OWN, wide)
    out_proj = TpSum(X, parts, pair, chip_send, chip_recv, tsems.at[0])
    out_proj.start()
    stage(5, 1)
    with scope("rs1mid"):
        out_proj.between()
    stage(6)
    with scope("rs1take"):
        mixer = out_proj.total().astype(bf16).astype(f32)
    with scope("norm1"):
        first = normed(stream_own[...].astype(f32) + mixer, mg_ref[...]).astype(bf16)
        x_all[pl.ds(chip, 1), pl.ds(core, 1)] = first[None, None]
    rows_out = TpGather(X, x_all, tsems.at[1], rowsems)
    rows_out.start()
    stage(7)
    with scope("agrelay"):
        rows_out.relay()
    stage(8)
    with scope("agtake"):
        rows_out.take()
    with scope("upwait"):
        for item in ups:
            item.finish()
    with scope("mlp1"):
        wide_f = min(FD, 256)
        for c in range(0, FD, wide_f):
            x = x_all[...].reshape(T, D)
            w = up_all[:, :, :, c : c + wide_f].reshape(D, wide_f)
            act = jnp.maximum(dg(x, w, 1, 0), 0.0)
            hidden[:, c : c + wide_f] = (act * act).astype(bf16)

    wide_d = NY * RW

    def columns(shift):
        return lax.rem(iz + shift, NZ)

    def second(shift):
        w = down_all[pl.ds(columns(shift), 1)].reshape(wide_d, FD)
        return dg(hidden[...], w, 1, 1).astype(bf16)

    shifts = sorted(range(NZ), key=lambda s: min(s, NZ - s))
    early = early_blocks(NZ)
    sums = []
    later = NZ - 1 - early
    if early:
        with scope("mlp2a"):
            for i in range(early):
                shift = shifts[i]
                for item, axis in zip(downs, (1, 0)):
                    item.near(axis, min(shift, NZ - shift))
                parts_a[:, :, i] = second(shift).reshape(X, 2, OWN, wide_d)
        sums.append(TpSum(X, parts_a, pair_a, send_a, recv_a, tsems.at[2]))
        sums[-1].start()
    with scope("mlp2b"):
        for item, axis in zip(downs, (1, 0)):
            item.near(axis, NZ // 2 - 1)
        for i in range(later):
            parts_b[:, i] = second(shifts[early + i]).reshape(TP, OWN, wide_d)
    later_sum = Direct("tp", TP, lambda j: parts_b.at[j], recv_b, recv_b.at[0 : TP - 1], hop.at[4])
    later_sum.send()
    recv_b[pl.ds(it, 1)] = parts_b[pl.ds(it, 1)]
    with scope("downwait"):
        for item in downs:
            item.finish()
    with scope("mlp2 last"):
        last_parts[...] = second(shifts[-1]).reshape(TP, OWN, wide_d)
    last_sum = Direct("tp", TP, lambda j: last_parts.at[j], last_recv, last_recv.at[0 : TP - 1], hop.at[3])
    last_sum.send()
    with scope("rs2mid"):
        for item in sums:
            item.between()
    last_recv[pl.ds(it, 1)] = last_parts[pl.ds(it, 1)]
    with scope("drain"):
        for item in (first_hop, second_hop, third_hop, out_proj, rows_out, *ups, *downs):
            item.drain()

    def put(shift, value):
        mlp_sum[:, pl.ds(pl.multiple_of(columns(shift) * wide_d, wide_d), wide_d)] = value

    with scope("rs2later"):
        later_sum.take()
        total_of = jnp.sum(recv_b[...].astype(f32), axis=0)
        for i in range(later):
            put(shifts[early + i], total_of[i])
    with scope("rs2last"):
        last_sum.take()
        put(shifts[-1], jnp.sum(last_recv[...].astype(f32), axis=0))
    with scope("rs2take"):
        for item in sums:
            total_of = item.total()
            for i in range(early):
                put(shifts[i], total_of[i])
        mlp_out = mlp_sum[...].astype(bf16).astype(f32)
    with scope("norm2"):
        base = x_all[pl.ds(chip, 1), pl.ds(core, 1)].reshape(OWN, D).astype(f32)
        out_ref[...] = normed(base + mlp_out, outg_ref[...]).astype(bf16)
    with scope("lastdrain"):
        for item in (*sums, later_sum, last_sum):
            item.drain()


def layer(
    sizes, query_one, key_one, query_two, key_two, values, out_gate, in_gate, forget_gate,
    head_gain, out_weight, stream, mix_gain, up_weight, down_weight, out_gain,
):
    NZ, NY, TP = sizes
    X = TP // 2
    T, D = stream.shape
    OWN = T // TP
    RW, FD = up_weight.shape
    SH = (query_one.shape[1] + query_two.shape[1]) // NY
    KA = query_one.shape[1]
    sem = pltpu.SemaphoreType.DMA
    half = max(NY, NZ) // 2
    trees = 2 if NY == NZ else 4
    early = early_blocks(NZ)
    operands = (
        query_one, key_one, query_two.T, key_two.T, values, out_gate, in_gate, forget_gate,
        head_gain.reshape(1, -1), out_weight, stream, mix_gain.reshape(1, -1), up_weight,
        down_weight.T, out_gain.reshape(1, -1),
    )
    copied = [operands[i] for i in (0, 1, 2, 3, 4, 5, 6, 7, 8, 9, 11, 14)]

    def exchange(*inner):
        return [pltpu.VMEM((X, 2) + inner, bf16)] + [pltpu.VMEM((X,) + inner, bf16)] * 3

    return pl.pallas_call(
        functools.partial(kernel, sizes),
        out_shape=jax.ShapeDtypeStruct((OWN, D), bf16),
        in_specs=[pl.BlockSpec(memory_space=pltpu.HBM)] * len(operands),
        out_specs=pl.BlockSpec(memory_space=pltpu.VMEM),
        scratch_shapes=[pltpu.VMEM(a.shape, a.dtype) for a in copied]
        + [
            pltpu.VMEM((NZ, NY, RW, FD), bf16),
            pltpu.VMEM((NZ, NY, RW, FD), bf16),
            pltpu.VMEM((NY, SH + META, KA), f32),
            pltpu.VMEM((NY, SH + META, KA), f32),
            pltpu.VMEM((SH + META, KA), f32),
            pltpu.VMEM((NZ, SH + META, KA), f32),
            pltpu.VMEM((NY, SH, KA), f32),
            pltpu.VMEM((NY, SH, KA), f32),
        ]
        + exchange(OWN, D)
        + [pltpu.VMEM((X, 2, OWN, D), bf16), pltpu.VMEM((T, FD), bf16)]
        + exchange(max(early, 1), OWN, NY * RW)
        + [
            pltpu.VMEM((TP, NZ - 1 - early, OWN, NY * RW), bf16),
            pltpu.VMEM((TP, NZ - 1 - early, OWN, NY * RW), bf16),
            pltpu.VMEM((TP, OWN, NY * RW), bf16),
            pltpu.VMEM((TP, OWN, NY * RW), bf16),
            pltpu.VMEM((OWN, D), f32),
            pltpu.VMEM((OWN, D), bf16),
            sem((15,)),
            sem((5, 2)), sem((4, 2)), sem((trees, half)), sem((trees, half, half + 1)), sem((3, 4)), sem((X,)),
        ],
        compiler_params=pltpu.CompilerParams(
            collective_id=0, has_side_effects=True, vmem_limit_bytes=60000 * 1024
        ),
    )(*operands)


def build(mesh, nz, ny):
    tp = mesh.shape["tp"]
    split = Mesh(mesh.devices.reshape(nz, ny, tp), ("z", "y", "tp"))
    SP = ("z", "y")
    return jax.shard_map(
        functools.partial(layer, (nz, ny, tp)),
        mesh=split,
        in_specs=(
            P(SP, "tp"), P(SP, "tp"), P(SP, "tp"), P(SP, "tp"), P(SP, "tp"), P(SP, "tp"),
            P("tp", SP), P("tp", SP), P("tp"), P("tp", None), P(SP, None), P(),
            P(SP, "tp"), P("tp", SP), P(),
        ),
        out_specs=P(("z", "y", "tp"), None),
        check_vma=False,
    )


def solution(mesh):
    return build(mesh, 8, 8)
```
